32 devices in a mesh: rep: 2 (over y), fs: 4 (over z), tp: 4 (over x, core).
Axes of the slice: x: 2, y: 2, z: 4, core: 2. Of those that a mesh axis runs over, the one named last changes fastest.
Arguments:
- stream: bfloat16 [4096, 2048], P(('rep', 'fs'), 'tp'), parts along dimension 0, may hold values from -6 to 6
- in_weight: bfloat16 [2048, 1024], P('fs', 'tp'), may hold values from -0.125 to 0.125
- pool_weight: bfloat16 [8, 128, 128], P('tp'), may hold values from -0.5 to 0.5
- pool_scale: bfloat16 [1024], P('tp'), may hold values from 0.099609375 to 1.8984375
- out_weight: bfloat16 [1024, 2048], P('tp', 'fs'), may hold values from -0.1875 to 0.1875
- mix_gain: bfloat16 [2048], replicated, may hold values from 0.099609375 to 1.8984375
- ffn_gain: bfloat16 [2048], replicated, may hold values from 0.099609375 to 1.8984375
- gate_weight: bfloat16 [2048, 5632], P('fs', 'tp'), may hold values from -0.125 to 0.125
- up_weight: bfloat16 [2048, 5632], P('fs', 'tp'), may hold values from -0.125 to 0.125
- down_weight: bfloat16 [5632, 2048], P('tp', 'fs'), may hold values from -0.078125 to 0.078125
Outputs:
- result: bfloat16 [4096, 2048], P(('rep', 'fs'), 'tp'), parts along dimension 0
The draws below stay inside these ranges and needn't reach their ends.
There are 2 independent parts, one for each index of `rep`. The reference program is written for one: setup_inputs(seed, part) draws one part's arguments, and reference() takes and returns one part's arrays. A program takes and returns all parts, laid end to end along the dimension named above; an argument that names none is the same for every part. Nothing has to cross between parts.
All inputs are finite; a program needn't handle non-finite values.
Results may differ from the reference program's by a relative error of at most 0.015.
Values may be sent and summed in bfloat16 or wider, within the bound.
A program may use at most 64 MiB of HBM per device.

```python
import jax
import jax.numpy as jnp
from jax import lax

D = 2048
GROUPS = 8
GROUP_DIM = 128
FF = 5632
SEQ = 128
POOL_CH = 1024
TOKENS = 2048
N_TP = 4


def block_scale(own_key, shape, split, least, high):
    factor_of, own = 1.0, jax.random.fold_in(own_key, 6)
    for axis_at, parts in split:
        steps = jnp.exp(jax.random.uniform(jax.random.fold_in(own, axis_at), (parts,), jnp.float32, least / len(split), high / len(split)))
        factor_of = factor_of * jnp.repeat(steps, shape[axis_at] // parts).reshape([-1 if axis == axis_at else 1 for axis in range(len(shape))])
    return factor_of


def bell_draw(rng, extent, width, bound, cuts=(), kind=jnp.bfloat16):
    array = width * jax.random.normal(rng, extent, jnp.float32)
    if cuts:
        array = array * block_scale(rng, extent, cuts, -0.22, 0.18)
    return jnp.clip(array, -bound, bound).astype(kind)


def setup_inputs(seed: int = 0, part: int = 0) -> dict:
    keys = jax.random.split(jax.random.key(seed), 11)
    part_keys = jax.random.split(jax.random.fold_in(keys[10], part), 11)
    return {
        "stream": bell_draw(part_keys[0], (TOKENS, D), 1.0, 6.0, ((0, 4), (1, 4))),
        "in_weight": bell_draw(keys[1], (D, POOL_CH), D ** -0.5, 0.125, ((0, 4), (1, 4))),
        "pool_weight": bell_draw(keys[2], (GROUPS, GROUP_DIM, GROUP_DIM), GROUP_DIM ** -0.5, 0.5, ((0, 4),)),
        "pool_scale": jnp.clip(1.0 + 0.18 * jax.random.normal(keys[3], (POOL_CH,), jnp.float32), 0.099609375, 1.8984375).astype(jnp.bfloat16),
        "out_weight": bell_draw(keys[4], (POOL_CH, D), POOL_CH ** -0.5, 0.1875, ((0, 4), (1, 4))),
        "mix_gain": jnp.clip(1.0 + 0.18 * jax.random.normal(keys[5], (D,), jnp.float32), 0.099609375, 1.8984375).astype(jnp.bfloat16),
        "ffn_gain": jnp.clip(1.0 + 0.18 * jax.random.normal(keys[6], (D,), jnp.float32), 0.099609375, 1.8984375).astype(jnp.bfloat16),
        "gate_weight": bell_draw(keys[7], (D, FF), D ** -0.5, 0.125, ((0, 4), (1, 4))),
        "up_weight": bell_draw(keys[8], (D, FF), D ** -0.5, 0.125, ((0, 4), (1, 4))),
        "down_weight": bell_draw(keys[9], (FF, D), FF ** -0.5, 0.078125, ((0, 4), (1, 4))),
    }


epsilon = 1e-06

def root_norm(values, gain_vec):
    widened = values.astype(jnp.float32)
    scaled = widened * lax.rsqrt(lax.optimization_barrier(jnp.mean(widened * widened, axis=-1, keepdims=True)) + epsilon)
    return (scaled * gain_vec.astype(jnp.float32)).astype(jnp.bfloat16)

def window_tables(first_group, group_count, seq_len, total_groups):
    group_ids = first_group + jnp.arange(group_count, dtype=jnp.int32)
    reaches = jnp.left_shift(jnp.int32(2), 4 * group_ids // total_groups)
    query_pos = jnp.arange(seq_len, dtype=jnp.int32)[:, None]
    earlier = jnp.arange(seq_len, dtype=jnp.int32)[None, :]
    inside = (earlier <= query_pos)[None] & (earlier[None] > query_pos[None] - reaches[:, None, None])
    counts = jnp.minimum(query_pos[:, 0][None, :] + 1, reaches[:, None]).astype(jnp.float32)
    return (inside, counts)

def block_sum(operand, weights):
    block_width = operand.shape[1] // N_TP
    running = jnp.zeros((operand.shape[0], weights.shape[1]), jnp.float32)
    for block_id in range(N_TP):
        product = jnp.dot(operand[:, block_id * block_width:(block_id + 1) * block_width], weights[block_id * block_width:(block_id + 1) * block_width], preferred_element_type=jnp.float32)
        rounded = lax.optimization_barrier(product.astype(jnp.bfloat16))
        running = running + rounded.astype(jnp.float32)
    return running

def reference(stream, in_weight, pool_weight, pool_scale, out_weight, mix_gain, ffn_gain, gate_weight, up_weight, down_weight):
    normed = root_norm(stream, mix_gain)
    pooled_in = jnp.dot(normed, in_weight, preferred_element_type=jnp.float32).astype(jnp.bfloat16)
    inside, counts = window_tables(0, GROUPS, SEQ, GROUPS)
    grouped = pooled_in.astype(jnp.float32).reshape(TOKENS // SEQ, SEQ, GROUPS, GROUP_DIM)
    window_sums = jnp.einsum('gts,nsgc->ntgc', inside.astype(jnp.float32), grouped, precision=lax.Precision.HIGHEST)
    contrast = (window_sums / counts.T[None, :, :, None] - grouped).astype(jnp.bfloat16)
    mixed_out = jnp.einsum('ntgc,gcd->ntgd', contrast.astype(jnp.float32), pool_weight.astype(jnp.float32))
    group_out = (mixed_out.reshape(TOKENS, POOL_CH) * pool_scale.astype(jnp.float32)).astype(jnp.bfloat16)
    mixer_sum = block_sum(group_out, out_weight)
    middle = (stream.astype(jnp.float32) + mixer_sum).astype(jnp.bfloat16)
    normed_ffn = root_norm(middle, ffn_gain)
    gate_acts = jnp.dot(normed_ffn, gate_weight, preferred_element_type=jnp.float32)
    up_acts = jnp.dot(normed_ffn, up_weight, preferred_element_type=jnp.float32)
    hidden = (jax.nn.silu(gate_acts) * up_acts).astype(jnp.bfloat16)
    ffn_sum = block_sum(hidden, down_weight)
    return (middle.astype(jnp.float32) + ffn_sum).astype(jnp.bfloat16)
```

```python
import functools

import jax
import jax.numpy as jnp
from jax import lax
from jax.experimental import pallas as pl
from jax.experimental.pallas import tpu as pltpu
from jax.sharding import PartitionSpec as P

SEQ = 128
EPSILON = 1e-06
MESH = pl.DeviceIdType.MESH
BY_ROWS = (True, False, True, True, False)
PIECES = ((0, 0), (1, 0), (2, 0), (3, 0), (2, 1), (3, 1), (4, 0), (4, 1))
CHUNKS = (1, 1, 2, 2, 2)


def ring_kernel(sizes, stream, in_w, out_w, up_w, gate_w, down_w, pool_w, scale,
           mix_gain, ffn_gain, result,
           in_all, out_all, up_all, gate_all, down_all,
           rows_all, normed, group_out, hidden, middle, mid_all,
           mix_send, mix_recv, ffn_send, ffn_recv,
           ring_send, ring_recv, fwd_send, fwd_recv, own_sem,
           tp_send, tp_recv, keep_sem):
    reps, fs, tp = sizes
    half = fs // 2
    my_rep, me, my_tp = lax.axis_index("rep"), lax.axis_index("fs"), lax.axis_index("tp")
    own = (in_w, out_w, up_w, gate_w, down_w)
    full = (in_all, out_all, up_all, gate_all, down_all)
    tokens, width = stream.shape

    def turn(at, by, count):
        return lax.rem(at + by + count, count)

    def piece(which, owner, row, count):
        block_rows, block_cols = own[which].shape
        if BY_ROWS[which]:
            return full[which].at[pl.ds(pl.multiple_of(owner * block_rows + row, 16), count), :]
        return full[which].at[pl.ds(pl.multiple_of(row, 16), count),
                              pl.ds(pl.multiple_of(owner * block_cols, 128), block_cols)]

    def span(number, step, way):
        which, chunk = PIECES[number]
        rows = own[which].shape[0]
        cut = rows % (CHUNKS[which] * reps * 2 * 16) == 0
        count = rows // CHUNKS[which] if cut else (rows, 0)[chunk]
        row = chunk * (rows // CHUNKS[which])
        count = count // reps
        row = row + my_rep * count
        if step == half:
            count = count // 2
            row = row + way * count
        return which, row, count

    def empty(number):
        return span(number, 1, 0)[2] == 0

    def ring(number, step, way):
        which, row, count = span(number, step, way)
        sign = 1 - 2 * way
        owner = turn(me, -sign * (step - 1), fs)
        if step == 1:
            source = own[which].at[pl.ds(pl.multiple_of(row, 16), count), :]
        else:
            source = piece(which, owner, row, count)
        return pltpu.make_async_remote_copy(
            src_ref=source, dst_ref=piece(which, owner, row, count),
            send_sem=ring_send.at[number, step - 1, way],
            recv_sem=ring_recv.at[number, step - 1, way],
            device_id={"fs": turn(me, sign, fs)}, device_id_type=MESH)

    def forward(number, step, way, peer):
        which, row, count = span(number, step, way)
        block = piece(which, turn(me, -(1 - 2 * way) * step, fs), row, count)
        return pltpu.make_async_remote_copy(
            src_ref=block, dst_ref=block,
            send_sem=fwd_send.at[number, peer - 1, step - 1, way],
            recv_sem=fwd_recv.at[number, peer - 1, step - 1, way],
            device_id={"rep": turn(my_rep, peer, reps)}, device_id_type=MESH)

    def begin(*numbers):
        for number in numbers:
            if not empty(number):
                for way in (0, 1):
                    ring(number, 1, way).start()

    def advance(number, step):
        if empty(number):
            return
        for way in (0, 1):
            ring(number, step, way).wait_recv()
            if step < half:
                ring(number, step + 1, way).start()
            for peer in range(1, reps):
                forward(number, step, way, peer).start()

    def early(*numbers):
        for number in numbers:
            for step in range(1, half):
                advance(number, step)

    def late(*numbers):
        for number in numbers:
            advance(number, half)

    def arrived(*numbers):
        for number in numbers:
            if PIECES[number][1] == 0:
                keeps[PIECES[number][0]].wait()
            if empty(number):
                continue
            for step in range(1, half + 1):
                for way in (0, 1):
                    for peer in range(1, reps):
                        forward(number, step, way, peer).wait()

    def tp_copy(stage, offset, source, target):
        return pltpu.make_async_remote_copy(
            src_ref=source, dst_ref=target,
            send_sem=tp_send.at[stage, offset - 1], recv_sem=tp_recv.at[stage, offset - 1],
            device_id={"tp": turn(my_tp, offset, tp)}, device_id_type=MESH)

    def feature_cols(owner):
        return pl.ds(pl.multiple_of(owner * width, 128), width)

    barrier = pltpu.get_barrier_semaphore()
    greeted = 0
    for name, at, count, offsets in (
            ("fs", me, fs, (1, -1)),
            ("tp", my_tp, tp, range(1, tp)),
            ("rep", my_rep, reps, range(1, reps))):
        for offset in offsets:
            pl.semaphore_signal(barrier, inc=1, device_id={name: turn(at, offset, count)},
                                device_id_type=MESH)
            greeted += 1
    pl.semaphore_wait(barrier, greeted)

    begin(0, 1)
    stream_sends = []
    for offset in range(1, tp):
        copy = tp_copy(0, offset, stream, rows_all.at[:, feature_cols(my_tp)])
        copy.start()
        stream_sends.append(copy)
    keeps = []
    for which in range(len(own)):
        keep = pltpu.make_async_copy(
            own[which], piece(which, me, 0, own[which].shape[0]), own_sem.at[which])
        keep.start()
        keeps.append(keep)
    keep_stream = pltpu.make_async_copy(
        stream, rows_all.at[:, feature_cols(my_tp)], keep_sem)
    keep_stream.start()
    early(0, 1)
    begin(2, 3, 4)
    late(0, 1)

    def norm_into(source, gain, target):
        tile = 64

        def body(i, carry):
            at = pl.ds(pl.multiple_of(i * tile, tile), tile)
            wide = source[at, :].astype(jnp.float32)
            mean = jnp.mean(wide * wide, axis=-1, keepdims=True)
            target[at, :] = (wide * lax.rsqrt(mean + EPSILON)
                             * gain[...].astype(jnp.float32)).astype(jnp.bfloat16)
            return carry

        lax.fori_loop(0, tokens // tile, body, 0)

    keep_stream.wait()
    for copy in stream_sends:
        copy.wait()
    norm_into(rows_all, mix_gain, normed)
    arrived(0)

    local_groups, group_dim = pool_w.shape[0], pool_w.shape[1]
    at_row = lax.broadcasted_iota(jnp.int32, (SEQ, SEQ), 0)
    at_col = lax.broadcasted_iota(jnp.int32, (SEQ, SEQ), 1)
    insides, inverses = [], []
    for g in range(local_groups):
        group = my_tp * local_groups + g
        level = lax.div(4 * group, local_groups * tp)
        reach = jnp.int32(2)
        for bit in range(1, 4):
            reach = jnp.where(level >= bit, jnp.int32(2 << bit), reach)
        inside = (at_col <= at_row) & (at_col > at_row - reach)
        insides.append(jnp.where(inside, 1.0, 0.0).astype(jnp.bfloat16))
        inverses.append(jnp.minimum(at_row + 1, reach).astype(jnp.float32)[:, :1])

    def mix(i, carry):
        at = pl.ds(pl.multiple_of(i * SEQ, SEQ), SEQ)
        pooled = jnp.dot(normed[at, :], in_all[...],
                         preferred_element_type=jnp.float32).astype(jnp.bfloat16)
        for g in range(local_groups):
            cols = slice(g * group_dim, (g + 1) * group_dim)
            part = pooled[:, cols]
            sums = jnp.dot(insides[g], part, preferred_element_type=jnp.float32)
            contrast = (sums / inverses[g] - part.astype(jnp.float32)).astype(jnp.bfloat16)
            mixed = jnp.dot(contrast, pool_w[g], preferred_element_type=jnp.float32)
            group_out[at, cols] = (mixed * scale[:, cols].astype(jnp.float32)).astype(jnp.bfloat16)
        return carry

    lax.fori_loop(0, tokens // SEQ, mix, 0)

    arrived(1)
    early(2)

    def spread(operand, weights, stage, sends, tile):
        def block(owner, target):
            def body(i, carry):
                at = pl.ds(pl.multiple_of(i * tile, tile), tile)
                target[at, :] = jnp.dot(operand[at, :], weights[:, feature_cols(owner)],
                                        preferred_element_type=jnp.float32).astype(jnp.bfloat16)
                return carry
            lax.fori_loop(0, tokens // tile, body, 0)

        copies = []
        recv = mix_recv if stage == 1 else ffn_recv
        for offset in sorted(range(1, tp), key=lambda o: -min(o, tp - o)):
            block(turn(my_tp, offset, tp), sends.at[offset - 1])
            copy = tp_copy(stage, offset, sends.at[offset - 1], recv.at[offset - 1])
            copy.start()
            copies.append(copy)
        block(my_tp, sends.at[tp - 1])
        return copies

    def gather_sum(base, recv, sends, target):
        tile = 64

        def body(i, carry):
            at = pl.ds(pl.multiple_of(i * tile, tile), tile)
            total = sends[tp - 1, at, :].astype(jnp.float32)
            for k in range(tp - 1):
                total = total + recv[k, at, :].astype(jnp.float32)
            target[at, :] = (base[at, :].astype(jnp.float32) + total).astype(jnp.bfloat16)
            return carry

        lax.fori_loop(0, tokens // tile, body, 0)

    mix_copies = spread(group_out, out_all, 1, mix_send, tokens // 2)
    early(3)
    begin(5)
    for copy in mix_copies:
        copy.wait()
    gather_sum(stream, mix_recv, mix_send, middle)
    keep_middle = pltpu.make_async_copy(middle, mid_all.at[:, feature_cols(my_tp)], keep_sem)
    keep_middle.start()
    middle_copies = []
    for offset in range(1, tp):
        copy = tp_copy(2, offset, middle, mid_all.at[:, feature_cols(my_tp)])
        copy.start()
        middle_copies.append(copy)
    early(4)
    begin(6, 7)
    late(2, 3)
    keep_middle.wait()
    for copy in middle_copies:
        copy.wait()
    norm_into(mid_all, ffn_gain, normed)
    early(5)
    late(4)
    early(6)
    late(5)
    early(7)
    late(6)
    arrived(2, 3, 4, 5)
    tile = tokens // 2

    def gated(i, carry):
        at = pl.ds(pl.multiple_of(i * tile, tile), tile)
        values = normed[at, :]
        gate = jnp.dot(values, gate_all[...], preferred_element_type=jnp.float32)
        up = jnp.dot(values, up_all[...], preferred_element_type=jnp.float32)
        hidden[at, :] = (gate / (1.0 + jnp.exp(-gate)) * up).astype(jnp.bfloat16)
        return carry

    lax.fori_loop(0, tokens // tile, gated, 0)
    late(7)
    arrived(6, 7)
    ffn_copies = spread(hidden, down_all, 3, ffn_send, tokens // 2)
    for number in range(len(PIECES)):
        if not empty(number):
            for step in range(1, half + 1):
                for way in (0, 1):
                    ring(number, step, way).wait_send()
    for copy in ffn_copies:
        copy.wait()
    gather_sum(middle, ffn_recv, ffn_send, result)


def ring_on_device(sizes, stream, in_weight, pool_weight, pool_scale, out_weight,
              mix_gain, ffn_gain, gate_weight, up_weight, down_weight):
    reps, fs, tp = sizes
    half = fs // 2
    tokens, width = stream.shape
    features = width * tp
    own = (in_weight, out_weight, up_weight, gate_weight, down_weight)
    full = [pltpu.VMEM((w.shape[0] * fs, w.shape[1]) if by_rows else (w.shape[0], w.shape[1] * fs),
                       jnp.bfloat16) for w, by_rows in zip(own, BY_ROWS)]
    units = gate_weight.shape[1]
    bf = jnp.bfloat16
    vmem = pl.BlockSpec(memory_space=pltpu.VMEM)
    hbm = pl.BlockSpec(memory_space=pl.ANY)
    dma = pltpu.SemaphoreType.DMA
    flops = 2 * tokens * (2 * features * in_weight.shape[1] + 3 * features * units)
    return pl.pallas_call(
        functools.partial(ring_kernel, sizes),
        out_shape=jax.ShapeDtypeStruct(stream.shape, bf),
        in_specs=[vmem] + [hbm] * 5 + [vmem] * 4,
        out_specs=vmem,
        scratch_shapes=full + [
            pltpu.VMEM((tokens, features), bf),
            pltpu.VMEM((tokens, features), bf),
            pltpu.VMEM((tokens, in_weight.shape[1]), bf),
            pltpu.VMEM((tokens, units), bf),
            pltpu.VMEM((tokens, width), bf),
            pltpu.VMEM((tokens, features), bf),
            pltpu.VMEM((tp, tokens, width), bf),
            pltpu.VMEM((tp - 1, tokens, width), bf),
            pltpu.VMEM((tp, tokens, width), bf),
            pltpu.VMEM((tp - 1, tokens, width), bf),
            dma((len(PIECES), half, 2)),
            dma((len(PIECES), half, 2)),
            dma((len(PIECES), max(reps - 1, 1), half, 2)),
            dma((len(PIECES), max(reps - 1, 1), half, 2)),
            dma((len(own),)),
            dma((4, tp - 1)),
            dma((4, tp - 1)),
            dma(()),
        ],
        compiler_params=pltpu.CompilerParams(
            collective_id=0, has_side_effects=True, vmem_limit_bytes=64 * 1024 * 1024 - 65536),
        cost_estimate=pl.CostEstimate(flops=flops, bytes_accessed=flops // 512, transcendentals=0),
    )(stream, in_weight, out_weight, up_weight, gate_weight, down_weight, pool_weight,
      pool_scale.reshape(1, -1), mix_gain.reshape(1, -1), ffn_gain.reshape(1, -1))


IN, OUT, UP, GATE, DOWN = range(5)
LANES = 128


def pair_kernel(sizes, stream, in_w, out_w, up_w, gate_w, down_w, pool_w, scale,
                mix_gain, ffn_gain, result,
                in_all, out_all, up_all, gate_all, down_all,
                rows_all, normed, group_out, hidden, mid_all, normed_ffn,
                pool_sib, scale_sib,
                mix_own, mix_send, mix_recv, ffn_own, ffn_send, ffn_recv, pair_send, pair_recv,
                last_send, last_recv,
                z_send, z_recv, pass_send, y_send, y_recv, d_send, d_recv, own_sem,
                in_send, in_recv, pool_send, pool_recv, mix_sems, mid_send, mid_recv,
                x_send, x_recv, p_send, p_recv, l_send, l_recv):
    reps, fs, tp = sizes
    y, z, lane_id = lax.axis_index("rep"), lax.axis_index("fs"), lax.axis_index("tp")
    x, core = lax.div(lane_id, 2), lax.rem(lane_id, 2)
    own = (in_w, out_w, up_w, gate_w, down_w)
    full = (in_all, out_all, up_all, gate_all, down_all)
    tokens, width = stream.shape
    rows = tokens // 2
    wide = 2 * width
    seat, pair = lax.rem(z, 2), lax.div(z, 2)
    peer = z + 1 - 2 * seat
    near = jnp.where(pair == 0, 2, 1)
    far = jnp.where(pair == 0, 3, 0)
    inner = (z == 1) | (z == 2)
    f32, bf16 = jnp.float32, jnp.bfloat16

    blocks = gate_w.shape[1] // LANES
    few, many = blocks // 2, blocks - blocks // 2

    SIB = {"tp": lane_id + 1 - 2 * core}
    XPEER = {"tp": lane_id + 2 - 4 * x}
    XSIB = {"tp": 2 * (1 - x) + 1 - core}
    YPEER = {"rep": 1 - y}
    ZPEER = {"fs": peer}

    def at_least(value, multiple):
        return pl.multiple_of(value, multiple)

    def remote(source, target, send, recv, device):
        return pltpu.make_async_remote_copy(
            src_ref=source, dst_ref=target, send_sem=send, recv_sem=recv,
            device_id=device, device_id_type=MESH)

    def sized(which, core_at, seat_at, act):
        if which in (IN, OUT) or few == many:
            act(many)
            return
        big = core_at == seat_at

        @pl.when(big)
        def _():
            act(many)

        @pl.when(jnp.logical_not(big))
        def _():
            act(few)

    def place(which, source, half, core_at, seat_at, count):
        block_rows, block_cols = own[which].shape
        ref = full[which]
        if which == IN:
            part = block_rows // 2
            row, size = (source * block_rows, block_rows) if half is None else (
                source * block_rows + half * part, part)
            return ref.at[pl.ds(at_least(row, 16), size),
                          pl.ds(at_least(core_at * block_cols, LANES), block_cols)]
        if which == OUT:
            part = block_rows // 2
            row, size = (core_at * block_rows, block_rows) if half is None else (
                core_at * block_rows + half * part, part)
            return ref.at[pl.ds(at_least(row, 16), size),
                          pl.ds(at_least(source * block_cols, LANES), block_cols)]
        first = core_at * jnp.where(seat_at == 0, many, few) * LANES
        if which == DOWN:
            part = block_cols // 2
            col, size = (source * block_cols, block_cols) if half is None else (
                source * block_cols + half * part, part)
            return ref.at[pl.ds(at_least(first, LANES), count * LANES),
                          pl.ds(at_least(col, LANES), size)]
        part = block_rows // 2
        row, size = (source * block_rows, block_rows) if half is None else (
            source * block_rows + half * part, part)
        return ref.at[pl.ds(at_least(row, 16), size),
                      pl.ds(at_least(first, LANES), count * LANES)]

    def held(which, half, seat_at, count):
        block_rows, block_cols = own[which].shape
        ref = own[which]
        if which in (IN, OUT):
            if half is None:
                return ref
            part = block_rows // 2
            return ref.at[pl.ds(at_least(half * part, 16), part), :]
        first = seat_at * jnp.where(core == 0, many, few) * LANES
        if which == DOWN:
            part = block_cols // 2
            unit_rows = pl.ds(at_least(first, LANES), count * LANES)
            if half is None:
                return ref.at[unit_rows, :]
            return ref.at[unit_rows, pl.ds(at_least(half * part, LANES), part)]
        part = block_rows // 2
        unit_cols = pl.ds(at_least(first, LANES), count * LANES)
        if half is None:
            return ref.at[:, unit_cols]
        return ref.at[pl.ds(at_least(half * part, 16), part), unit_cols]

    def z_start(which, dest):
        to = lax.rem(dest, 2)
        sized(which, core, to, lambda n: remote(
            held(which, y, to, n), place(which, z, y, core, to, n),
            z_send.at[which, dest], z_recv.at[which, z], {"fs": dest}).start())

    def z_sent(which, dest):
        to = lax.rem(dest, 2)
        sized(which, core, to, lambda n: remote(
            held(which, y, to, n), place(which, z, y, core, to, n),
            z_send.at[which, dest], z_recv.at[which, z], {"fs": dest}).wait_send())

    def z_pass(which, source):
        block = place(which, source, y, core, seat, many)
        return remote(block, block, pass_send.at[which, lax.rem(source, 2)],
                      z_recv.at[which, source], ZPEER)

    def arrived(which, source):
        def act(n):
            block = place(which, source, y, core, seat, n)
            remote(block, block, y_send.at[which, source], z_recv.at[which, source],
                   YPEER).wait_recv()
        sized(which, core, seat, act)

    def across(which, source, step):
        def act(n):
            half = 1 - y if step == "recv" else y
            block = place(which, source, half, core, seat, n)
            copy = remote(block, block, y_send.at[which, source], y_recv.at[which, source], YPEER)
            {"start": copy.start, "recv": copy.wait_recv, "send": copy.wait_send}[step]()
        sized(which, core, seat, act)

    def beside(which, source, half, step, mine=False):
        slot = 0 if half is None else half
        whose = 1 - core if step == "recv" else core

        def act(n):
            block = place(which, source, half, whose, seat, n)
            start = held(which, half, seat, n) if mine else block
            copy = remote(start, block, d_send.at[which, source, slot],
                          d_recv.at[which, source, slot], SIB)
            {"start": copy.start, "recv": copy.wait_recv, "send": copy.wait_send}[step]()
        sized(which, whose, seat, act)

    def keep(which, step):
        def act(n):
            copy = pltpu.make_async_copy(held(which, None, seat, n),
                                         place(which, z, None, core, seat, n), own_sem.at[which])
            {"start": copy.start, "wait": copy.wait}[step]()
        sized(which, core, seat, act)

    def relay(which, source):
        arrived(which, source)
        across(which, source, "start")

    def share(which, source):
        across(which, source, "recv")
        beside(which, source, None, "start")

    def feature_cols(owner):
        return pl.ds(at_least(owner * width, LANES), width)

    def token_rows(half):
        return pl.ds(at_least(half * rows, 16), rows)

    def stream_copy(number, device, half):
        return remote(stream.at[token_rows(half), :], rows_all.at[:, feature_cols(lane_id)],
                      in_send.at[number], in_recv.at[number], device)

    barrier = pltpu.get_barrier_semaphore()
    greeted = 0
    for device in (SIB, XPEER, XSIB, YPEER, ZPEER, {"fs": near}, {"fs": far}):
        pl.semaphore_signal(barrier, inc=1, device_id=device, device_id_type=MESH)
        greeted += 1
    pl.semaphore_wait(barrier, greeted)

    for which in (IN, OUT):
        z_start(which, near)
        z_start(which, peer)
        if which == IN:
            stream_copies = [stream_copy(0, XPEER, core), stream_copy(1, XSIB, 1 - core),
                             stream_copy(2, SIB, 1 - core)]
            for copy in stream_copies:
                copy.start()
            pool_copy = remote(pool_w, pool_sib, pool_send.at[0], pool_recv.at[0], SIB)
            scale_copy = remote(scale, scale_sib, pool_send.at[1], pool_recv.at[1], SIB)
            pool_copy.start()
            scale_copy.start()
    for which in range(5):
        keep(which, "start")
        if which == DOWN:
            for half in (0, 1):
                beside(which, z, half, "start", mine=True)
        else:
            beside(which, z, None, "start", mine=True)
    for which in (GATE, UP):
        z_start(which, peer)
    for which in (GATE, UP):
        z_start(which, far)

    @pl.when(inner)
    def _():
        for which in (GATE, UP):
            z_start(which, near)

    rows_all[:, feature_cols(lane_id)] = stream[token_rows(core), :]

    def take(which):
        relay(which, peer)
        for source in (near, far):
            arrived(which, source)

            @pl.when(inner)
            def _():
                z_pass(which, source).start()
            across(which, source, "start")

    take(IN)

    def norm_into(source, gain, target, first, count):
        tile = 64

        def body(i, carry):
            at = pl.ds(at_least(first + i * tile, tile), tile)
            values = source[at, :].astype(f32)
            mean = jnp.mean(values * values, axis=-1, keepdims=True)
            target[at, :] = (values * lax.rsqrt(mean + EPSILON)
                             * gain[...].astype(f32)).astype(bf16)
            return carry

        lax.fori_loop(0, count // tile, body, 0)

    for copy in stream_copies:
        copy.wait()
    norm_into(rows_all, mix_gain, normed, 0, rows)
    for source in (peer, near, far):
        share(IN, source)
    take(OUT)
    pool_copy.wait()
    scale_copy.wait()
    for source in (z, peer, near, far):
        beside(IN, source, None, "recv")
    keep(IN, "wait")

    local_groups, group_dim = pool_w.shape[0], pool_w.shape[1]
    at_row = lax.broadcasted_iota(jnp.int32, (SEQ, SEQ), 0)
    at_col = lax.broadcasted_iota(jnp.int32, (SEQ, SEQ), 1)
    pooled = jnp.dot(normed[...], in_all[...], preferred_element_type=f32).astype(bf16)
    for g in range(2 * local_groups):
        owner, place_in = divmod(g, local_groups)
        group = x * 2 * local_groups + g
        level = lax.div(4 * group, local_groups * tp)
        reach = jnp.int32(2)
        for bit in range(1, 4):
            reach = jnp.where(level >= bit, jnp.int32(2 << bit), reach)
        inside = jnp.where((at_col <= at_row) & (at_col > at_row - reach), 1.0, 0.0).astype(bf16)
        counts = jnp.minimum(at_row + 1, reach).astype(f32)[:, :1]
        is_own = core == owner
        cols = slice(g * group_dim, (g + 1) * group_dim)
        own_cols = slice(place_in * group_dim, (place_in + 1) * group_dim)
        weight = jnp.where(is_own, pool_w[place_in], pool_sib[place_in])
        factor = jnp.where(is_own, scale[:, own_cols].astype(f32),
                           scale_sib[:, own_cols].astype(f32))
        for s in range(rows // SEQ):
            at = slice(s * SEQ, (s + 1) * SEQ)
            part = pooled[at, cols]
            sums = jnp.dot(inside, part, preferred_element_type=f32)
            contrast = (sums / counts - part.astype(f32)).astype(bf16)
            mixed = jnp.dot(contrast, weight, preferred_element_type=f32)
            group_out[at, cols] = (mixed * factor).astype(bf16)

    for source in (peer, near, far):
        share(OUT, source)
    for source in (z, peer, near, far):
        beside(OUT, source, None, "recv")
    keep(OUT, "wait")

    def half_cols(owner):
        return pl.ds(at_least(owner * wide, LANES), wide)

    mix_send[...] = jnp.dot(group_out[...], out_all[:, half_cols(1 - x)],
                            preferred_element_type=f32).astype(bf16)
    mix_copy = remote(mix_send, mix_recv, mix_sems.at[0], mix_sems.at[1], XPEER)
    mix_copy.start()
    mix_own[...] = jnp.dot(group_out[...], out_all[:, half_cols(x)], preferred_element_type=f32)
    for which in (GATE, UP):
        relay(which, peer)
    mix_copy.wait()
    mid_rows = pl.ds(at_least(seat * rows, 16), rows)
    mid_all[mid_rows, half_cols(x)] = (
        rows_all[:, half_cols(x)].astype(f32) + (mix_own[...] + mix_recv[...].astype(f32))).astype(bf16)

    def mid_copy(number, block, device):
        view = mid_all.at[pl.ds(at_least(block * rows, 16), rows), half_cols(x)]
        return remote(view, view, mid_send.at[number], mid_recv.at[number], device)

    to_pair, to_x, to_x_later = mid_copy(0, seat, ZPEER), mid_copy(1, seat, XPEER), mid_copy(2, 1 - seat, XPEER)
    to_pair.start()
    to_x.start()

    @pl.when(jnp.logical_not(inner))
    def _():
        for which in (GATE, UP):
            z_start(which, near)

    for which in (GATE, UP):
        share(which, peer)
    to_pair.wait_recv()
    to_x_later.start()
    for which in (GATE, UP):
        relay(which, near)
    to_x.wait_recv()
    norm_into(mid_all, ffn_gain, normed_ffn, seat * rows, rows)
    for which in (GATE, UP):
        share(which, near)
    z_start(DOWN, peer)
    z_start(DOWN, near)
    z_start(DOWN, far)
    to_x_later.wait_recv()
    norm_into(mid_all, ffn_gain, normed_ffn, (1 - seat) * rows, rows)
    for which in (GATE, UP):
        relay(which, far)
    for which in (GATE, UP):
        share(which, far)
    relay(DOWN, peer)
    beside(DOWN, peer, y, "start")
    for which in (GATE, UP):
        for source in (z, peer, near, far):
            beside(which, source, None, "recv")
        keep(which, "wait")

    tile = rows

    def gated(i, carry):
        at = pl.ds(at_least(i * tile, tile), tile)
        values = normed_ffn[at, :]
        gate = jnp.dot(values, gate_all[...], preferred_element_type=f32)
        up = jnp.dot(values, up_all[...], preferred_element_type=f32)
        hidden[at, :] = (gate / (1.0 + jnp.exp(-gate)) * up).astype(bf16)
        return carry

    lax.fori_loop(0, 2 * rows // tile, gated, 0)

    sub = width // 2
    order = (z, peer, near, far)
    keeps_early = x == pair

    def is_kept(o):
        return keeps_early if o < 2 else jnp.logical_not(keeps_early)

    def half_of(turn):
        return y if turn == 0 else 1 - y

    def column_block(o, turn):
        at = pl.ds(at_least(order[o] * width + half_of(turn) * sub, LANES), sub)
        slot = 2 * (o % 2) + turn
        values = jnp.dot(hidden[...], down_all[:, at], preferred_element_type=f32)

        @pl.when(is_kept(o))
        def _():
            ffn_own[slot] = values

        @pl.when(jnp.logical_not(is_kept(o)))
        def _():
            ffn_send[slot] = values.astype(bf16)
            x_copy(slot).start()

    def x_copy(slot):
        return remote(ffn_send.at[slot], ffn_recv.at[slot], x_send.at[slot], x_recv.at[slot], XPEER)

    def pair_copy(o, turn):
        quarter, half = lax.rem(order[o], 2), half_of(turn)
        return remote(pair_send.at[quarter, half], pair_recv.at[quarter, half],
                      p_send.at[quarter, half], p_recv.at[quarter, half], ZPEER)

    def fold(o, turn):
        slot = 2 * (o % 2) + turn
        quarter, half = lax.rem(order[o], 2), half_of(turn)

        @pl.when(is_kept(o))
        def _():
            x_copy(slot).wait_recv()
            theirs = pl.ds(at_least((1 - seat) * rows, 16), rows)
            pair_send[quarter, half] = (ffn_own[slot, theirs, :]
                                        + ffn_recv[slot, theirs, :].astype(f32)).astype(bf16)
            pair_copy(o, turn).start()

    def last_copy(half):
        return remote(last_send.at[half], last_recv.at[half], l_send.at[half], l_recv.at[half], SIB)

    def settle(o, turn):
        slot = 2 * (o % 2) + turn
        quarter, half = lax.rem(order[o], 2), half_of(turn)

        @pl.when(is_kept(o))
        def _():
            pair_copy(o, turn).wait_recv()
            ours = pl.ds(at_least(seat * rows, 16), rows)
            cols = pl.ds(at_least(order[o] * width + half * sub, LANES), sub)
            total = (ffn_own[slot, ours, :] + ffn_recv[slot, ours, :].astype(f32)
                     + pair_recv[quarter, half].astype(f32))
            value = (mid_all[ours, cols].astype(f32) + total).astype(bf16)

            @pl.when(quarter == core)
            def _():
                result[token_rows(core), pl.ds(at_least(half * sub, LANES), sub)] = value

            @pl.when(quarter != core)
            def _():
                last_send[half] = value
                last_copy(half).start()

    def pour(source):
        across(DOWN, source, "recv")
        beside(DOWN, source, 1 - y, "start")

    def ready(source, turn):
        beside(DOWN, source, half_of(turn), "recv")

    pour(peer)
    keep(DOWN, "wait")
    for turn in (0, 1):
        ready(z, turn)
    for turn in (0, 1):
        column_block(0, turn)
    for turn in (0, 1):
        ready(peer, turn)
        column_block(1, turn)
    relay(DOWN, near)
    beside(DOWN, near, y, "start")
    for o in (0, 1):
        for turn in (0, 1):
            fold(o, turn)
    pour(near)
    for turn in (0, 1):
        ready(near, turn)
        column_block(2, turn)
    relay(DOWN, far)
    beside(DOWN, far, y, "start")
    ready(far, 0)
    column_block(3, 0)
    fold(2, 0)
    fold(2, 1)
    pour(far)
    for o in (0, 1):
        for turn in (0, 1):
            settle(o, turn)
    ready(far, 1)
    column_block(3, 1)
    fold(3, 0)
    fold(3, 1)
    for o in (2, 3):
        for turn in (0, 1):
            settle(o, turn)

    for half in (0, 1):
        last_copy(half).wait()
        result[token_rows(1 - core), half * sub:(half + 1) * sub] = last_recv[half]

    for which in range(5):
        z_sent(which, peer)
        z_sent(which, near)
        if which not in (IN, OUT):
            z_sent(which, far)
        else:
            @pl.when(inner)
            def _():
                for source in (near, far):
                    z_pass(which, source).wait_send()
        for source in (peer, near, far):
            across(which, source, "send")
        for source in order:
            for half in (0, 1) if which == DOWN else (None,):
                beside(which, source, half, "send", mine=False)
    for copy in (to_pair, to_x, to_x_later):
        copy.wait_send()
    for slot in range(4):
        x_copy(slot).wait_send()
    for quarter in (0, 1):
        for half in (0, 1):
            remote(pair_send.at[quarter, half], pair_recv.at[quarter, half],
                   p_send.at[quarter, half], p_recv.at[quarter, half], ZPEER).wait_send()


def pairs_fit(sizes, stream, in_weight, pool_weight, out_weight, gate_weight, down_weight):
    reps, fs, tp = sizes
    tokens, width = stream.shape
    return (reps == 2 and fs == 4 and tp == 4 and tokens % (2 * SEQ) == 0
            and width % (2 * LANES) == 0 and gate_weight.shape[1] % LANES == 0
            and in_weight.shape[1] % LANES == 0 and in_weight.shape[0] % 32 == 0
            and out_weight.shape[0] % 32 == 0 and gate_weight.shape[0] % 32 == 0
            and down_weight.shape[1] == width)


def pair_on_device(sizes, stream, in_weight, pool_weight, pool_scale, out_weight,
                   mix_gain, ffn_gain, gate_weight, up_weight, down_weight):
    if not pairs_fit(sizes, stream, in_weight, pool_weight, out_weight, gate_weight, down_weight):
        return ring_on_device(sizes, stream, in_weight, pool_weight, pool_scale, out_weight,
                              mix_gain, ffn_gain, gate_weight, up_weight, down_weight)
    reps, fs, tp = sizes
    tokens, width = stream.shape
    rows, sub = tokens // 2, width // 2
    features = width * tp
    channels = in_weight.shape[1]
    units = gate_weight.shape[1]
    bf, f32 = jnp.bfloat16, jnp.float32
    vmem = pl.BlockSpec(memory_space=pltpu.VMEM)
    hbm = pl.BlockSpec(memory_space=pl.ANY)
    dma = pltpu.SemaphoreType.DMA
    flops = 2 * tokens * (2 * features * channels + 3 * features * units)
    return pl.pallas_call(
        functools.partial(pair_kernel, sizes),
        out_shape=jax.ShapeDtypeStruct(stream.shape, bf),
        in_specs=[vmem] + [hbm] * 5 + [vmem] * 4,
        out_specs=vmem,
        scratch_shapes=[
            pltpu.VMEM((in_weight.shape[0] * fs, 2 * channels), bf),
            pltpu.VMEM((2 * out_weight.shape[0], out_weight.shape[1] * fs), bf),
            pltpu.VMEM((up_weight.shape[0] * fs, units), bf),
            pltpu.VMEM((gate_weight.shape[0] * fs, units), bf),
            pltpu.VMEM((units, down_weight.shape[1] * fs), bf),
            pltpu.VMEM((rows, features), bf),
            pltpu.VMEM((rows, features), bf),
            pltpu.VMEM((rows, 2 * channels), bf),
            pltpu.VMEM((2 * rows, units), bf),
            pltpu.VMEM((2 * rows, features), bf),
            pltpu.VMEM((2 * rows, features), bf),
            pltpu.VMEM(pool_weight.shape, bf),
            pltpu.VMEM((1, channels), bf),
            pltpu.VMEM((rows, 2 * width), f32),
            pltpu.VMEM((rows, 2 * width), bf),
            pltpu.VMEM((rows, 2 * width), bf),
            pltpu.VMEM((4, 2 * rows, sub), f32),
            pltpu.VMEM((4, 2 * rows, sub), bf),
            pltpu.VMEM((4, 2 * rows, sub), bf),
            pltpu.VMEM((2, 2, rows, sub), bf),
            pltpu.VMEM((2, 2, rows, sub), bf),
            pltpu.VMEM((2, rows, sub), bf),
            pltpu.VMEM((2, rows, sub), bf),
            dma((5, fs)), dma((5, fs)), dma((2, 2)), dma((5, fs)), dma((5, fs)),
            dma((5, fs, 2)), dma((5, fs, 2)), dma((5,)),
            dma((3,)), dma((3,)), dma((2,)), dma((2,)), dma((2,)), dma((3,)), dma((3,)),
            dma((4,)), dma((4,)), dma((2, 2)), dma((2, 2)), dma((2,)), dma((2,)),
        ],
        compiler_params=pltpu.CompilerParams(
            collective_id=0, has_side_effects=True, vmem_limit_bytes=64 * 1024 * 1024 - 65536),
        cost_estimate=pl.CostEstimate(flops=flops, bytes_accessed=flops // 512, transcendentals=0),
    )(stream, in_weight, out_weight, up_weight, gate_weight, down_weight, pool_weight,
      pool_scale.reshape(1, -1), mix_gain.reshape(1, -1), ffn_gain.reshape(1, -1))


def solution(mesh):
    sizes = tuple(mesh.shape[name] for name in ("rep", "fs", "tp"))
    return jax.shard_map(
        functools.partial(pair_on_device, sizes),
        mesh=mesh,
        in_specs=(
            P(("rep", "fs"), "tp"),
            P("fs", "tp"),
            P("tp", None, None),
            P("tp"),
            P("tp", "fs"),
            P(),
            P(),
            P("fs", "tp"),
            P("fs", "tp"),
            P("tp", "fs"),
        ),
        out_specs=P(("rep", "fs"), "tp"),
        check_vma=False,
    )
```

```python
import functools

import jax
import jax.numpy as jnp
from jax import lax
from jax.experimental import pallas as pl
from jax.experimental.pallas import tpu as pltpu
from jax.sharding import PartitionSpec as P

SEQ = 128
EPSILON = 1e-06
MESH = pl.DeviceIdType.MESH
BY_ROWS = (True, False, True, True, False)
PIECES = ((0, 0), (1, 0), (2, 0), (3, 0), (2, 1), (3, 1), (4, 0), (4, 1))
CHUNKS = (1, 1, 2, 2, 2)


def ring_kernel(sizes, stream, in_w, out_w, up_w, gate_w, down_w, pool_w, scale,
           mix_gain, ffn_gain, result,
           in_all, out_all, up_all, gate_all, down_all,
           rows_all, normed, group_out, hidden, middle, mid_all,
           mix_send, mix_recv, ffn_send, ffn_recv,
           ring_send, ring_recv, fwd_send, fwd_recv, own_sem,
           tp_send, tp_recv, keep_sem):
    reps, fs, tp = sizes
    half = fs // 2
    my_rep, me, my_tp = lax.axis_index("rep"), lax.axis_index("fs"), lax.axis_index("tp")
    own = (in_w, out_w, up_w, gate_w, down_w)
    full = (in_all, out_all, up_all, gate_all, down_all)
    tokens, width = stream.shape

    def turn(at, by, count):
        return lax.rem(at + by + count, count)

    def piece(which, owner, row, count):
        block_rows, block_cols = own[which].shape
        if BY_ROWS[which]:
            return full[which].at[pl.ds(pl.multiple_of(owner * block_rows + row, 16), count), :]
        return full[which].at[pl.ds(pl.multiple_of(row, 16), count),
                              pl.ds(pl.multiple_of(owner * block_cols, 128), block_cols)]

    def span(number, step, way):
        which, chunk = PIECES[number]
        rows = own[which].shape[0]
        cut = rows % (CHUNKS[which] * reps * 2 * 16) == 0
        count = rows // CHUNKS[which] if cut else (rows, 0)[chunk]
        row = chunk * (rows // CHUNKS[which])
        count = count // reps
        row = row + my_rep * count
        if step == half:
            count = count // 2
            row = row + way * count
        return which, row, count

    def empty(number):
        return span(number, 1, 0)[2] == 0

    def ring(number, step, way):
        which, row, count = span(number, step, way)
        sign = 1 - 2 * way
        owner = turn(me, -sign * (step - 1), fs)
        if step == 1:
            source = own[which].at[pl.ds(pl.multiple_of(row, 16), count), :]
        else:
            source = piece(which, owner, row, count)
        return pltpu.make_async_remote_copy(
            src_ref=source, dst_ref=piece(which, owner, row, count),
            send_sem=ring_send.at[number, step - 1, way],
            recv_sem=ring_recv.at[number, step - 1, way],
            device_id={"fs": turn(me, sign, fs)}, device_id_type=MESH)

    def forward(number, step, way, peer):
        which, row, count = span(number, step, way)
        block = piece(which, turn(me, -(1 - 2 * way) * step, fs), row, count)
        return pltpu.make_async_remote_copy(
            src_ref=block, dst_ref=block,
            send_sem=fwd_send.at[number, peer - 1, step - 1, way],
            recv_sem=fwd_recv.at[number, peer - 1, step - 1, way],
            device_id={"rep": turn(my_rep, peer, reps)}, device_id_type=MESH)

    def begin(*numbers):
        for number in numbers:
            if not empty(number):
                for way in (0, 1):
                    ring(number, 1, way).start()

    def advance(number, step):
        if empty(number):
            return
        for way in (0, 1):
            ring(number, step, way).wait_recv()
            if step < half:
                ring(number, step + 1, way).start()
            for peer in range(1, reps):
                forward(number, step, way, peer).start()

    def early(*numbers):
        for number in numbers:
            for step in range(1, half):
                advance(number, step)

    def late(*numbers):
        for number in numbers:
            advance(number, half)

    def arrived(*numbers):
        for number in numbers:
            if PIECES[number][1] == 0:
                keeps[PIECES[number][0]].wait()
            if empty(number):
                continue
            for step in range(1, half + 1):
                for way in (0, 1):
                    for peer in range(1, reps):
                        forward(number, step, way, peer).wait()

    def tp_copy(stage, offset, source, target):
        return pltpu.make_async_remote_copy(
            src_ref=source, dst_ref=target,
            send_sem=tp_send.at[stage, offset - 1], recv_sem=tp_recv.at[stage, offset - 1],
            device_id={"tp": turn(my_tp, offset, tp)}, device_id_type=MESH)

    def feature_cols(owner):
        return pl.ds(pl.multiple_of(owner * width, 128), width)

    barrier = pltpu.get_barrier_semaphore()
    greeted = 0
    for name, at, count, offsets in (
            ("fs", me, fs, (1, -1)),
            ("tp", my_tp, tp, range(1, tp)),
            ("rep", my_rep, reps, range(1, reps))):
        for offset in offsets:
            pl.semaphore_signal(barrier, inc=1, device_id={name: turn(at, offset, count)},
                                device_id_type=MESH)
            greeted += 1
    pl.semaphore_wait(barrier, greeted)

    begin(0, 1)
    stream_sends = []
    for offset in range(1, tp):
        copy = tp_copy(0, offset, stream, rows_all.at[:, feature_cols(my_tp)])
        copy.start()
        stream_sends.append(copy)
    keeps = []
    for which in range(len(own)):
        keep = pltpu.make_async_copy(
            own[which], piece(which, me, 0, own[which].shape[0]), own_sem.at[which])
        keep.start()
        keeps.append(keep)
    keep_stream = pltpu.make_async_copy(
        stream, rows_all.at[:, feature_cols(my_tp)], keep_sem)
    keep_stream.start()
    early(0, 1)
    begin(2, 3, 4)
    late(0, 1)

    def norm_into(source, gain, target):
        tile = 64

        def body(i, carry):
            at = pl.ds(pl.multiple_of(i * tile, tile), tile)
            wide = source[at, :].astype(jnp.float32)
            mean = jnp.mean(wide * wide, axis=-1, keepdims=True)
            target[at, :] = (wide * lax.rsqrt(mean + EPSILON)
                             * gain[...].astype(jnp.float32)).astype(jnp.bfloat16)
            return carry

        lax.fori_loop(0, tokens // tile, body, 0)

    keep_stream.wait()
    for copy in stream_sends:
        copy.wait()
    norm_into(rows_all, mix_gain, normed)
    arrived(0)

    local_groups, group_dim = pool_w.shape[0], pool_w.shape[1]
    at_row = lax.broadcasted_iota(jnp.int32, (SEQ, SEQ), 0)
    at_col = lax.broadcasted_iota(jnp.int32, (SEQ, SEQ), 1)
    insides, inverses = [], []
    for g in range(local_groups):
        group = my_tp * local_groups + g
        level = lax.div(4 * group, local_groups * tp)
        reach = jnp.int32(2)
        for bit in range(1, 4):
            reach = jnp.where(level >= bit, jnp.int32(2 << bit), reach)
        inside = (at_col <= at_row) & (at_col > at_row - reach)
        insides.append(jnp.where(inside, 1.0, 0.0).astype(jnp.bfloat16))
        inverses.append(jnp.minimum(at_row + 1, reach).astype(jnp.float32)[:, :1])

    def mix(i, carry):
        at = pl.ds(pl.multiple_of(i * SEQ, SEQ), SEQ)
        pooled = jnp.dot(normed[at, :], in_all[...],
                         preferred_element_type=jnp.float32).astype(jnp.bfloat16)
        for g in range(local_groups):
            cols = slice(g * group_dim, (g + 1) * group_dim)
            part = pooled[:, cols]
            sums = jnp.dot(insides[g], part, preferred_element_type=jnp.float32)
            contrast = (sums / inverses[g] - part.astype(jnp.float32)).astype(jnp.bfloat16)
            mixed = jnp.dot(contrast, pool_w[g], preferred_element_type=jnp.float32)
            group_out[at, cols] = (mixed * scale[:, cols].astype(jnp.float32)).astype(jnp.bfloat16)
        return carry

    lax.fori_loop(0, tokens // SEQ, mix, 0)

    arrived(1)
    early(2)

    def spread(operand, weights, stage, sends, tile):
        def block(owner, target):
            def body(i, carry):
                at = pl.ds(pl.multiple_of(i * tile, tile), tile)
                target[at, :] = jnp.dot(operand[at, :], weights[:, feature_cols(owner)],
                                        preferred_element_type=jnp.float32).astype(jnp.bfloat16)
                return carry
            lax.fori_loop(0, tokens // tile, body, 0)

        copies = []
        recv = mix_recv if stage == 1 else ffn_recv
        for offset in sorted(range(1, tp), key=lambda o: -min(o, tp - o)):
            block(turn(my_tp, offset, tp), sends.at[offset - 1])
            copy = tp_copy(stage, offset, sends.at[offset - 1], recv.at[offset - 1])
            copy.start()
            copies.append(copy)
        block(my_tp, sends.at[tp - 1])
        return copies

    def gather_sum(base, recv, sends, target):
        tile = 64

        def body(i, carry):
            at = pl.ds(pl.multiple_of(i * tile, tile), tile)
            total = sends[tp - 1, at, :].astype(jnp.float32)
            for k in range(tp - 1):
                total = total + recv[k, at, :].astype(jnp.float32)
            target[at, :] = (base[at, :].astype(jnp.float32) + total).astype(jnp.bfloat16)
            return carry

        lax.fori_loop(0, tokens // tile, body, 0)

    mix_copies = spread(group_out, out_all, 1, mix_send, tokens // 2)
    early(3)
    begin(5)
    for copy in mix_copies:
        copy.wait()
    gather_sum(stream, mix_recv, mix_send, middle)
    keep_middle = pltpu.make_async_copy(middle, mid_all.at[:, feature_cols(my_tp)], keep_sem)
    keep_middle.start()
    middle_copies = []
    for offset in range(1, tp):
        copy = tp_copy(2, offset, middle, mid_all.at[:, feature_cols(my_tp)])
        copy.start()
        middle_copies.append(copy)
    early(4)
    begin(6, 7)
    late(2, 3)
    keep_middle.wait()
    for copy in middle_copies:
        copy.wait()
    norm_into(mid_all, ffn_gain, normed)
    early(5)
    late(4)
    early(6)
    late(5)
    early(7)
    late(6)
    arrived(2, 3, 4, 5)
    tile = tokens // 2

    def gated(i, carry):
        at = pl.ds(pl.multiple_of(i * tile, tile), tile)
        values = normed[at, :]
        gate = jnp.dot(values, gate_all[...], preferred_element_type=jnp.float32)
        up = jnp.dot(values, up_all[...], preferred_element_type=jnp.float32)
        hidden[at, :] = (gate / (1.0 + jnp.exp(-gate)) * up).astype(jnp.bfloat16)
        return carry

    lax.fori_loop(0, tokens // tile, gated, 0)
    late(7)
    arrived(6, 7)
    ffn_copies = spread(hidden, down_all, 3, ffn_send, tokens // 2)
    for number in range(len(PIECES)):
        if not empty(number):
            for step in range(1, half + 1):
                for way in (0, 1):
                    ring(number, step, way).wait_send()
    for copy in ffn_copies:
        copy.wait()
    gather_sum(middle, ffn_recv, ffn_send, result)


def ring_on_device(sizes, stream, in_weight, pool_weight, pool_scale, out_weight,
              mix_gain, ffn_gain, gate_weight, up_weight, down_weight):
    reps, fs, tp = sizes
    half = fs // 2
    tokens, width = stream.shape
    features = width * tp
    own = (in_weight, out_weight, up_weight, gate_weight, down_weight)
    full = [pltpu.VMEM((w.shape[0] * fs, w.shape[1]) if by_rows else (w.shape[0], w.shape[1] * fs),
                       jnp.bfloat16) for w, by_rows in zip(own, BY_ROWS)]
    units = gate_weight.shape[1]
    bf = jnp.bfloat16
    vmem = pl.BlockSpec(memory_space=pltpu.VMEM)
    hbm = pl.BlockSpec(memory_space=pl.ANY)
    dma = pltpu.SemaphoreType.DMA
    flops = 2 * tokens * (2 * features * in_weight.shape[1] + 3 * features * units)
    return pl.pallas_call(
        functools.partial(ring_kernel, sizes),
        out_shape=jax.ShapeDtypeStruct(stream.shape, bf),
        in_specs=[vmem] + [hbm] * 5 + [vmem] * 4,
        out_specs=vmem,
        scratch_shapes=full + [
            pltpu.VMEM((tokens, features), bf),
            pltpu.VMEM((tokens, features), bf),
            pltpu.VMEM((tokens, in_weight.shape[1]), bf),
            pltpu.VMEM((tokens, units), bf),
            pltpu.VMEM((tokens, width), bf),
            pltpu.VMEM((tokens, features), bf),
            pltpu.VMEM((tp, tokens, width), bf),
            pltpu.VMEM((tp - 1, tokens, width), bf),
            pltpu.VMEM((tp, tokens, width), bf),
            pltpu.VMEM((tp - 1, tokens, width), bf),
            dma((len(PIECES), half, 2)),
            dma((len(PIECES), half, 2)),
            dma((len(PIECES), max(reps - 1, 1), half, 2)),
            dma((len(PIECES), max(reps - 1, 1), half, 2)),
            dma((len(own),)),
            dma((4, tp - 1)),
            dma((4, tp - 1)),
            dma(()),
        ],
        compiler_params=pltpu.CompilerParams(
            collective_id=0, has_side_effects=True, vmem_limit_bytes=64 * 1024 * 1024 - 65536),
        cost_estimate=pl.CostEstimate(flops=flops, bytes_accessed=flops // 512, transcendentals=0),
    )(stream, in_weight, out_weight, up_weight, gate_weight, down_weight, pool_weight,
      pool_scale.reshape(1, -1), mix_gain.reshape(1, -1), ffn_gain.reshape(1, -1))


IN, OUT, UP, GATE, DOWN = range(5)
LANES = 128


def pair_kernel(sizes, stream, in_w, out_w, up_w, gate_w, down_w, pool_w, scale,
                mix_gain, ffn_gain, result,
                in_all, out_all, up_all, gate_all, down_all,
                rows_all, normed, group_out, hidden, gate_acts, mid_all, normed_ffn,
                pool_sib, scale_sib,
                mix_own, mix_send, mix_recv, ffn_own, ffn_send, ffn_recv, pair_send, pair_recv,
                last_send, last_recv,
                z_send, z_recv, pass_send, y_send, y_recv, d_send, d_recv, own_sem,
                in_send, in_recv, pool_send, pool_recv, mix_sems, mid_send, mid_recv,
                x_send, x_recv, p_send, p_recv, l_send, l_recv):
    reps, fs, tp = sizes
    y, z, lane_id = lax.axis_index("rep"), lax.axis_index("fs"), lax.axis_index("tp")
    x, core = lax.div(lane_id, 2), lax.rem(lane_id, 2)
    own = (in_w, out_w, up_w, gate_w, down_w)
    full = (in_all, out_all, up_all, gate_all, down_all)
    tokens, width = stream.shape
    rows = tokens // 2
    wide = 2 * width
    seat, pair = lax.rem(z, 2), lax.div(z, 2)
    peer = z + 1 - 2 * seat
    near = jnp.where(pair == 0, 2, 1)
    far = jnp.where(pair == 0, 3, 0)
    inner = (z == 1) | (z == 2)
    f32, bf16 = jnp.float32, jnp.bfloat16

    blocks = gate_w.shape[1] // LANES
    few, many = blocks // 2, blocks - blocks // 2

    SIB = {"tp": lane_id + 1 - 2 * core}
    XPEER = {"tp": lane_id + 2 - 4 * x}
    XSIB = {"tp": 2 * (1 - x) + 1 - core}
    YPEER = {"rep": 1 - y}
    ZPEER = {"fs": peer}

    def at_least(value, multiple):
        return pl.multiple_of(value, multiple)

    def remote(source, target, send, recv, device):
        return pltpu.make_async_remote_copy(
            src_ref=source, dst_ref=target, send_sem=send, recv_sem=recv,
            device_id=device, device_id_type=MESH)

    def sized(which, core_at, seat_at, act):
        if which in (IN, OUT) or few == many:
            act(many)
            return
        big = core_at == seat_at

        @pl.when(big)
        def _():
            act(many)

        @pl.when(jnp.logical_not(big))
        def _():
            act(few)

    def place(which, source, half, core_at, seat_at, count):
        block_rows, block_cols = own[which].shape
        ref = full[which]
        if which == IN:
            part = block_rows // 2
            row, size = (source * block_rows, block_rows) if half is None else (
                source * block_rows + half * part, part)
            return ref.at[pl.ds(at_least(row, 16), size),
                          pl.ds(at_least(core_at * block_cols, LANES), block_cols)]
        if which == OUT:
            part = block_rows // 2
            row, size = (core_at * block_rows, block_rows) if half is None else (
                core_at * block_rows + half * part, part)
            return ref.at[pl.ds(at_least(row, 16), size),
                          pl.ds(at_least(source * block_cols, LANES), block_cols)]
        first = core_at * jnp.where(seat_at == 0, many, few) * LANES
        if which == DOWN:
            part = block_cols // 2
            col, size = (source * block_cols, block_cols) if half is None else (
                source * block_cols + half * part, part)
            return ref.at[pl.ds(at_least(first, LANES), count * LANES),
                          pl.ds(at_least(col, LANES), size)]
        part = block_rows // 2
        row, size = (source * block_rows, block_rows) if half is None else (
            source * block_rows + half * part, part)
        return ref.at[pl.ds(at_least(row, 16), size),
                      pl.ds(at_least(first, LANES), count * LANES)]

    def held(which, half, seat_at, count):
        block_rows, block_cols = own[which].shape
        ref = own[which]
        if which in (IN, OUT):
            if half is None:
                return ref
            part = block_rows // 2
            return ref.at[pl.ds(at_least(half * part, 16), part), :]
        first = seat_at * jnp.where(core == 0, many, few) * LANES
        if which == DOWN:
            part = block_cols // 2
            unit_rows = pl.ds(at_least(first, LANES), count * LANES)
            if half is None:
                return ref.at[unit_rows, :]
            return ref.at[unit_rows, pl.ds(at_least(half * part, LANES), part)]
        part = block_rows // 2
        unit_cols = pl.ds(at_least(first, LANES), count * LANES)
        if half is None:
            return ref.at[:, unit_cols]
        return ref.at[pl.ds(at_least(half * part, 16), part), unit_cols]

    def z_start(which, dest):
        to = lax.rem(dest, 2)
        sized(which, core, to, lambda n: remote(
            held(which, y, to, n), place(which, z, y, core, to, n),
            z_send.at[which, dest], z_recv.at[which, z], {"fs": dest}).start())

    def z_sent(which, dest):
        to = lax.rem(dest, 2)
        sized(which, core, to, lambda n: remote(
            held(which, y, to, n), place(which, z, y, core, to, n),
            z_send.at[which, dest], z_recv.at[which, z], {"fs": dest}).wait_send())

    def z_pass(which, source):
        block = place(which, source, y, core, seat, many)
        return remote(block, block, pass_send.at[which, lax.rem(source, 2)],
                      z_recv.at[which, source], ZPEER)

    def arrived(which, source):
        def act(n):
            block = place(which, source, y, core, seat, n)
            remote(block, block, y_send.at[which, source], z_recv.at[which, source],
                   YPEER).wait_recv()
        sized(which, core, seat, act)

    def across(which, source, step):
        def act(n):
            half = 1 - y if step == "recv" else y
            block = place(which, source, half, core, seat, n)
            copy = remote(block, block, y_send.at[which, source], y_recv.at[which, source], YPEER)
            {"start": copy.start, "recv": copy.wait_recv, "send": copy.wait_send}[step]()
        sized(which, core, seat, act)

    def beside(which, source, half, step, mine=False):
        slot = 0 if half is None else half
        whose = 1 - core if step == "recv" else core

        def act(n):
            block = place(which, source, half, whose, seat, n)
            start = held(which, half, seat, n) if mine else block
            copy = remote(start, block, d_send.at[which, source, slot],
                          d_recv.at[which, source, slot], SIB)
            {"start": copy.start, "recv": copy.wait_recv, "send": copy.wait_send}[step]()
        sized(which, whose, seat, act)

    def keep(which, step):
        def act(n):
            copy = pltpu.make_async_copy(held(which, None, seat, n),
                                         place(which, z, None, core, seat, n), own_sem.at[which])
            {"start": copy.start, "wait": copy.wait}[step]()
        sized(which, core, seat, act)

    def relay(which, source):
        arrived(which, source)
        across(which, source, "start")

    def share(which, source):
        across(which, source, "recv")
        beside(which, source, None, "start")

    def feature_cols(owner):
        return pl.ds(at_least(owner * width, LANES), width)

    def token_rows(half):
        return pl.ds(at_least(half * rows, 16), rows)

    def stream_copy(number, device, half):
        return remote(stream.at[token_rows(half), :], rows_all.at[:, feature_cols(lane_id)],
                      in_send.at[number], in_recv.at[number], device)

    barrier = pltpu.get_barrier_semaphore()
    greeted = 0
    for device in (SIB, XPEER, XSIB, YPEER, ZPEER, {"fs": near}, {"fs": far}):
        pl.semaphore_signal(barrier, inc=1, device_id=device, device_id_type=MESH)
        greeted += 1
    pl.semaphore_wait(barrier, greeted)

    outer = jnp.logical_not(inner)
    z_start(IN, near)
    z_start(IN, peer)
    stream_copies = [stream_copy(0, XPEER, core), stream_copy(1, XSIB, 1 - core),
                     stream_copy(2, SIB, 1 - core)]
    for copy in stream_copies:
        copy.start()
    z_start(OUT, near)
    z_start(OUT, peer)
    keep(IN, "start")
    beside(IN, z, None, "start", mine=True)
    pool_copy = remote(pool_w, pool_sib, pool_send.at[0], pool_recv.at[0], SIB)
    scale_copy = remote(scale, scale_sib, pool_send.at[1], pool_recv.at[1], SIB)
    pool_copy.start()
    scale_copy.start()

    @pl.when(inner)
    def _():
        z_start(GATE, near)
        z_start(GATE, far)
        z_start(UP, near)

    @pl.when(outer)
    def _():
        z_start(GATE, peer)
        z_start(GATE, far)
        z_start(UP, far)
        z_start(UP, peer)

    for which in (OUT, GATE, UP, DOWN):
        keep(which, "start")
        for half in (0, 1) if which == DOWN else (None,):
            beside(which, z, half, "start", mine=True)

    rows_all[:, feature_cols(lane_id)] = stream[token_rows(core), :]

    def take(which):
        relay(which, peer)
        for source in (near, far):
            arrived(which, source)

            @pl.when(inner)
            def _():
                z_pass(which, source).start()
            across(which, source, "start")

    take(IN)

    @pl.when(inner)
    def _():
        take(OUT)

    def norm_into(source, gain, target, first, count):
        tile = 64

        def body(i, carry):
            at = pl.ds(at_least(first + i * tile, tile), tile)
            values = source[at, :].astype(f32)
            mean = jnp.mean(values * values, axis=-1, keepdims=True)
            target[at, :] = (values * lax.rsqrt(mean + EPSILON)
                             * gain[...].astype(f32)).astype(bf16)
            return carry

        lax.fori_loop(0, count // tile, body, 0)

    for copy in stream_copies:
        copy.wait()
    norm_into(rows_all, mix_gain, normed, 0, rows)
    for source in (peer, near, far):
        share(IN, source)

    @pl.when(outer)
    def _():
        take(OUT)

    pool_copy.wait()
    scale_copy.wait()
    for source in (z, peer, near, far):
        beside(IN, source, None, "recv")
    keep(IN, "wait")

    local_groups, group_dim = pool_w.shape[0], pool_w.shape[1]
    at_row = lax.broadcasted_iota(jnp.int32, (SEQ, SEQ), 0)
    at_col = lax.broadcasted_iota(jnp.int32, (SEQ, SEQ), 1)
    pooled = jnp.dot(normed[...], in_all[...], preferred_element_type=f32).astype(bf16)
    for g in range(2 * local_groups):
        owner, place_in = divmod(g, local_groups)
        group = x * 2 * local_groups + g
        level = lax.div(4 * group, local_groups * tp)
        reach = jnp.int32(2)
        for bit in range(1, 4):
            reach = jnp.where(level >= bit, jnp.int32(2 << bit), reach)
        inside = jnp.where((at_col <= at_row) & (at_col > at_row - reach), 1.0, 0.0).astype(bf16)
        counts = jnp.minimum(at_row + 1, reach).astype(f32)[:, :1]
        is_own = core == owner
        cols = slice(g * group_dim, (g + 1) * group_dim)
        own_cols = slice(place_in * group_dim, (place_in + 1) * group_dim)
        weight = jnp.where(is_own, pool_w[place_in], pool_sib[place_in])
        factor = jnp.where(is_own, scale[:, own_cols].astype(f32),
                           scale_sib[:, own_cols].astype(f32))
        for s in range(rows // SEQ):
            at = slice(s * SEQ, (s + 1) * SEQ)
            part = pooled[at, cols]
            sums = jnp.dot(inside, part, preferred_element_type=f32)
            contrast = (sums / counts - part.astype(f32)).astype(bf16)
            mixed = jnp.dot(contrast, weight, preferred_element_type=f32)
            group_out[at, cols] = (mixed * factor).astype(bf16)

    for source in (peer, near, far):
        share(OUT, source)
    for source in (z, peer, near, far):
        beside(OUT, source, None, "recv")
    keep(OUT, "wait")

    def half_cols(owner):
        return pl.ds(at_least(owner * wide, LANES), wide)

    mix_send[...] = jnp.dot(group_out[...], out_all[:, half_cols(1 - x)],
                            preferred_element_type=f32).astype(bf16)
    mix_copy = remote(mix_send, mix_recv, mix_sems.at[0], mix_sems.at[1], XPEER)
    mix_copy.start()
    mix_own[...] = jnp.dot(group_out[...], out_all[:, half_cols(x)], preferred_element_type=f32)

    @pl.when(inner)
    def _():
        relay(GATE, peer)
        relay(GATE, near)

    @pl.when(outer)
    def _():
        relay(GATE, far)

    mix_copy.wait()
    mid_rows = pl.ds(at_least(seat * rows, 16), rows)
    mid_all[mid_rows, half_cols(x)] = (
        rows_all[:, half_cols(x)].astype(f32) + (mix_own[...] + mix_recv[...].astype(f32))).astype(bf16)

    def mid_copy(number, block, device):
        view = mid_all.at[pl.ds(at_least(block * rows, 16), rows), half_cols(x)]
        return remote(view, view, mid_send.at[number], mid_recv.at[number], device)

    to_pair, to_x, to_x_later = mid_copy(0, seat, ZPEER), mid_copy(1, seat, XPEER), mid_copy(2, 1 - seat, XPEER)
    to_pair.start()
    to_x.start()

    @pl.when(inner)
    def _():
        z_start(GATE, peer)
        z_start(UP, peer)
        z_start(UP, far)
        share(GATE, peer)
        share(GATE, near)
        relay(UP, peer)

    @pl.when(outer)
    def _():
        z_start(GATE, near)
        z_start(UP, near)
        share(GATE, far)
        relay(UP, far)
        relay(GATE, near)

    to_pair.wait_recv()
    to_x_later.start()

    @pl.when(inner)
    def _():
        z_start(DOWN, far)
        z_start(DOWN, near)
        z_start(DOWN, peer)
        share(UP, peer)
        relay(UP, near)

    @pl.when(outer)
    def _():
        z_start(DOWN, peer)
        z_start(DOWN, near)
        z_start(DOWN, far)
        share(UP, far)

    to_x.wait_recv()
    norm_into(mid_all, ffn_gain, normed_ffn, seat * rows, rows)

    @pl.when(inner)
    def _():
        relay(GATE, far)
        share(UP, near)

    @pl.when(outer)
    def _():
        share(GATE, near)
        relay(GATE, peer)

    to_x_later.wait_recv()
    norm_into(mid_all, ffn_gain, normed_ffn, (1 - seat) * rows, rows)

    @pl.when(inner)
    def _():
        relay(UP, far)
        share(GATE, far)

    @pl.when(outer)
    def _():
        relay(UP, peer)
        share(GATE, peer)

    for source in (z, peer, near, far):
        beside(GATE, source, None, "recv")
    keep(GATE, "wait")

    tile = rows

    def gated(i, carry):
        at = pl.ds(at_least(i * tile, tile), tile)
        gate = jnp.dot(normed_ffn[at, :], gate_all[...], preferred_element_type=f32)
        gate_acts[at, :] = gate / (1.0 + jnp.exp(-gate))
        return carry

    lax.fori_loop(0, 2 * rows // tile, gated, 0)

    @pl.when(inner)
    def _():
        share(UP, far)

    @pl.when(outer)
    def _():
        share(UP, peer)
        relay(UP, near)
        share(UP, near)

    for source in (z, peer, near, far):
        beside(UP, source, None, "recv")
    keep(UP, "wait")

    def raised(i, carry):
        at = pl.ds(at_least(i * tile, tile), tile)
        up = jnp.dot(normed_ffn[at, :], up_all[...], preferred_element_type=f32)
        hidden[at, :] = (gate_acts[at, :] * up).astype(bf16)
        return carry

    lax.fori_loop(0, 2 * rows // tile, raised, 0)

    sub = width // 2
    order = (z, peer, far, near)
    keeps_early = x == pair

    def is_kept(o):
        return keeps_early if o < 2 else jnp.logical_not(keeps_early)

    def half_of(turn):
        return y if turn == 0 else 1 - y

    def column_block(o, turn):
        at = pl.ds(at_least(order[o] * width + half_of(turn) * sub, LANES), sub)
        slot = 2 * (o % 2) + turn
        values = jnp.dot(hidden[...], down_all[:, at], preferred_element_type=f32)

        @pl.when(is_kept(o))
        def _():
            ffn_own[slot] = values

        @pl.when(jnp.logical_not(is_kept(o)))
        def _():
            ffn_send[slot] = values.astype(bf16)
            x_copy(slot).start()

    def x_copy(slot):
        return remote(ffn_send.at[slot], ffn_recv.at[slot], x_send.at[slot], x_recv.at[slot], XPEER)

    def pair_copy(o, turn):
        quarter, half = lax.rem(order[o], 2), half_of(turn)
        return remote(pair_send.at[quarter, half], pair_recv.at[quarter, half],
                      p_send.at[quarter, half], p_recv.at[quarter, half], ZPEER)

    def fold(o, turn):
        slot = 2 * (o % 2) + turn
        quarter, half = lax.rem(order[o], 2), half_of(turn)

        @pl.when(is_kept(o))
        def _():
            x_copy(slot).wait_recv()
            theirs = pl.ds(at_least((1 - seat) * rows, 16), rows)
            pair_send[quarter, half] = (ffn_own[slot, theirs, :]
                                        + ffn_recv[slot, theirs, :].astype(f32)).astype(bf16)
            pair_copy(o, turn).start()

    def last_copy(half):
        return remote(last_send.at[half], last_recv.at[half], l_send.at[half], l_recv.at[half], SIB)

    def settle(o, turn):
        slot = 2 * (o % 2) + turn
        quarter, half = lax.rem(order[o], 2), half_of(turn)

        @pl.when(is_kept(o))
        def _():
            pair_copy(o, turn).wait_recv()
            ours = pl.ds(at_least(seat * rows, 16), rows)
            cols = pl.ds(at_least(order[o] * width + half * sub, LANES), sub)
            total = (ffn_own[slot, ours, :] + ffn_recv[slot, ours, :].astype(f32)
                     + pair_recv[quarter, half].astype(f32))
            value = (mid_all[ours, cols].astype(f32) + total).astype(bf16)

            @pl.when(quarter == core)
            def _():
                result[token_rows(core), pl.ds(at_least(half * sub, LANES), sub)] = value

            @pl.when(quarter != core)
            def _():
                last_send[half] = value
                last_copy(half).start()

    def pour(source):
        across(DOWN, source, "recv")
        beside(DOWN, source, 1 - y, "start")

    def ready(source, turn):
        beside(DOWN, source, half_of(turn), "recv")

    def bring(source):
        relay(DOWN, source)
        beside(DOWN, source, y, "start")

    def block(o, turn):
        ready(order[o], turn)
        column_block(o, turn)

    keep(DOWN, "wait")
    block(0, 0)
    block(0, 1)
    bring(peer)
    block(1, 0)
    pour(peer)
    block(1, 1)
    bring(far)
    fold(0, 0)
    block(2, 0)
    pour(far)
    block(2, 1)
    fold(0, 1)
    bring(near)
    fold(1, 0)
    block(3, 0)
    pour(near)
    fold(2, 0)
    fold(1, 1)
    fold(2, 1)
    block(3, 1)
    fold(3, 0)
    for o in (0, 1):
        for turn in (0, 1):
            settle(o, turn)
    fold(3, 1)
    for o in (2, 3):
        for turn in (0, 1):
            settle(o, turn)

    for half in (0, 1):
        last_copy(half).wait()
        result[token_rows(1 - core), half * sub:(half + 1) * sub] = last_recv[half]

    for which in range(5):
        z_sent(which, peer)
        z_sent(which, near)
        if which not in (IN, OUT):
            z_sent(which, far)
        else:
            @pl.when(inner)
            def _():
                for source in (near, far):
                    z_pass(which, source).wait_send()
        for source in (peer, near, far):
            across(which, source, "send")
        for source in order:
            for half in (0, 1) if which == DOWN else (None,):
                beside(which, source, half, "send", mine=False)
    for copy in (to_pair, to_x, to_x_later):
        copy.wait_send()
    for slot in range(4):
        x_copy(slot).wait_send()
    for quarter in (0, 1):
        for half in (0, 1):
            remote(pair_send.at[quarter, half], pair_recv.at[quarter, half],
                   p_send.at[quarter, half], p_recv.at[quarter, half], ZPEER).wait_send()


def pairs_fit(sizes, stream, in_weight, pool_weight, out_weight, gate_weight, down_weight):
    reps, fs, tp = sizes
    tokens, width = stream.shape
    return (reps == 2 and fs == 4 and tp == 4 and tokens % (2 * SEQ) == 0
            and width % (2 * LANES) == 0 and gate_weight.shape[1] % LANES == 0
            and in_weight.shape[1] % LANES == 0 and in_weight.shape[0] % 32 == 0
            and out_weight.shape[0] % 32 == 0 and gate_weight.shape[0] % 32 == 0
            and down_weight.shape[1] == width)


def pair_on_device(sizes, stream, in_weight, pool_weight, pool_scale, out_weight,
                   mix_gain, ffn_gain, gate_weight, up_weight, down_weight):
    if not pairs_fit(sizes, stream, in_weight, pool_weight, out_weight, gate_weight, down_weight):
        return ring_on_device(sizes, stream, in_weight, pool_weight, pool_scale, out_weight,
                              mix_gain, ffn_gain, gate_weight, up_weight, down_weight)
    reps, fs, tp = sizes
    tokens, width = stream.shape
    rows, sub = tokens // 2, width // 2
    features = width * tp
    channels = in_weight.shape[1]
    units = gate_weight.shape[1]
    bf, f32 = jnp.bfloat16, jnp.float32
    vmem = pl.BlockSpec(memory_space=pltpu.VMEM)
    hbm = pl.BlockSpec(memory_space=pl.ANY)
    dma = pltpu.SemaphoreType.DMA
    flops = 2 * tokens * (2 * features * channels + 3 * features * units)
    return pl.pallas_call(
        functools.partial(pair_kernel, sizes),
        out_shape=jax.ShapeDtypeStruct(stream.shape, bf),
        in_specs=[vmem] + [hbm] * 5 + [vmem] * 4,
        out_specs=vmem,
        scratch_shapes=[
            pltpu.VMEM((in_weight.shape[0] * fs, 2 * channels), bf),
            pltpu.VMEM((2 * out_weight.shape[0], out_weight.shape[1] * fs), bf),
            pltpu.VMEM((up_weight.shape[0] * fs, units), bf),
            pltpu.VMEM((gate_weight.shape[0] * fs, units), bf),
            pltpu.VMEM((units, down_weight.shape[1] * fs), bf),
            pltpu.VMEM((rows, features), bf),
            pltpu.VMEM((rows, features), bf),
            pltpu.VMEM((rows, 2 * channels), bf),
            pltpu.VMEM((2 * rows, units), bf),
            pltpu.VMEM((2 * rows, units), f32),
            pltpu.VMEM((2 * rows, features), bf),
            pltpu.VMEM((2 * rows, features), bf),
            pltpu.VMEM(pool_weight.shape, bf),
            pltpu.VMEM((1, channels), bf),
            pltpu.VMEM((rows, 2 * width), f32),
            pltpu.VMEM((rows, 2 * width), bf),
            pltpu.VMEM((rows, 2 * width), bf),
            pltpu.VMEM((4, 2 * rows, sub), f32),
            pltpu.VMEM((4, 2 * rows, sub), bf),
            pltpu.VMEM((4, 2 * rows, sub), bf),
            pltpu.VMEM((2, 2, rows, sub), bf),
            pltpu.VMEM((2, 2, rows, sub), bf),
            pltpu.VMEM((2, rows, sub), bf),
            pltpu.VMEM((2, rows, sub), bf),
            dma((5, fs)), dma((5, fs)), dma((2, 2)), dma((5, fs)), dma((5, fs)),
            dma((5, fs, 2)), dma((5, fs, 2)), dma((5,)),
            dma((3,)), dma((3,)), dma((2,)), dma((2,)), dma((2,)), dma((3,)), dma((3,)),
            dma((4,)), dma((4,)), dma((2, 2)), dma((2, 2)), dma((2,)), dma((2,)),
        ],
        compiler_params=pltpu.CompilerParams(
            collective_id=0, has_side_effects=True, vmem_limit_bytes=64 * 1024 * 1024 - 65536),
        cost_estimate=pl.CostEstimate(flops=flops, bytes_accessed=flops // 512, transcendentals=0),
    )(stream, in_weight, out_weight, up_weight, gate_weight, down_weight, pool_weight,
      pool_scale.reshape(1, -1), mix_gain.reshape(1, -1), ffn_gain.reshape(1, -1))


def solution(mesh):
    sizes = tuple(mesh.shape[name] for name in ("rep", "fs", "tp"))
    return jax.shard_map(
        functools.partial(pair_on_device, sizes),
        mesh=mesh,
        in_specs=(
            P(("rep", "fs"), "tp"),
            P("fs", "tp"),
            P("tp", None, None),
            P("tp"),
            P("tp", "fs"),
            P(),
            P(),
            P("fs", "tp"),
            P("fs", "tp"),
            P("tp", "fs"),
        ),
        out_specs=P(("rep", "fs"), "tp"),
        check_vma=False,
    )
```

```python
import functools

import jax
import jax.numpy as jnp
from jax import lax
from jax.experimental import pallas as pl
from jax.experimental.pallas import tpu as pltpu
from jax.sharding import PartitionSpec as P

SEQ = 128
EPSILON = 1e-06
MESH = pl.DeviceIdType.MESH
BY_ROWS = (True, False, True, True, False)
PIECES = ((0, 0), (1, 0), (2, 0), (3, 0), (2, 1), (3, 1), (4, 0), (4, 1))
CHUNKS = (1, 1, 2, 2, 2)


def ring_kernel(sizes, stream, in_w, out_w, up_w, gate_w, down_w, pool_w, scale,
           mix_gain, ffn_gain, result,
           in_all, out_all, up_all, gate_all, down_all,
           rows_all, normed, group_out, hidden, middle, mid_all,
           mix_send, mix_recv, ffn_send, ffn_recv,
           ring_send, ring_recv, fwd_send, fwd_recv, own_sem,
           tp_send, tp_recv, keep_sem):
    reps, fs, tp = sizes
    half = fs // 2
    my_rep, me, my_tp = lax.axis_index("rep"), lax.axis_index("fs"), lax.axis_index("tp")
    own = (in_w, out_w, up_w, gate_w, down_w)
    full = (in_all, out_all, up_all, gate_all, down_all)
    tokens, width = stream.shape

    def turn(at, by, count):
        return lax.rem(at + by + count, count)

    def piece(which, owner, row, count):
        block_rows, block_cols = own[which].shape
        if BY_ROWS[which]:
            return full[which].at[pl.ds(pl.multiple_of(owner * block_rows + row, 16), count), :]
        return full[which].at[pl.ds(pl.multiple_of(row, 16), count),
                              pl.ds(pl.multiple_of(owner * block_cols, 128), block_cols)]

    def span(number, step, way):
        which, chunk = PIECES[number]
        rows = own[which].shape[0]
        cut = rows % (CHUNKS[which] * reps * 2 * 16) == 0
        count = rows // CHUNKS[which] if cut else (rows, 0)[chunk]
        row = chunk * (rows // CHUNKS[which])
        count = count // reps
        row = row + my_rep * count
        if step == half:
            count = count // 2
            row = row + way * count
        return which, row, count

    def empty(number):
        return span(number, 1, 0)[2] == 0

    def ring(number, step, way):
        which, row, count = span(number, step, way)
        sign = 1 - 2 * way
        owner = turn(me, -sign * (step - 1), fs)
        if step == 1:
            source = own[which].at[pl.ds(pl.multiple_of(row, 16), count), :]
        else:
            source = piece(which, owner, row, count)
        return pltpu.make_async_remote_copy(
            src_ref=source, dst_ref=piece(which, owner, row, count),
            send_sem=ring_send.at[number, step - 1, way],
            recv_sem=ring_recv.at[number, step - 1, way],
            device_id={"fs": turn(me, sign, fs)}, device_id_type=MESH)

    def forward(number, step, way, peer):
        which, row, count = span(number, step, way)
        block = piece(which, turn(me, -(1 - 2 * way) * step, fs), row, count)
        return pltpu.make_async_remote_copy(
            src_ref=block, dst_ref=block,
            send_sem=fwd_send.at[number, peer - 1, step - 1, way],
            recv_sem=fwd_recv.at[number, peer - 1, step - 1, way],
            device_id={"rep": turn(my_rep, peer, reps)}, device_id_type=MESH)

    def begin(*numbers):
        for number in numbers:
            if not empty(number):
                for way in (0, 1):
                    ring(number, 1, way).start()

    def advance(number, step):
        if empty(number):
            return
        for way in (0, 1):
            ring(number, step, way).wait_recv()
            if step < half:
                ring(number, step + 1, way).start()
            for peer in range(1, reps):
                forward(number, step, way, peer).start()

    def early(*numbers):
        for number in numbers:
            for step in range(1, half):
                advance(number, step)

    def late(*numbers):
        for number in numbers:
            advance(number, half)

    def arrived(*numbers):
        for number in numbers:
            if PIECES[number][1] == 0:
                keeps[PIECES[number][0]].wait()
            if empty(number):
                continue
            for step in range(1, half + 1):
                for way in (0, 1):
                    for peer in range(1, reps):
                        forward(number, step, way, peer).wait()

    def tp_copy(stage, offset, source, target):
        return pltpu.make_async_remote_copy(
            src_ref=source, dst_ref=target,
            send_sem=tp_send.at[stage, offset - 1], recv_sem=tp_recv.at[stage, offset - 1],
            device_id={"tp": turn(my_tp, offset, tp)}, device_id_type=MESH)

    def feature_cols(owner):
        return pl.ds(pl.multiple_of(owner * width, 128), width)

    barrier = pltpu.get_barrier_semaphore()
    greeted = 0
    for name, at, count, offsets in (
            ("fs", me, fs, (1, -1)),
            ("tp", my_tp, tp, range(1, tp)),
            ("rep", my_rep, reps, range(1, reps))):
        for offset in offsets:
            pl.semaphore_signal(barrier, inc=1, device_id={name: turn(at, offset, count)},
                                device_id_type=MESH)
            greeted += 1
    pl.semaphore_wait(barrier, greeted)

    begin(0, 1)
    stream_sends = []
    for offset in range(1, tp):
        copy = tp_copy(0, offset, stream, rows_all.at[:, feature_cols(my_tp)])
        copy.start()
        stream_sends.append(copy)
    keeps = []
    for which in range(len(own)):
        keep = pltpu.make_async_copy(
            own[which], piece(which, me, 0, own[which].shape[0]), own_sem.at[which])
        keep.start()
        keeps.append(keep)
    keep_stream = pltpu.make_async_copy(
        stream, rows_all.at[:, feature_cols(my_tp)], keep_sem)
    keep_stream.start()
    early(0, 1)
    begin(2, 3, 4)
    late(0, 1)

    def norm_into(source, gain, target):
        tile = 64

        def body(i, carry):
            at = pl.ds(pl.multiple_of(i * tile, tile), tile)
            wide = source[at, :].astype(jnp.float32)
            mean = jnp.mean(wide * wide, axis=-1, keepdims=True)
            target[at, :] = (wide * lax.rsqrt(mean + EPSILON)
                             * gain[...].astype(jnp.float32)).astype(jnp.bfloat16)
            return carry

        lax.fori_loop(0, tokens // tile, body, 0)

    keep_stream.wait()
    for copy in stream_sends:
        copy.wait()
    norm_into(rows_all, mix_gain, normed)
    arrived(0)

    local_groups, group_dim = pool_w.shape[0], pool_w.shape[1]
    at_row = lax.broadcasted_iota(jnp.int32, (SEQ, SEQ), 0)
    at_col = lax.broadcasted_iota(jnp.int32, (SEQ, SEQ), 1)
    insides, inverses = [], []
    for g in range(local_groups):
        group = my_tp * local_groups + g
        level = lax.div(4 * group, local_groups * tp)
        reach = jnp.int32(2)
        for bit in range(1, 4):
            reach = jnp.where(level >= bit, jnp.int32(2 << bit), reach)
        inside = (at_col <= at_row) & (at_col > at_row - reach)
        insides.append(jnp.where(inside, 1.0, 0.0).astype(jnp.bfloat16))
        inverses.append(jnp.minimum(at_row + 1, reach).astype(jnp.float32)[:, :1])

    def mix(i, carry):
        at = pl.ds(pl.multiple_of(i * SEQ, SEQ), SEQ)
        pooled = jnp.dot(normed[at, :], in_all[...],
                         preferred_element_type=jnp.float32).astype(jnp.bfloat16)
        for g in range(local_groups):
            cols = slice(g * group_dim, (g + 1) * group_dim)
            part = pooled[:, cols]
            sums = jnp.dot(insides[g], part, preferred_element_type=jnp.float32)
            contrast = (sums / inverses[g] - part.astype(jnp.float32)).astype(jnp.bfloat16)
            mixed = jnp.dot(contrast, pool_w[g], preferred_element_type=jnp.float32)
            group_out[at, cols] = (mixed * scale[:, cols].astype(jnp.float32)).astype(jnp.bfloat16)
        return carry

    lax.fori_loop(0, tokens // SEQ, mix, 0)

    arrived(1)
    early(2)

    def spread(operand, weights, stage, sends, tile):
        def block(owner, target):
            def body(i, carry):
                at = pl.ds(pl.multiple_of(i * tile, tile), tile)
                target[at, :] = jnp.dot(operand[at, :], weights[:, feature_cols(owner)],
                                        preferred_element_type=jnp.float32).astype(jnp.bfloat16)
                return carry
            lax.fori_loop(0, tokens // tile, body, 0)

        copies = []
        recv = mix_recv if stage == 1 else ffn_recv
        for offset in sorted(range(1, tp), key=lambda o: -min(o, tp - o)):
            block(turn(my_tp, offset, tp), sends.at[offset - 1])
            copy = tp_copy(stage, offset, sends.at[offset - 1], recv.at[offset - 1])
            copy.start()
            copies.append(copy)
        block(my_tp, sends.at[tp - 1])
        return copies

    def gather_sum(base, recv, sends, target):
        tile = 64

        def body(i, carry):
            at = pl.ds(pl.multiple_of(i * tile, tile), tile)
            total = sends[tp - 1, at, :].astype(jnp.float32)
            for k in range(tp - 1):
                total = total + recv[k, at, :].astype(jnp.float32)
            target[at, :] = (base[at, :].astype(jnp.float32) + total).astype(jnp.bfloat16)
            return carry

        lax.fori_loop(0, tokens // tile, body, 0)

    mix_copies = spread(group_out, out_all, 1, mix_send, tokens // 2)
    early(3)
    begin(5)
    for copy in mix_copies:
        copy.wait()
    gather_sum(stream, mix_recv, mix_send, middle)
    keep_middle = pltpu.make_async_copy(middle, mid_all.at[:, feature_cols(my_tp)], keep_sem)
    keep_middle.start()
    middle_copies = []
    for offset in range(1, tp):
        copy = tp_copy(2, offset, middle, mid_all.at[:, feature_cols(my_tp)])
        copy.start()
        middle_copies.append(copy)
    early(4)
    begin(6, 7)
    late(2, 3)
    keep_middle.wait()
    for copy in middle_copies:
        copy.wait()
    norm_into(mid_all, ffn_gain, normed)
    early(5)
    late(4)
    early(6)
    late(5)
    early(7)
    late(6)
    arrived(2, 3, 4, 5)
    tile = tokens // 2

    def gated(i, carry):
        at = pl.ds(pl.multiple_of(i * tile, tile), tile)
        values = normed[at, :]
        gate = jnp.dot(values, gate_all[...], preferred_element_type=jnp.float32)
        up = jnp.dot(values, up_all[...], preferred_element_type=jnp.float32)
        hidden[at, :] = (gate / (1.0 + jnp.exp(-gate)) * up).astype(jnp.bfloat16)
        return carry

    lax.fori_loop(0, tokens // tile, gated, 0)
    late(7)
    arrived(6, 7)
    ffn_copies = spread(hidden, down_all, 3, ffn_send, tokens // 2)
    for number in range(len(PIECES)):
        if not empty(number):
            for step in range(1, half + 1):
                for way in (0, 1):
                    ring(number, step, way).wait_send()
    for copy in ffn_copies:
        copy.wait()
    gather_sum(middle, ffn_recv, ffn_send, result)


def ring_on_device(sizes, stream, in_weight, pool_weight, pool_scale, out_weight,
              mix_gain, ffn_gain, gate_weight, up_weight, down_weight):
    reps, fs, tp = sizes
    half = fs // 2
    tokens, width = stream.shape
    features = width * tp
    own = (in_weight, out_weight, up_weight, gate_weight, down_weight)
    full = [pltpu.VMEM((w.shape[0] * fs, w.shape[1]) if by_rows else (w.shape[0], w.shape[1] * fs),
                       jnp.bfloat16) for w, by_rows in zip(own, BY_ROWS)]
    units = gate_weight.shape[1]
    bf = jnp.bfloat16
    vmem = pl.BlockSpec(memory_space=pltpu.VMEM)
    hbm = pl.BlockSpec(memory_space=pl.ANY)
    dma = pltpu.SemaphoreType.DMA
    flops = 2 * tokens * (2 * features * in_weight.shape[1] + 3 * features * units)
    return pl.pallas_call(
        functools.partial(ring_kernel, sizes),
        out_shape=jax.ShapeDtypeStruct(stream.shape, bf),
        in_specs=[vmem] + [hbm] * 5 + [vmem] * 4,
        out_specs=vmem,
        scratch_shapes=full + [
            pltpu.VMEM((tokens, features), bf),
            pltpu.VMEM((tokens, features), bf),
            pltpu.VMEM((tokens, in_weight.shape[1]), bf),
            pltpu.VMEM((tokens, units), bf),
            pltpu.VMEM((tokens, width), bf),
            pltpu.VMEM((tokens, features), bf),
            pltpu.VMEM((tp, tokens, width), bf),
            pltpu.VMEM((tp - 1, tokens, width), bf),
            pltpu.VMEM((tp, tokens, width), bf),
            pltpu.VMEM((tp - 1, tokens, width), bf),
            dma((len(PIECES), half, 2)),
            dma((len(PIECES), half, 2)),
            dma((len(PIECES), max(reps - 1, 1), half, 2)),
            dma((len(PIECES), max(reps - 1, 1), half, 2)),
            dma((len(own),)),
            dma((4, tp - 1)),
            dma((4, tp - 1)),
            dma(()),
        ],
        compiler_params=pltpu.CompilerParams(
            collective_id=0, has_side_effects=True, vmem_limit_bytes=64 * 1024 * 1024 - 65536),
        cost_estimate=pl.CostEstimate(flops=flops, bytes_accessed=flops // 512, transcendentals=0),
    )(stream, in_weight, out_weight, up_weight, gate_weight, down_weight, pool_weight,
      pool_scale.reshape(1, -1), mix_gain.reshape(1, -1), ffn_gain.reshape(1, -1))


IN, OUT, UP, GATE, DOWN = range(5)
LANES = 128


def pair_kernel(sizes, stream, in_w, out_w, up_w, gate_w, down_w, pool_w, scale,
                mix_gain, ffn_gain, result,
                in_all, out_all, up_all, gate_all, down_all,
                rows_all, normed, group_out, hidden, gate_acts, up_acts, mid_all, normed_ffn,
                pool_sib, scale_sib,
                mix_own, mix_send, mix_recv, ffn_own, ffn_send, ffn_recv, pair_send, pair_recv,
                last_send, last_recv,
                z_send, z_recv, pass_send, y_send, y_recv, d_send, d_recv, own_sem,
                in_send, in_recv, pool_send, pool_recv, mix_sems, mid_send, mid_recv,
                x_send, x_recv, p_send, p_recv, l_send, l_recv):
    reps, fs, tp = sizes
    y, z, lane_id = lax.axis_index("rep"), lax.axis_index("fs"), lax.axis_index("tp")
    x, core = lax.div(lane_id, 2), lax.rem(lane_id, 2)
    own = (in_w, out_w, up_w, gate_w, down_w)
    full = (in_all, out_all, up_all, gate_all, down_all)
    tokens, width = stream.shape
    rows = tokens // 2
    wide = 2 * width
    seat, pair = lax.rem(z, 2), lax.div(z, 2)
    peer = z + 1 - 2 * seat
    near = jnp.where(pair == 0, 2, 1)
    far = jnp.where(pair == 0, 3, 0)
    inner = (z == 1) | (z == 2)
    f32, bf16 = jnp.float32, jnp.bfloat16

    blocks = gate_w.shape[1] // LANES
    few, many = blocks // 2, blocks - blocks // 2

    SIB = {"tp": lane_id + 1 - 2 * core}
    XPEER = {"tp": lane_id + 2 - 4 * x}
    XSIB = {"tp": 2 * (1 - x) + 1 - core}
    YPEER = {"rep": 1 - y}
    ZPEER = {"fs": peer}

    def at_least(value, multiple):
        return pl.multiple_of(value, multiple)

    def remote(source, target, send, recv, device):
        return pltpu.make_async_remote_copy(
            src_ref=source, dst_ref=target, send_sem=send, recv_sem=recv,
            device_id=device, device_id_type=MESH)

    def sized(which, core_at, seat_at, act):
        if which in (IN, OUT) or few == many:
            act(many)
            return
        big = core_at == seat_at

        @pl.when(big)
        def _():
            act(many)

        @pl.when(jnp.logical_not(big))
        def _():
            act(few)

    def extent(which):
        return own[which].shape[1 if which == DOWN else 0]

    def half_span(which, half, part=None):
        size = extent(which) // 2
        if half is None:
            return 0, 2 * size
        if part is None:
            return half * size, size
        return half * size + part * (size // 2), size // 2

    def parts(which):
        return (0, 1) if which in (UP, DOWN) else (None,)

    def place(which, source, span, core_at, seat_at, count):
        block_rows, block_cols = own[which].shape
        ref = full[which]
        start, size = span
        if which == OUT:
            return ref.at[pl.ds(at_least(core_at * block_rows + start, 16), size),
                          pl.ds(at_least(source * block_cols, LANES), block_cols)]
        if which == IN:
            return ref.at[pl.ds(at_least(source * block_rows + start, 16), size),
                          pl.ds(at_least(core_at * block_cols, LANES), block_cols)]
        first = core_at * jnp.where(seat_at == 0, many, few) * LANES
        if which == DOWN:
            return ref.at[pl.ds(at_least(first, LANES), count * LANES),
                          pl.ds(at_least(source * block_cols + start, LANES), size)]
        return ref.at[pl.ds(at_least(source * block_rows + start, 16), size),
                      pl.ds(at_least(first, LANES), count * LANES)]

    def held(which, span, seat_at, count):
        ref = own[which]
        start, size = span
        if which in (IN, OUT):
            return ref.at[pl.ds(at_least(start, 16), size), :]
        first = seat_at * jnp.where(core == 0, many, few) * LANES
        if which == DOWN:
            return ref.at[pl.ds(at_least(first, LANES), count * LANES),
                          pl.ds(at_least(start, LANES), size)]
        return ref.at[pl.ds(at_least(start, 16), size),
                      pl.ds(at_least(first, LANES), count * LANES)]

    def z_copies(which, dest, step):
        to = lax.rem(dest, 2)

        def act(n):
            for part in parts(which):
                span, slot = half_span(which, y, part), part or 0
                copy = remote(held(which, span, to, n), place(which, z, span, core, to, n),
                              z_send.at[which, dest, slot], z_recv.at[which, z, slot],
                              {"fs": dest})
                {"start": copy.start, "send": copy.wait_send}[step]()
        sized(which, core, to, act)

    def z_start(which, dest):
        z_copies(which, dest, "start")

    def z_sent(which, dest):
        z_copies(which, dest, "send")

    def z_pass(which, source):
        block = place(which, source, half_span(which, y), core, seat, many)
        return remote(block, block, pass_send.at[which, lax.rem(source, 2)],
                      z_recv.at[which, source, 0], ZPEER)

    def arrived(which, source, part):
        def act(n):
            block = place(which, source, half_span(which, y, part), core, seat, n)
            remote(block, block, y_send.at[which, source, part or 0],
                   z_recv.at[which, source, part or 0], YPEER).wait_recv()
        sized(which, core, seat, act)

    def across(which, source, part, step):
        def act(n):
            half = 1 - y if step == "recv" else y
            block = place(which, source, half_span(which, half, part), core, seat, n)
            copy = remote(block, block, y_send.at[which, source, part or 0],
                          y_recv.at[which, source, part or 0], YPEER)
            {"start": copy.start, "recv": copy.wait_recv, "send": copy.wait_send}[step]()
        sized(which, core, seat, act)

    def beside(which, source, half, step, mine=False):
        slot = 0 if half is None else half
        whose = 1 - core if step == "recv" else core

        def act(n):
            span = half_span(which, half)
            block = place(which, source, span, whose, seat, n)
            start = held(which, span, seat, n) if mine else block
            copy = remote(start, block, d_send.at[which, source, slot],
                          d_recv.at[which, source, slot], SIB)
            {"start": copy.start, "recv": copy.wait_recv, "send": copy.wait_send}[step]()
        sized(which, whose, seat, act)

    def keep(which, step):
        def act(n):
            span = half_span(which, None)
            copy = pltpu.make_async_copy(held(which, span, seat, n),
                                         place(which, z, span, core, seat, n), own_sem.at[which])
            {"start": copy.start, "wait": copy.wait}[step]()
        sized(which, core, seat, act)

    def relay(which, source, only=None):
        for part in parts(which):
            if only is None or part == only:
                arrived(which, source, part)
                across(which, source, part, "start")

    def share(which, source):
        for part in parts(which):
            across(which, source, part, "recv")
        beside(which, source, None, "start")

    def feature_cols(owner):
        return pl.ds(at_least(owner * width, LANES), width)

    def token_rows(half):
        return pl.ds(at_least(half * rows, 16), rows)

    def stream_copy(number, device, half):
        return remote(stream.at[token_rows(half), :], rows_all.at[:, feature_cols(lane_id)],
                      in_send.at[number], in_recv.at[number], device)

    barrier = pltpu.get_barrier_semaphore()
    greeted = 0
    for device in (SIB, XPEER, XSIB, YPEER, ZPEER, {"fs": near}, {"fs": far}):
        pl.semaphore_signal(barrier, inc=1, device_id=device, device_id_type=MESH)
        greeted += 1
    pl.semaphore_wait(barrier, greeted)

    outer = jnp.logical_not(inner)
    z_start(IN, near)
    z_start(IN, peer)
    stream_copies = [stream_copy(0, XPEER, core), stream_copy(1, XSIB, 1 - core),
                     stream_copy(2, SIB, 1 - core)]
    for copy in stream_copies:
        copy.start()
    z_start(OUT, near)
    z_start(OUT, peer)
    keep(IN, "start")
    beside(IN, z, None, "start", mine=True)
    pool_copy = remote(pool_w, pool_sib, pool_send.at[0], pool_recv.at[0], SIB)
    scale_copy = remote(scale, scale_sib, pool_send.at[1], pool_recv.at[1], SIB)
    pool_copy.start()
    scale_copy.start()

    @pl.when(inner)
    def _():
        z_start(GATE, near)
        z_start(GATE, far)
        z_start(UP, near)

    @pl.when(outer)
    def _():
        z_start(GATE, peer)
        z_start(GATE, far)
        z_start(UP, far)
        z_start(UP, peer)

    for which in (OUT, GATE, UP, DOWN):
        keep(which, "start")
        for half in (0, 1) if which == DOWN else (None,):
            beside(which, z, half, "start", mine=True)

    rows_all[:, feature_cols(lane_id)] = stream[token_rows(core), :]

    def take(which):
        relay(which, peer)
        for source in (near, far):
            arrived(which, source, None)

            @pl.when(inner)
            def _():
                z_pass(which, source).start()
            across(which, source, None, "start")

    take(IN)

    @pl.when(inner)
    def _():
        take(OUT)

    def norm_into(source, gain, target, first, count):
        tile = 64

        def body(i, carry):
            at = pl.ds(at_least(first + i * tile, tile), tile)
            values = source[at, :].astype(f32)
            mean = jnp.mean(values * values, axis=-1, keepdims=True)
            target[at, :] = (values * lax.rsqrt(mean + EPSILON)
                             * gain[...].astype(f32)).astype(bf16)
            return carry

        lax.fori_loop(0, count // tile, body, 0)

    for copy in stream_copies:
        copy.wait()
    norm_into(rows_all, mix_gain, normed, 0, rows)
    for source in (peer, near, far):
        share(IN, source)

    @pl.when(outer)
    def _():
        take(OUT)

    pool_copy.wait()
    scale_copy.wait()
    for source in (z, peer, near, far):
        beside(IN, source, None, "recv")
    keep(IN, "wait")

    local_groups, group_dim = pool_w.shape[0], pool_w.shape[1]
    at_row = lax.broadcasted_iota(jnp.int32, (SEQ, SEQ), 0)
    at_col = lax.broadcasted_iota(jnp.int32, (SEQ, SEQ), 1)
    pooled = jnp.dot(normed[...], in_all[...], preferred_element_type=f32).astype(bf16)
    for g in range(2 * local_groups):
        owner, place_in = divmod(g, local_groups)
        group = x * 2 * local_groups + g
        level = lax.div(4 * group, local_groups * tp)
        reach = jnp.int32(2)
        for bit in range(1, 4):
            reach = jnp.where(level >= bit, jnp.int32(2 << bit), reach)
        inside = jnp.where((at_col <= at_row) & (at_col > at_row - reach), 1.0, 0.0).astype(bf16)
        counts = jnp.minimum(at_row + 1, reach).astype(f32)[:, :1]
        is_own = core == owner
        cols = slice(g * group_dim, (g + 1) * group_dim)
        own_cols = slice(place_in * group_dim, (place_in + 1) * group_dim)
        weight = jnp.where(is_own, pool_w[place_in], pool_sib[place_in])
        factor = jnp.where(is_own, scale[:, own_cols].astype(f32),
                           scale_sib[:, own_cols].astype(f32))
        for s in range(rows // SEQ):
            at = slice(s * SEQ, (s + 1) * SEQ)
            part = pooled[at, cols]
            sums = jnp.dot(inside, part, preferred_element_type=f32)
            contrast = (sums / counts - part.astype(f32)).astype(bf16)
            mixed = jnp.dot(contrast, weight, preferred_element_type=f32)
            group_out[at, cols] = (mixed * factor).astype(bf16)

    for source in (peer, near, far):
        share(OUT, source)
    for source in (z, peer, near, far):
        beside(OUT, source, None, "recv")
    keep(OUT, "wait")

    def half_cols(owner):
        return pl.ds(at_least(owner * wide, LANES), wide)

    mix_send[...] = jnp.dot(group_out[...], out_all[:, half_cols(1 - x)],
                            preferred_element_type=f32).astype(bf16)
    mix_copy = remote(mix_send, mix_recv, mix_sems.at[0], mix_sems.at[1], XPEER)
    mix_copy.start()
    mix_own[...] = jnp.dot(group_out[...], out_all[:, half_cols(x)], preferred_element_type=f32)

    @pl.when(inner)
    def _():
        relay(GATE, peer)
        relay(GATE, near)

    @pl.when(outer)
    def _():
        relay(GATE, far)

    mix_copy.wait()
    mid_rows = pl.ds(at_least(seat * rows, 16), rows)
    mid_all[mid_rows, half_cols(x)] = (
        rows_all[:, half_cols(x)].astype(f32) + (mix_own[...] + mix_recv[...].astype(f32))).astype(bf16)

    def mid_copy(number, block, device):
        view = mid_all.at[pl.ds(at_least(block * rows, 16), rows), half_cols(x)]
        return remote(view, view, mid_send.at[number], mid_recv.at[number], device)

    to_pair, to_x, to_x_later = mid_copy(0, seat, ZPEER), mid_copy(1, seat, XPEER), mid_copy(2, 1 - seat, XPEER)
    to_pair.start()
    to_x.start()

    @pl.when(inner)
    def _():
        z_start(GATE, peer)
        z_start(UP, peer)
        z_start(UP, far)
        share(GATE, peer)
        share(GATE, near)
        relay(UP, peer)
        relay(UP, near)

    @pl.when(outer)
    def _():
        z_start(GATE, near)
        z_start(UP, near)
        share(GATE, far)
        relay(UP, far)
        relay(GATE, near)

    to_pair.wait_recv()
    to_x_later.start()

    @pl.when(inner)
    def _():
        z_start(DOWN, far)
        z_start(DOWN, near)
        z_start(DOWN, peer)
        share(UP, peer)

    @pl.when(outer)
    def _():
        z_start(DOWN, peer)
        z_start(DOWN, near)
        z_start(DOWN, far)
        share(UP, far)
        share(GATE, near)

    to_x.wait_recv()
    norm_into(mid_all, ffn_gain, normed_ffn, seat * rows, rows)

    @pl.when(inner)
    def _():
        share(UP, near)
        relay(GATE, far)

    @pl.when(outer)
    def _():
        relay(GATE, peer)

    to_x_later.wait_recv()
    norm_into(mid_all, ffn_gain, normed_ffn, (1 - seat) * rows, rows)

    early = (jnp.where(inner, z, far), jnp.where(inner, peer, near))
    later = (jnp.where(inner, near, z), jnp.where(inner, far, peer))
    depth = gate_all.shape[0] // 2
    early_at = pl.ds(at_least(jnp.where(inner, pair, 1 - pair) * depth, LANES), depth)
    later_at = pl.ds(at_least(jnp.where(inner, 1 - pair, pair) * depth, LANES), depth)
    tile = rows

    def by_tiles(body):
        def step(i, carry):
            body(pl.ds(at_least(i * tile, tile), tile))
            return carry
        lax.fori_loop(0, 2 * rows // tile, step, 0)

    def partial_dot(at, depth_at, weights):
        return jnp.dot(normed_ffn[at, depth_at], weights[depth_at, :], preferred_element_type=f32)

    def gate_first(at):
        gate_acts[at, :] = partial_dot(at, early_at, gate_all)

    def gate_second(at):
        gate = gate_acts[at, :] + partial_dot(at, later_at, gate_all)
        gate_acts[at, :] = gate / (1.0 + jnp.exp(-gate))

    def up_first(at):
        up_acts[at, :] = partial_dot(at, early_at, up_all)

    def up_second(at):
        up = up_acts[at, :] + partial_dot(at, later_at, up_all)
        hidden[at, :] = (gate_acts[at, :] * up).astype(bf16)

    keep(GATE, "wait")
    for source in early:
        beside(GATE, source, None, "recv")
    by_tiles(gate_first)

    @pl.when(inner)
    def _():
        relay(UP, far)
        share(GATE, far)

    @pl.when(outer)
    def _():
        relay(UP, near)
        share(GATE, peer)

    for source in later:
        beside(GATE, source, None, "recv")
    by_tiles(gate_second)

    @pl.when(outer)
    def _():
        share(UP, near)
        relay(UP, peer)

    keep(UP, "wait")
    for source in early:
        beside(UP, source, None, "recv")
    by_tiles(up_first)

    @pl.when(inner)
    def _():
        share(UP, far)

    @pl.when(outer)
    def _():
        share(UP, peer)
        relay(DOWN, far, 0)

    for source in later:
        beside(UP, source, None, "recv")
    by_tiles(up_second)

    sub = width // 2
    order = (z, peer, far, near)
    keeps_early = x == pair

    def is_kept(o):
        return keeps_early if o < 2 else jnp.logical_not(keeps_early)

    def half_of(turn):
        return y if turn == 0 else 1 - y

    def column_block(o, turn):
        at = pl.ds(at_least(order[o] * width + half_of(turn) * sub, LANES), sub)
        slot = 2 * (o % 2) + turn
        values = jnp.dot(hidden[...], down_all[:, at], preferred_element_type=f32)

        @pl.when(is_kept(o))
        def _():
            ffn_own[slot] = values

        @pl.when(jnp.logical_not(is_kept(o)))
        def _():
            ffn_send[slot] = values.astype(bf16)
            x_copy(slot).start()

    def x_copy(slot):
        return remote(ffn_send.at[slot], ffn_recv.at[slot], x_send.at[slot], x_recv.at[slot], XPEER)

    def pair_copy(o, turn):
        quarter, half = lax.rem(order[o], 2), half_of(turn)
        return remote(pair_send.at[quarter, half], pair_recv.at[quarter, half],
                      p_send.at[quarter, half], p_recv.at[quarter, half], ZPEER)

    def fold(o, turn):
        slot = 2 * (o % 2) + turn
        quarter, half = lax.rem(order[o], 2), half_of(turn)

        @pl.when(is_kept(o))
        def _():
            x_copy(slot).wait_recv()
            theirs = pl.ds(at_least((1 - seat) * rows, 16), rows)
            pair_send[quarter, half] = (ffn_own[slot, theirs, :]
                                        + ffn_recv[slot, theirs, :].astype(f32)).astype(bf16)
            pair_copy(o, turn).start()

    def last_copy(half):
        return remote(last_send.at[half], last_recv.at[half], l_send.at[half], l_recv.at[half], SIB)

    def settle(o, turn):
        slot = 2 * (o % 2) + turn
        quarter, half = lax.rem(order[o], 2), half_of(turn)

        @pl.when(is_kept(o))
        def _():
            pair_copy(o, turn).wait_recv()
            ours = pl.ds(at_least(seat * rows, 16), rows)
            cols = pl.ds(at_least(order[o] * width + half * sub, LANES), sub)
            total = (ffn_own[slot, ours, :] + ffn_recv[slot, ours, :].astype(f32)
                     + pair_recv[quarter, half].astype(f32))
            value = (mid_all[ours, cols].astype(f32) + total).astype(bf16)

            @pl.when(quarter == core)
            def _():
                result[token_rows(core), pl.ds(at_least(half * sub, LANES), sub)] = value

            @pl.when(quarter != core)
            def _():
                last_send[half] = value
                last_copy(half).start()

    def pour(source):
        for part in parts(DOWN):
            across(DOWN, source, part, "recv")
        beside(DOWN, source, 1 - y, "start")

    def ready(source, turn):
        beside(DOWN, source, half_of(turn), "recv")

    OWN, PEER, FAR, NEAR = range(4)

    def bring(o, only=None):
        relay(DOWN, order[o], only)
        beside(DOWN, order[o], y, "start")

    def block(o, turn):
        ready(order[o], turn)
        column_block(o, turn)

    keep(DOWN, "wait")

    @pl.when(outer)
    def _():
        bring(FAR, 1)
        block(OWN, 0)
        block(OWN, 1)
        bring(PEER)
        block(FAR, 0)
        pour(far)
        block(FAR, 1)
        bring(NEAR)
        block(PEER, 0)
        pour(peer)
        block(PEER, 1)
        fold(OWN, 0)
        block(NEAR, 0)
        fold(OWN, 1)
        fold(FAR, 0)
        fold(FAR, 1)
        pour(near)
        block(NEAR, 1)
        fold(PEER, 0)

    @pl.when(inner)
    def _():
        block(OWN, 0)
        block(OWN, 1)
        bring(PEER)
        block(PEER, 0)
        bring(FAR)
        pour(peer)
        block(PEER, 1)
        fold(OWN, 0)
        block(FAR, 0)
        pour(far)
        block(FAR, 1)
        fold(OWN, 1)
        fold(PEER, 0)
        fold(FAR, 0)
        bring(NEAR)
        fold(FAR, 1)
        block(NEAR, 0)
        pour(near)
        block(NEAR, 1)

    fold(PEER, 1)
    fold(NEAR, 0)
    for o in (OWN, PEER):
        for turn in (0, 1):
            settle(o, turn)
    for turn in (0, 1):
        settle(FAR, turn)
    fold(NEAR, 1)
    for turn in (0, 1):
        settle(NEAR, turn)

    for half in (0, 1):
        last_copy(half).wait()
        result[token_rows(1 - core), half * sub:(half + 1) * sub] = last_recv[half]

    for which in range(5):
        z_sent(which, peer)
        z_sent(which, near)
        if which not in (IN, OUT):
            z_sent(which, far)
        else:
            @pl.when(inner)
            def _():
                for source in (near, far):
                    z_pass(which, source).wait_send()
        for source in (peer, near, far):
            for part in parts(which):
                across(which, source, part, "send")
        for source in order:
            for half in (0, 1) if which == DOWN else (None,):
                beside(which, source, half, "send", mine=False)
    for copy in (to_pair, to_x, to_x_later):
        copy.wait_send()
    for slot in range(4):
        x_copy(slot).wait_send()
    for quarter in (0, 1):
        for half in (0, 1):
            remote(pair_send.at[quarter, half], pair_recv.at[quarter, half],
                   p_send.at[quarter, half], p_recv.at[quarter, half], ZPEER).wait_send()


def pairs_fit(sizes, stream, in_weight, pool_weight, out_weight, gate_weight, down_weight):
    reps, fs, tp = sizes
    tokens, width = stream.shape
    return (reps == 2 and fs == 4 and tp == 4 and tokens % (2 * SEQ) == 0
            and width % (2 * LANES) == 0 and gate_weight.shape[1] % LANES == 0
            and in_weight.shape[1] % LANES == 0 and in_weight.shape[0] % 32 == 0
            and out_weight.shape[0] % 32 == 0 and gate_weight.shape[0] % 32 == 0
            and down_weight.shape[1] == width)


def pair_on_device(sizes, stream, in_weight, pool_weight, pool_scale, out_weight,
                   mix_gain, ffn_gain, gate_weight, up_weight, down_weight):
    if not pairs_fit(sizes, stream, in_weight, pool_weight, out_weight, gate_weight, down_weight):
        return ring_on_device(sizes, stream, in_weight, pool_weight, pool_scale, out_weight,
                              mix_gain, ffn_gain, gate_weight, up_weight, down_weight)
    reps, fs, tp = sizes
    tokens, width = stream.shape
    rows, sub = tokens // 2, width // 2
    features = width * tp
    channels = in_weight.shape[1]
    units = gate_weight.shape[1]
    bf, f32 = jnp.bfloat16, jnp.float32
    vmem = pl.BlockSpec(memory_space=pltpu.VMEM)
    hbm = pl.BlockSpec(memory_space=pl.ANY)
    dma = pltpu.SemaphoreType.DMA
    flops = 2 * tokens * (2 * features * channels + 3 * features * units)
    return pl.pallas_call(
        functools.partial(pair_kernel, sizes),
        out_shape=jax.ShapeDtypeStruct(stream.shape, bf),
        in_specs=[vmem] + [hbm] * 5 + [vmem] * 4,
        out_specs=vmem,
        scratch_shapes=[
            pltpu.VMEM((in_weight.shape[0] * fs, 2 * channels), bf),
            pltpu.VMEM((2 * out_weight.shape[0], out_weight.shape[1] * fs), bf),
            pltpu.VMEM((up_weight.shape[0] * fs, units), bf),
            pltpu.VMEM((gate_weight.shape[0] * fs, units), bf),
            pltpu.VMEM((units, down_weight.shape[1] * fs), bf),
            pltpu.VMEM((rows, features), bf),
            pltpu.VMEM((rows, features), bf),
            pltpu.VMEM((rows, 2 * channels), bf),
            pltpu.VMEM((2 * rows, units), bf),
            pltpu.VMEM((2 * rows, units), f32),
            pltpu.VMEM((2 * rows, units), f32),
            pltpu.VMEM((2 * rows, features), bf),
            pltpu.VMEM((2 * rows, features), bf),
            pltpu.VMEM(pool_weight.shape, bf),
            pltpu.VMEM((1, channels), bf),
            pltpu.VMEM((rows, 2 * width), f32),
            pltpu.VMEM((rows, 2 * width), bf),
            pltpu.VMEM((rows, 2 * width), bf),
            pltpu.VMEM((4, 2 * rows, sub), f32),
            pltpu.VMEM((4, 2 * rows, sub), bf),
            pltpu.VMEM((4, 2 * rows, sub), bf),
            pltpu.VMEM((2, 2, rows, sub), bf),
            pltpu.VMEM((2, 2, rows, sub), bf),
            pltpu.VMEM((2, rows, sub), bf),
            pltpu.VMEM((2, rows, sub), bf),
            dma((5, fs, 2)), dma((5, fs, 2)), dma((2, 2)), dma((5, fs, 2)), dma((5, fs, 2)),
            dma((5, fs, 2)), dma((5, fs, 2)), dma((5,)),
            dma((3,)), dma((3,)), dma((2,)), dma((2,)), dma((2,)), dma((3,)), dma((3,)),
            dma((4,)), dma((4,)), dma((2, 2)), dma((2, 2)), dma((2,)), dma((2,)),
        ],
        compiler_params=pltpu.CompilerParams(
            collective_id=0, has_side_effects=True, vmem_limit_bytes=64 * 1024 * 1024 - 65536),
        cost_estimate=pl.CostEstimate(flops=flops, bytes_accessed=flops // 512, transcendentals=0),
    )(stream, in_weight, out_weight, up_weight, gate_weight, down_weight, pool_weight,
      pool_scale.reshape(1, -1), mix_gain.reshape(1, -1), ffn_gain.reshape(1, -1))


def solution(mesh):
    sizes = tuple(mesh.shape[name] for name in ("rep", "fs", "tp"))
    return jax.shard_map(
        functools.partial(pair_on_device, sizes),
        mesh=mesh,
        in_specs=(
            P(("rep", "fs"), "tp"),
            P("fs", "tp"),
            P("tp", None, None),
            P("tp"),
            P("tp", "fs"),
            P(),
            P(),
            P("fs", "tp"),
            P("fs", "tp"),
            P("tp", "fs"),
        ),
        out_specs=P(("rep", "fs"), "tp"),
        check_vma=False,
    )
```

```python
import functools

import jax
import jax.numpy as jnp
from jax import lax
from jax.experimental import pallas as pl
from jax.experimental.pallas import tpu as pltpu
from jax.sharding import PartitionSpec as P

SEQ = 128
EPSILON = 1e-06
MESH = pl.DeviceIdType.MESH
BY_ROWS = (True, False, True, True, False)
PIECES = ((0, 0), (1, 0), (2, 0), (3, 0), (2, 1), (3, 1), (4, 0), (4, 1))
CHUNKS = (1, 1, 2, 2, 2)


def ring_kernel(sizes, stream, in_w, out_w, up_w, gate_w, down_w, pool_w, scale,
           mix_gain, ffn_gain, result,
           in_all, out_all, up_all, gate_all, down_all,
           rows_all, normed, group_out, hidden, middle, mid_all,
           mix_send, mix_recv, ffn_send, ffn_recv,
           ring_send, ring_recv, fwd_send, fwd_recv, own_sem,
           tp_send, tp_recv, keep_sem):
    reps, fs, tp = sizes
    half = fs // 2
    my_rep, me, my_tp = lax.axis_index("rep"), lax.axis_index("fs"), lax.axis_index("tp")
    own = (in_w, out_w, up_w, gate_w, down_w)
    full = (in_all, out_all, up_all, gate_all, down_all)
    tokens, width = stream.shape

    def turn(at, by, count):
        return lax.rem(at + by + count, count)

    def piece(which, owner, row, count):
        block_rows, block_cols = own[which].shape
        if BY_ROWS[which]:
            return full[which].at[pl.ds(pl.multiple_of(owner * block_rows + row, 16), count), :]
        return full[which].at[pl.ds(pl.multiple_of(row, 16), count),
                              pl.ds(pl.multiple_of(owner * block_cols, 128), block_cols)]

    def span(number, step, way):
        which, chunk = PIECES[number]
        rows = own[which].shape[0]
        cut = rows % (CHUNKS[which] * reps * 2 * 16) == 0
        count = rows // CHUNKS[which] if cut else (rows, 0)[chunk]
        row = chunk * (rows // CHUNKS[which])
        count = count // reps
        row = row + my_rep * count
        if step == half:
            count = count // 2
            row = row + way * count
        return which, row, count

    def empty(number):
        return span(number, 1, 0)[2] == 0

    def ring(number, step, way):
        which, row, count = span(number, step, way)
        sign = 1 - 2 * way
        owner = turn(me, -sign * (step - 1), fs)
        if step == 1:
            source = own[which].at[pl.ds(pl.multiple_of(row, 16), count), :]
        else:
            source = piece(which, owner, row, count)
        return pltpu.make_async_remote_copy(
            src_ref=source, dst_ref=piece(which, owner, row, count),
            send_sem=ring_send.at[number, step - 1, way],
            recv_sem=ring_recv.at[number, step - 1, way],
            device_id={"fs": turn(me, sign, fs)}, device_id_type=MESH)

    def forward(number, step, way, peer):
        which, row, count = span(number, step, way)
        block = piece(which, turn(me, -(1 - 2 * way) * step, fs), row, count)
        return pltpu.make_async_remote_copy(
            src_ref=block, dst_ref=block,
            send_sem=fwd_send.at[number, peer - 1, step - 1, way],
            recv_sem=fwd_recv.at[number, peer - 1, step - 1, way],
            device_id={"rep": turn(my_rep, peer, reps)}, device_id_type=MESH)

    def begin(*numbers):
        for number in numbers:
            if not empty(number):
                for way in (0, 1):
                    ring(number, 1, way).start()

    def advance(number, step):
        if empty(number):
            return
        for way in (0, 1):
            ring(number, step, way).wait_recv()
            if step < half:
                ring(number, step + 1, way).start()
            for peer in range(1, reps):
                forward(number, step, way, peer).start()

    def early(*numbers):
        for number in numbers:
            for step in range(1, half):
                advance(number, step)

    def late(*numbers):
        for number in numbers:
            advance(number, half)

    def arrived(*numbers):
        for number in numbers:
            if PIECES[number][1] == 0:
                keeps[PIECES[number][0]].wait()
            if empty(number):
                continue
            for step in range(1, half + 1):
                for way in (0, 1):
                    for peer in range(1, reps):
                        forward(number, step, way, peer).wait()

    def tp_copy(stage, offset, source, target):
        return pltpu.make_async_remote_copy(
            src_ref=source, dst_ref=target,
            send_sem=tp_send.at[stage, offset - 1], recv_sem=tp_recv.at[stage, offset - 1],
            device_id={"tp": turn(my_tp, offset, tp)}, device_id_type=MESH)

    def feature_cols(owner):
        return pl.ds(pl.multiple_of(owner * width, 128), width)

    barrier = pltpu.get_barrier_semaphore()
    greeted = 0
    for name, at, count, offsets in (
            ("fs", me, fs, (1, -1)),
            ("tp", my_tp, tp, range(1, tp)),
            ("rep", my_rep, reps, range(1, reps))):
        for offset in offsets:
            pl.semaphore_signal(barrier, inc=1, device_id={name: turn(at, offset, count)},
                                device_id_type=MESH)
            greeted += 1
    pl.semaphore_wait(barrier, greeted)

    begin(0, 1)
    stream_sends = []
    for offset in range(1, tp):
        copy = tp_copy(0, offset, stream, rows_all.at[:, feature_cols(my_tp)])
        copy.start()
        stream_sends.append(copy)
    keeps = []
    for which in range(len(own)):
        keep = pltpu.make_async_copy(
            own[which], piece(which, me, 0, own[which].shape[0]), own_sem.at[which])
        keep.start()
        keeps.append(keep)
    keep_stream = pltpu.make_async_copy(
        stream, rows_all.at[:, feature_cols(my_tp)], keep_sem)
    keep_stream.start()
    early(0, 1)
    begin(2, 3, 4)
    late(0, 1)

    def norm_into(source, gain, target):
        tile = 64

        def body(i, carry):
            at = pl.ds(pl.multiple_of(i * tile, tile), tile)
            wide = source[at, :].astype(jnp.float32)
            mean = jnp.mean(wide * wide, axis=-1, keepdims=True)
            target[at, :] = (wide * lax.rsqrt(mean + EPSILON)
                             * gain[...].astype(jnp.float32)).astype(jnp.bfloat16)
            return carry

        lax.fori_loop(0, tokens // tile, body, 0)

    keep_stream.wait()
    for copy in stream_sends:
        copy.wait()
    norm_into(rows_all, mix_gain, normed)
    arrived(0)

    local_groups, group_dim = pool_w.shape[0], pool_w.shape[1]
    at_row = lax.broadcasted_iota(jnp.int32, (SEQ, SEQ), 0)
    at_col = lax.broadcasted_iota(jnp.int32, (SEQ, SEQ), 1)
    insides, inverses = [], []
    for g in range(local_groups):
        group = my_tp * local_groups + g
        level = lax.div(4 * group, local_groups * tp)
        reach = jnp.int32(2)
        for bit in range(1, 4):
            reach = jnp.where(level >= bit, jnp.int32(2 << bit), reach)
        inside = (at_col <= at_row) & (at_col > at_row - reach)
        insides.append(jnp.where(inside, 1.0, 0.0).astype(jnp.bfloat16))
        inverses.append(jnp.minimum(at_row + 1, reach).astype(jnp.float32)[:, :1])

    def mix(i, carry):
        at = pl.ds(pl.multiple_of(i * SEQ, SEQ), SEQ)
        pooled = jnp.dot(normed[at, :], in_all[...],
                         preferred_element_type=jnp.float32).astype(jnp.bfloat16)
        for g in range(local_groups):
            cols = slice(g * group_dim, (g + 1) * group_dim)
            part = pooled[:, cols]
            sums = jnp.dot(insides[g], part, preferred_element_type=jnp.float32)
            contrast = (sums / inverses[g] - part.astype(jnp.float32)).astype(jnp.bfloat16)
            mixed = jnp.dot(contrast, pool_w[g], preferred_element_type=jnp.float32)
            group_out[at, cols] = (mixed * scale[:, cols].astype(jnp.float32)).astype(jnp.bfloat16)
        return carry

    lax.fori_loop(0, tokens // SEQ, mix, 0)

    arrived(1)
    early(2)

    def spread(operand, weights, stage, sends, tile):
        def block(owner, target):
            def body(i, carry):
                at = pl.ds(pl.multiple_of(i * tile, tile), tile)
                target[at, :] = jnp.dot(operand[at, :], weights[:, feature_cols(owner)],
                                        preferred_element_type=jnp.float32).astype(jnp.bfloat16)
                return carry
            lax.fori_loop(0, tokens // tile, body, 0)

        copies = []
        recv = mix_recv if stage == 1 else ffn_recv
        for offset in sorted(range(1, tp), key=lambda o: -min(o, tp - o)):
            block(turn(my_tp, offset, tp), sends.at[offset - 1])
            copy = tp_copy(stage, offset, sends.at[offset - 1], recv.at[offset - 1])
            copy.start()
            copies.append(copy)
        block(my_tp, sends.at[tp - 1])
        return copies

    def gather_sum(base, recv, sends, target):
        tile = 64

        def body(i, carry):
            at = pl.ds(pl.multiple_of(i * tile, tile), tile)
            total = sends[tp - 1, at, :].astype(jnp.float32)
            for k in range(tp - 1):
                total = total + recv[k, at, :].astype(jnp.float32)
            target[at, :] = (base[at, :].astype(jnp.float32) + total).astype(jnp.bfloat16)
            return carry

        lax.fori_loop(0, tokens // tile, body, 0)

    mix_copies = spread(group_out, out_all, 1, mix_send, tokens // 2)
    early(3)
    begin(5)
    for copy in mix_copies:
        copy.wait()
    gather_sum(stream, mix_recv, mix_send, middle)
    keep_middle = pltpu.make_async_copy(middle, mid_all.at[:, feature_cols(my_tp)], keep_sem)
    keep_middle.start()
    middle_copies = []
    for offset in range(1, tp):
        copy = tp_copy(2, offset, middle, mid_all.at[:, feature_cols(my_tp)])
        copy.start()
        middle_copies.append(copy)
    early(4)
    begin(6, 7)
    late(2, 3)
    keep_middle.wait()
    for copy in middle_copies:
        copy.wait()
    norm_into(mid_all, ffn_gain, normed)
    early(5)
    late(4)
    early(6)
    late(5)
    early(7)
    late(6)
    arrived(2, 3, 4, 5)
    tile = tokens // 2

    def gated(i, carry):
        at = pl.ds(pl.multiple_of(i * tile, tile), tile)
        values = normed[at, :]
        gate = jnp.dot(values, gate_all[...], preferred_element_type=jnp.float32)
        up = jnp.dot(values, up_all[...], preferred_element_type=jnp.float32)
        hidden[at, :] = (gate / (1.0 + jnp.exp(-gate)) * up).astype(jnp.bfloat16)
        return carry

    lax.fori_loop(0, tokens // tile, gated, 0)
    late(7)
    arrived(6, 7)
    ffn_copies = spread(hidden, down_all, 3, ffn_send, tokens // 2)
    for number in range(len(PIECES)):
        if not empty(number):
            for step in range(1, half + 1):
                for way in (0, 1):
                    ring(number, step, way).wait_send()
    for copy in ffn_copies:
        copy.wait()
    gather_sum(middle, ffn_recv, ffn_send, result)


def ring_on_device(sizes, stream, in_weight, pool_weight, pool_scale, out_weight,
              mix_gain, ffn_gain, gate_weight, up_weight, down_weight):
    reps, fs, tp = sizes
    half = fs // 2
    tokens, width = stream.shape
    features = width * tp
    own = (in_weight, out_weight, up_weight, gate_weight, down_weight)
    full = [pltpu.VMEM((w.shape[0] * fs, w.shape[1]) if by_rows else (w.shape[0], w.shape[1] * fs),
                       jnp.bfloat16) for w, by_rows in zip(own, BY_ROWS)]
    units = gate_weight.shape[1]
    bf = jnp.bfloat16
    vmem = pl.BlockSpec(memory_space=pltpu.VMEM)
    hbm = pl.BlockSpec(memory_space=pl.ANY)
    dma = pltpu.SemaphoreType.DMA
    flops = 2 * tokens * (2 * features * in_weight.shape[1] + 3 * features * units)
    return pl.pallas_call(
        functools.partial(ring_kernel, sizes),
        out_shape=jax.ShapeDtypeStruct(stream.shape, bf),
        in_specs=[vmem] + [hbm] * 5 + [vmem] * 4,
        out_specs=vmem,
        scratch_shapes=full + [
            pltpu.VMEM((tokens, features), bf),
            pltpu.VMEM((tokens, features), bf),
            pltpu.VMEM((tokens, in_weight.shape[1]), bf),
            pltpu.VMEM((tokens, units), bf),
            pltpu.VMEM((tokens, width), bf),
            pltpu.VMEM((tokens, features), bf),
            pltpu.VMEM((tp, tokens, width), bf),
            pltpu.VMEM((tp - 1, tokens, width), bf),
            pltpu.VMEM((tp, tokens, width), bf),
            pltpu.VMEM((tp - 1, tokens, width), bf),
            dma((len(PIECES), half, 2)),
            dma((len(PIECES), half, 2)),
            dma((len(PIECES), max(reps - 1, 1), half, 2)),
            dma((len(PIECES), max(reps - 1, 1), half, 2)),
            dma((len(own),)),
            dma((4, tp - 1)),
            dma((4, tp - 1)),
            dma(()),
        ],
        compiler_params=pltpu.CompilerParams(
            collective_id=0, has_side_effects=True, vmem_limit_bytes=64 * 1024 * 1024 - 65536),
        cost_estimate=pl.CostEstimate(flops=flops, bytes_accessed=flops // 512, transcendentals=0),
    )(stream, in_weight, out_weight, up_weight, gate_weight, down_weight, pool_weight,
      pool_scale.reshape(1, -1), mix_gain.reshape(1, -1), ffn_gain.reshape(1, -1))


IN, OUT, UP, GATE, DOWN = range(5)
LANES = 128


def pair_kernel(sizes, stream, in_w, out_w, up_w, gate_w, down_w, pool_w, scale,
                mix_gain, ffn_gain, result,
                in_all, out_all, up_all, gate_all, down_all,
                rows_all, normed, group_out, hidden, gate_acts, up_acts, mid_all, normed_ffn,
                pool_sib, scale_sib,
                mix_own, mix_send, mix_recv, ffn_own, ffn_send, ffn_recv, pair_send, pair_recv,
                last_send, last_recv,
                z_send, z_recv, pass_send, y_send, y_recv, d_send, d_recv, own_sem,
                in_send, in_recv, pool_send, pool_recv, mix_sems, mid_send, mid_recv,
                x_send, x_recv, p_send, p_recv, l_send, l_recv):
    reps, fs, tp = sizes
    y, z, lane_id = lax.axis_index("rep"), lax.axis_index("fs"), lax.axis_index("tp")
    x, core = lax.div(lane_id, 2), lax.rem(lane_id, 2)
    own = (in_w, out_w, up_w, gate_w, down_w)
    full = (in_all, out_all, up_all, gate_all, down_all)
    tokens, width = stream.shape
    rows = tokens // 2
    wide = 2 * width
    seat, pair = lax.rem(z, 2), lax.div(z, 2)
    peer = z + 1 - 2 * seat
    near = jnp.where(pair == 0, 2, 1)
    far = jnp.where(pair == 0, 3, 0)
    inner = (z == 1) | (z == 2)
    f32, bf16 = jnp.float32, jnp.bfloat16

    blocks = gate_w.shape[1] // LANES
    few, many = blocks // 2, blocks - blocks // 2

    SIB = {"tp": lane_id + 1 - 2 * core}
    XPEER = {"tp": lane_id + 2 - 4 * x}
    XSIB = {"tp": 2 * (1 - x) + 1 - core}
    YPEER = {"rep": 1 - y}
    ZPEER = {"fs": peer}

    def at_least(value, multiple):
        return pl.multiple_of(value, multiple)

    def remote(source, target, send, recv, device):
        return pltpu.make_async_remote_copy(
            src_ref=source, dst_ref=target, send_sem=send, recv_sem=recv,
            device_id=device, device_id_type=MESH)

    def sized(which, roomy, act):
        if which in (IN, OUT) or few == many:
            act(many)
            return

        @pl.when(roomy)
        def _():
            act(many)

        @pl.when(jnp.logical_not(roomy))
        def _():
            act(few)

    def extent(which):
        return own[which].shape[1 if which == DOWN else 0]

    def half_span(which, half, part=None):
        size = extent(which) // 2
        if half is None:
            return 0, 2 * size
        if part is None:
            return half * size, size
        return half * size + part * (size // 2), size // 2

    def parts(which):
        return (0, 1) if which in (UP, DOWN) else (None,)

    def place(which, source, span, core_at, count):
        block_rows, block_cols = own[which].shape
        ref = full[which]
        start, size = span
        if which == OUT:
            return ref.at[pl.ds(at_least(core_at * block_rows + start, 16), size),
                          pl.ds(at_least(source * block_cols, LANES), block_cols)]
        if which == IN:
            return ref.at[pl.ds(at_least(source * block_rows + start, 16), size),
                          pl.ds(at_least(core_at * block_cols, LANES), block_cols)]
        first = core_at * (count * LANES)
        if which == DOWN:
            return ref.at[pl.ds(at_least(first, LANES), count * LANES),
                          pl.ds(at_least(source * block_cols + start, LANES), size)]
        return ref.at[pl.ds(at_least(source * block_rows + start, 16), size),
                      pl.ds(at_least(first, LANES), count * LANES)]

    def held(which, span, roomy, count):
        ref = own[which]
        start, size = span
        if which in (IN, OUT):
            return ref.at[pl.ds(at_least(start, 16), size), :]
        first = jnp.where(roomy, 0, many * LANES)
        if which == DOWN:
            return ref.at[pl.ds(at_least(first, LANES), count * LANES),
                          pl.ds(at_least(start, LANES), size)]
        return ref.at[pl.ds(at_least(start, 16), size),
                      pl.ds(at_least(first, LANES), count * LANES)]

    def z_copies(which, dest, step, only=None):
        roomy = (dest == 1) | (dest == 2)

        def act(n):
            for part in parts(which) if only is None else (only,):
                span, slot = half_span(which, y, part), part or 0
                copy = remote(held(which, span, roomy, n), place(which, z, span, core, n),
                              z_send.at[which, dest, slot], z_recv.at[which, z, slot],
                              {"fs": dest})
                {"start": copy.start, "send": copy.wait_send}[step]()
        sized(which, roomy, act)

    def z_start(which, dest, only=None):
        z_copies(which, dest, "start", only)

    def z_sent(which, dest):
        z_copies(which, dest, "send")

    def z_pass(which, source):
        block = place(which, source, half_span(which, y), core, many)
        return remote(block, block, pass_send.at[which, lax.rem(source, 2)],
                      z_recv.at[which, source, 0], ZPEER)

    def arrived(which, source, part):
        def act(n):
            block = place(which, source, half_span(which, y, part), core, n)
            remote(block, block, y_send.at[which, source, part or 0],
                   z_recv.at[which, source, part or 0], YPEER).wait_recv()
        sized(which, inner, act)

    def across(which, source, part, step):
        def act(n):
            half = 1 - y if step == "recv" else y
            block = place(which, source, half_span(which, half, part), core, n)
            copy = remote(block, block, y_send.at[which, source, part or 0],
                          y_recv.at[which, source, part or 0], YPEER)
            {"start": copy.start, "recv": copy.wait_recv, "send": copy.wait_send}[step]()
        sized(which, inner, act)

    def beside(which, source, half, step, mine=False):
        slot = 0 if half is None else half
        whose = 1 - core if step == "recv" else core

        def act(n):
            span = half_span(which, half)
            block = place(which, source, span, whose, n)
            start = held(which, span, inner, n) if mine else block
            copy = remote(start, block, d_send.at[which, source, slot],
                          d_recv.at[which, source, slot], SIB)
            {"start": copy.start, "recv": copy.wait_recv, "send": copy.wait_send}[step]()
        sized(which, inner, act)

    def keep(which, step):
        def act(n):
            span = half_span(which, None)
            copy = pltpu.make_async_copy(held(which, span, inner, n),
                                         place(which, z, span, core, n), own_sem.at[which])
            {"start": copy.start, "wait": copy.wait}[step]()
        sized(which, inner, act)

    def relay(which, source, only=None):
        for part in parts(which):
            if only is None or part == only:
                arrived(which, source, part)
                across(which, source, part, "start")

    def share(which, source):
        for part in parts(which):
            across(which, source, part, "recv")
        beside(which, source, None, "start")

    def feature_cols(owner):
        return pl.ds(at_least(owner * width, LANES), width)

    def token_rows(half):
        return pl.ds(at_least(half * rows, 16), rows)

    def stream_copy(number, device, half):
        return remote(stream.at[token_rows(half), :], rows_all.at[:, feature_cols(lane_id)],
                      in_send.at[number], in_recv.at[number], device)

    barrier = pltpu.get_barrier_semaphore()
    greeted = 0
    for device in (SIB, XPEER, XSIB, YPEER, ZPEER, {"fs": near}, {"fs": far}):
        pl.semaphore_signal(barrier, inc=1, device_id=device, device_id_type=MESH)
        greeted += 1
    pl.semaphore_wait(barrier, greeted)

    outer = jnp.logical_not(inner)
    z_start(IN, near)
    z_start(IN, peer)
    stream_copies = [stream_copy(0, XPEER, core), stream_copy(1, XSIB, 1 - core),
                     stream_copy(2, SIB, 1 - core)]
    for copy in stream_copies:
        copy.start()
    z_start(OUT, near)
    z_start(OUT, peer)
    keep(IN, "start")
    beside(IN, z, None, "start", mine=True)
    pool_copy = remote(pool_w, pool_sib, pool_send.at[0], pool_recv.at[0], SIB)
    scale_copy = remote(scale, scale_sib, pool_send.at[1], pool_recv.at[1], SIB)
    pool_copy.start()
    scale_copy.start()

    @pl.when(inner)
    def _():
        z_start(GATE, near)
        z_start(GATE, far)
        z_start(UP, near)

    @pl.when(outer)
    def _():
        z_start(GATE, peer)
        z_start(GATE, far)
        z_start(UP, far)
        z_start(UP, peer)

    for which in (OUT, GATE, UP, DOWN):
        keep(which, "start")
        for half in (0, 1) if which == DOWN else (None,):
            beside(which, z, half, "start", mine=True)

    rows_all[:, feature_cols(lane_id)] = stream[token_rows(core), :]

    def take(which):
        relay(which, peer)
        for source in (near, far):
            arrived(which, source, None)

            @pl.when(inner)
            def _():
                z_pass(which, source).start()
            across(which, source, None, "start")

    take(IN)

    @pl.when(inner)
    def _():
        take(OUT)

    def norm_into(source, gain, target, first, count):
        tile = 64

        def body(i, carry):
            at = pl.ds(at_least(first + i * tile, tile), tile)
            values = source[at, :].astype(f32)
            mean = jnp.mean(values * values, axis=-1, keepdims=True)
            target[at, :] = (values * lax.rsqrt(mean + EPSILON)
                             * gain[...].astype(f32).reshape(1, -1)).astype(bf16)
            return carry

        lax.fori_loop(0, count // tile, body, 0)

    for copy in stream_copies:
        copy.wait()
    norm_into(rows_all, mix_gain, normed, 0, rows)
    for source in (peer, near, far):
        share(IN, source)

    @pl.when(outer)
    def _():
        take(OUT)

    pool_copy.wait()
    scale_copy.wait()
    for source in (z, peer, near, far):
        beside(IN, source, None, "recv")
    keep(IN, "wait")

    local_groups, group_dim = pool_w.shape[0], pool_w.shape[1]
    at_row = lax.broadcasted_iota(jnp.int32, (SEQ, SEQ), 0)
    at_col = lax.broadcasted_iota(jnp.int32, (SEQ, SEQ), 1)
    pooled = jnp.dot(normed[...], in_all[...], preferred_element_type=f32).astype(bf16)
    for g in range(2 * local_groups):
        owner, place_in = divmod(g, local_groups)
        group = x * 2 * local_groups + g
        level = lax.div(4 * group, local_groups * tp)
        reach = jnp.int32(2)
        for bit in range(1, 4):
            reach = jnp.where(level >= bit, jnp.int32(2 << bit), reach)
        inside = jnp.where((at_col <= at_row) & (at_col > at_row - reach), 1.0, 0.0).astype(bf16)
        counts = jnp.minimum(at_row + 1, reach).astype(f32)[:, :1]
        is_own = core == owner
        cols = slice(g * group_dim, (g + 1) * group_dim)
        own_cols = slice(place_in * group_dim, (place_in + 1) * group_dim)
        weight = jnp.where(is_own, pool_w[place_in], pool_sib[place_in])
        factor = jnp.where(is_own, scale[own_cols].astype(f32).reshape(1, -1),
                           scale_sib[own_cols].astype(f32).reshape(1, -1))
        for s in range(rows // SEQ):
            at = slice(s * SEQ, (s + 1) * SEQ)
            part = pooled[at, cols]
            sums = jnp.dot(inside, part, preferred_element_type=f32)
            contrast = (sums / counts - part.astype(f32)).astype(bf16)
            mixed = jnp.dot(contrast, weight, preferred_element_type=f32)
            group_out[at, cols] = (mixed * factor).astype(bf16)

    for source in (peer, near, far):
        share(OUT, source)
    for source in (z, peer, near, far):
        beside(OUT, source, None, "recv")
    keep(OUT, "wait")

    def half_cols(owner):
        return pl.ds(at_least(owner * wide, LANES), wide)

    mix_send[...] = jnp.dot(group_out[...], out_all[:, half_cols(1 - x)],
                            preferred_element_type=f32).astype(bf16)
    mix_copy = remote(mix_send, mix_recv, mix_sems.at[0], mix_sems.at[1], XPEER)
    mix_copy.start()
    mix_own[...] = jnp.dot(group_out[...], out_all[:, half_cols(x)], preferred_element_type=f32)

    @pl.when(inner)
    def _():
        relay(GATE, peer)
        relay(GATE, near)

    @pl.when(outer)
    def _():
        relay(GATE, far)

    mix_copy.wait()
    mid_rows = pl.ds(at_least(seat * rows, 16), rows)
    mid_all[mid_rows, half_cols(x)] = (
        rows_all[:, half_cols(x)].astype(f32) + (mix_own[...] + mix_recv[...].astype(f32))).astype(bf16)

    def mid_copy(number, block, device):
        view = mid_all.at[pl.ds(at_least(block * rows, 16), rows), half_cols(x)]
        return remote(view, view, mid_send.at[number], mid_recv.at[number], device)

    to_pair, to_x, to_x_later = mid_copy(0, seat, ZPEER), mid_copy(1, seat, XPEER), mid_copy(2, 1 - seat, XPEER)
    to_pair.start()
    to_x.start()

    @pl.when(inner)
    def _():
        z_start(GATE, peer)
        z_start(UP, peer)
        z_start(DOWN, near, 0)
        z_start(UP, far)
        z_start(DOWN, far)
        z_start(DOWN, near, 1)
        share(GATE, peer)
        share(GATE, near)
        relay(UP, peer)
        relay(UP, near)

    @pl.when(outer)
    def _():
        z_start(GATE, near)
        z_start(UP, near)
        share(GATE, far)
        relay(UP, far)
        relay(GATE, near)

    to_pair.wait_recv()
    to_x_later.start()

    @pl.when(inner)
    def _():
        z_start(DOWN, peer)
        share(UP, peer)
        relay(DOWN, near, 0)

    @pl.when(outer)
    def _():
        z_start(DOWN, peer)
        z_start(DOWN, near)
        z_start(DOWN, far)
        share(UP, far)
        share(GATE, near)

    to_x.wait_recv()
    norm_into(mid_all, ffn_gain, normed_ffn, seat * rows, rows)

    @pl.when(inner)
    def _():
        share(UP, near)
        relay(GATE, far)

    @pl.when(outer)
    def _():
        relay(GATE, peer)

    to_x_later.wait_recv()
    norm_into(mid_all, ffn_gain, normed_ffn, (1 - seat) * rows, rows)

    depth = gate_all.shape[0] // 2
    pair_at = pl.ds(at_least(pair * depth, LANES), depth)
    cross_at = pl.ds(at_least((1 - pair) * depth, LANES), depth)
    early_at = pl.ds(at_least(jnp.where(inner, pair, 1 - pair) * depth, LANES), depth)
    later_at = pl.ds(at_least(jnp.where(inner, 1 - pair, pair) * depth, LANES), depth)
    tile = rows

    def by_tiles(body):
        def all_tiles(count):
            wide_units = 2 * count * LANES

            def step(i, carry):
                body(pl.ds(at_least(i * tile, tile), tile), wide_units)
                return carry
            lax.fori_loop(0, 2 * rows // tile, step, 0)
        sized(UP, inner, all_tiles)

    def partial_dot(at, depth_at, weights, n):
        return jnp.dot(normed_ffn[at, depth_at], weights[depth_at, :n], preferred_element_type=f32)

    def gate_first(at, n):
        gate_acts[at, :n] = partial_dot(at, early_at, gate_all, n)

    def gate_second(at, n):
        gate = gate_acts[at, :n] + partial_dot(at, later_at, gate_all, n)
        gate_acts[at, :n] = gate / (1.0 + jnp.exp(-gate))

    def up_first(at, n):
        up_acts[at, :n] = partial_dot(at, pair_at, up_all, n)

    def up_second(at, n):
        up = up_acts[at, :n] + partial_dot(at, cross_at, up_all, n)
        hidden[at, :n] = (gate_acts[at, :n] * up).astype(bf16)

    keep(GATE, "wait")
    for source in (jnp.where(inner, z, far), jnp.where(inner, peer, near)):
        beside(GATE, source, None, "recv")
    by_tiles(gate_first)

    @pl.when(inner)
    def _():
        relay(UP, far)
        share(GATE, far)

    @pl.when(outer)
    def _():
        relay(UP, peer)
        share(GATE, peer)

    for source in (jnp.where(inner, near, z), jnp.where(inner, far, peer)):
        beside(GATE, source, None, "recv")
    by_tiles(gate_second)

    @pl.when(outer)
    def _():
        share(UP, peer)
        relay(UP, near)

    keep(UP, "wait")
    for source in (z, peer):
        beside(UP, source, None, "recv")
    by_tiles(up_first)
    relay(DOWN, peer)

    @pl.when(inner)
    def _():
        share(UP, far)

    @pl.when(outer)
    def _():
        share(UP, near)

    beside(DOWN, peer, y, "start")
    for source in (near, far):
        beside(UP, source, None, "recv")
    by_tiles(up_second)

    sub = width // 2
    order = (z, peer, far, near)
    keeps_early = x == pair

    def is_kept(o):
        return keeps_early if o < 2 else jnp.logical_not(keeps_early)

    def half_of(turn):
        return y if turn == 0 else 1 - y

    def column_block(o, turn, n):
        at = pl.ds(at_least(order[o] * width + half_of(turn) * sub, LANES), sub)
        slot = 2 * (o % 2) + turn
        values = jnp.dot(hidden[:, :n], down_all[:n, at], preferred_element_type=f32)

        @pl.when(is_kept(o))
        def _():
            ffn_own[slot] = values

        @pl.when(jnp.logical_not(is_kept(o)))
        def _():
            ffn_send[slot] = values.astype(bf16)
            x_copy(slot, 0).start()
            x_copy(slot, 1).start()

    def x_copy(slot, ours):
        at = pl.ds(at_least((seat if ours else 1 - seat) * rows, 16), rows)
        return remote(ffn_send.at[slot, at, :], ffn_recv.at[slot, at, :],
                      x_send.at[slot, ours], x_recv.at[slot, ours], XPEER)

    def pair_copy(o, turn):
        quarter, half = lax.rem(order[o], 2), half_of(turn)
        return remote(pair_send.at[quarter, half], pair_recv.at[quarter, half],
                      p_send.at[quarter, half], p_recv.at[quarter, half], ZPEER)

    def fold(o, turn):
        slot = 2 * (o % 2) + turn
        quarter, half = lax.rem(order[o], 2), half_of(turn)

        @pl.when(is_kept(o))
        def _():
            x_copy(slot, 0).wait_recv()
            theirs = pl.ds(at_least((1 - seat) * rows, 16), rows)
            pair_send[quarter, half] = (ffn_own[slot, theirs, :]
                                        + ffn_recv[slot, theirs, :].astype(f32)).astype(bf16)
            pair_copy(o, turn).start()

    def last_copy(half):
        return remote(last_send.at[half], last_recv.at[half], l_send.at[half], l_recv.at[half], SIB)

    def settle(o, turn):
        slot = 2 * (o % 2) + turn
        quarter, half = lax.rem(order[o], 2), half_of(turn)

        @pl.when(is_kept(o))
        def _():
            x_copy(slot, 1).wait_recv()
            pair_copy(o, turn).wait_recv()
            ours = pl.ds(at_least(seat * rows, 16), rows)
            cols = pl.ds(at_least(order[o] * width + half * sub, LANES), sub)
            total = (ffn_own[slot, ours, :] + ffn_recv[slot, ours, :].astype(f32)
                     + pair_recv[quarter, half].astype(f32))
            value = (mid_all[ours, cols].astype(f32) + total).astype(bf16)

            @pl.when(quarter == core)
            def _():
                result[token_rows(core), pl.ds(at_least(half * sub, LANES), sub)] = value

            @pl.when(quarter != core)
            def _():
                last_send[half] = value
                last_copy(half).start()

    def pour(source):
        for part in parts(DOWN):
            across(DOWN, source, part, "recv")
        beside(DOWN, source, 1 - y, "start")

    def ready(source, turn):
        beside(DOWN, source, half_of(turn), "recv")

    OWN, PEER, FAR, NEAR = range(4)

    def bring(o, only=None):
        relay(DOWN, order[o], only)
        beside(DOWN, order[o], y, "start")

    def block(o, turn, count):
        ready(order[o], turn)
        column_block(o, turn, 2 * count * LANES)

    keep(DOWN, "wait")

    @pl.when(outer)
    def _():
        block(OWN, 0, few)
        block(OWN, 1, few)
        block(PEER, 0, few)
        pour(peer)
        bring(FAR)
        block(PEER, 1, few)
        block(FAR, 0, few)
        fold(OWN, 0)
        bring(NEAR)
        pour(far)
        block(FAR, 1, few)
        block(NEAR, 0, few)
        fold(OWN, 1)
        fold(PEER, 0)
        pour(near)
        block(NEAR, 1, few)

    @pl.when(inner)
    def _():
        block(OWN, 0, many)
        block(OWN, 1, many)
        block(PEER, 0, many)
        bring(FAR)
        pour(peer)
        block(PEER, 1, many)
        block(FAR, 0, many)
        fold(OWN, 0)
        pour(far)
        block(FAR, 1, many)
        bring(NEAR, 1)
        fold(OWN, 1)
        block(NEAR, 0, many)
        fold(PEER, 0)
        pour(near)
        block(NEAR, 1, many)

    fold(FAR, 0)
    fold(FAR, 1)
    fold(PEER, 1)
    fold(NEAR, 0)
    for o in (OWN, PEER):
        for turn in (0, 1):
            settle(o, turn)
    for turn in (0, 1):
        settle(FAR, turn)
    fold(NEAR, 1)
    for turn in (0, 1):
        settle(NEAR, turn)

    for half in (0, 1):
        last_copy(half).wait()
        result[token_rows(1 - core), half * sub:(half + 1) * sub] = last_recv[half]

    for which in range(5):
        z_sent(which, peer)
        z_sent(which, near)
        if which not in (IN, OUT):
            z_sent(which, far)
        else:
            @pl.when(inner)
            def _():
                for source in (near, far):
                    z_pass(which, source).wait_send()
        for source in (peer, near, far):
            for part in parts(which):
                across(which, source, part, "send")
        for source in order:
            for half in (0, 1) if which == DOWN else (None,):
                beside(which, source, half, "send", mine=False)
    for copy in (to_pair, to_x, to_x_later):
        copy.wait_send()
    for slot in range(4):
        for ours in (0, 1):
            x_copy(slot, ours).wait_send()
    for quarter in (0, 1):
        for half in (0, 1):
            remote(pair_send.at[quarter, half], pair_recv.at[quarter, half],
                   p_send.at[quarter, half], p_recv.at[quarter, half], ZPEER).wait_send()


def pairs_fit(sizes, stream, in_weight, pool_weight, out_weight, gate_weight, down_weight):
    reps, fs, tp = sizes
    tokens, width = stream.shape
    return (reps == 2 and fs == 4 and tp == 4 and tokens % (2 * SEQ) == 0
            and width % (2 * LANES) == 0 and gate_weight.shape[1] % LANES == 0
            and in_weight.shape[1] % LANES == 0 and in_weight.shape[0] % 32 == 0
            and out_weight.shape[0] % 32 == 0 and gate_weight.shape[0] % 32 == 0
            and down_weight.shape[1] == width)


def pair_on_device(sizes, stream, in_weight, pool_weight, pool_scale, out_weight,
                   mix_gain, ffn_gain, gate_weight, up_weight, down_weight):
    if not pairs_fit(sizes, stream, in_weight, pool_weight, out_weight, gate_weight, down_weight):
        return ring_on_device(sizes, stream, in_weight, pool_weight, pool_scale, out_weight,
                              mix_gain, ffn_gain, gate_weight, up_weight, down_weight)
    reps, fs, tp = sizes
    tokens, width = stream.shape
    rows, sub = tokens // 2, width // 2
    features = width * tp
    channels = in_weight.shape[1]
    blocks = gate_weight.shape[1] // LANES
    units = 2 * LANES * (blocks - blocks // 2)
    bf, f32 = jnp.bfloat16, jnp.float32
    vmem = pl.BlockSpec(memory_space=pltpu.VMEM)
    hbm = pl.BlockSpec(memory_space=pl.ANY)
    dma = pltpu.SemaphoreType.DMA
    flops = 2 * tokens * (2 * features * channels + 3 * features * gate_weight.shape[1])
    return pl.pallas_call(
        functools.partial(pair_kernel, sizes),
        out_shape=jax.ShapeDtypeStruct(stream.shape, bf),
        in_specs=[vmem] + [hbm] * 5 + [vmem] * 4,
        out_specs=vmem,
        scratch_shapes=[
            pltpu.VMEM((in_weight.shape[0] * fs, 2 * channels), bf),
            pltpu.VMEM((2 * out_weight.shape[0], out_weight.shape[1] * fs), bf),
            pltpu.VMEM((up_weight.shape[0] * fs, units), bf),
            pltpu.VMEM((gate_weight.shape[0] * fs, units), bf),
            pltpu.VMEM((units, down_weight.shape[1] * fs), bf),
            pltpu.VMEM((rows, features), bf),
            pltpu.VMEM((rows, features), bf),
            pltpu.VMEM((rows, 2 * channels), bf),
            pltpu.VMEM((2 * rows, units), bf),
            pltpu.VMEM((2 * rows, units), f32),
            pltpu.VMEM((2 * rows, units), f32),
            pltpu.VMEM((2 * rows, features), bf),
            pltpu.VMEM((2 * rows, features), bf),
            pltpu.VMEM(pool_weight.shape, bf),
            pltpu.VMEM((channels,), bf),
            pltpu.VMEM((rows, 2 * width), f32),
            pltpu.VMEM((rows, 2 * width), bf),
            pltpu.VMEM((rows, 2 * width), bf),
            pltpu.VMEM((4, 2 * rows, sub), f32),
            pltpu.VMEM((4, 2 * rows, sub), bf),
            pltpu.VMEM((4, 2 * rows, sub), bf),
            pltpu.VMEM((2, 2, rows, sub), bf),
            pltpu.VMEM((2, 2, rows, sub), bf),
            pltpu.VMEM((2, rows, sub), bf),
            pltpu.VMEM((2, rows, sub), bf),
            dma((5, fs, 2)), dma((5, fs, 2)), dma((2, 2)), dma((5, fs, 2)), dma((5, fs, 2)),
            dma((5, fs, 2)), dma((5, fs, 2)), dma((5,)),
            dma((3,)), dma((3,)), dma((2,)), dma((2,)), dma((2,)), dma((3,)), dma((3,)),
            dma((4, 2)), dma((4, 2)), dma((2, 2)), dma((2, 2)), dma((2,)), dma((2,)),
        ],
        compiler_params=pltpu.CompilerParams(
            collective_id=0, has_side_effects=True, vmem_limit_bytes=64 * 1024 * 1024 - 65536),
        cost_estimate=pl.CostEstimate(flops=flops, bytes_accessed=flops // 512, transcendentals=0),
    )(stream, in_weight, out_weight, up_weight, gate_weight, down_weight, pool_weight,
      pool_scale, mix_gain, ffn_gain)


def solution(mesh):
    sizes = tuple(mesh.shape[name] for name in ("rep", "fs", "tp"))
    return jax.shard_map(
        functools.partial(pair_on_device, sizes),
        mesh=mesh,
        in_specs=(
            P(("rep", "fs"), "tp"),
            P("fs", "tp"),
            P("tp", None, None),
            P("tp"),
            P("tp", "fs"),
            P(),
            P(),
            P("fs", "tp"),
            P("fs", "tp"),
            P("tp", "fs"),
        ),
        out_specs=P(("rep", "fs"), "tp"),
        check_vma=False,
    )
```

```python
import functools

import jax
import jax.numpy as jnp
from jax import lax
from jax.experimental import pallas as pl
from jax.experimental.pallas import tpu as pltpu
from jax.sharding import PartitionSpec as P

SEQ = 128
EPSILON = 1e-06
MESH = pl.DeviceIdType.MESH
BY_ROWS = (True, False, True, True, False)
PIECES = ((0, 0), (1, 0), (2, 0), (3, 0), (2, 1), (3, 1), (4, 0), (4, 1))
CHUNKS = (1, 1, 2, 2, 2)


def ring_kernel(sizes, stream, in_w, out_w, up_w, gate_w, down_w, pool_w, scale,
           mix_gain, ffn_gain, result,
           in_all, out_all, up_all, gate_all, down_all,
           rows_all, normed, group_out, hidden, middle, mid_all,
           mix_send, mix_recv, ffn_send, ffn_recv,
           ring_send, ring_recv, fwd_send, fwd_recv, own_sem,
           tp_send, tp_recv, keep_sem):
    reps, fs, tp = sizes
    half = fs // 2
    my_rep, me, my_tp = lax.axis_index("rep"), lax.axis_index("fs"), lax.axis_index("tp")
    own = (in_w, out_w, up_w, gate_w, down_w)
    full = (in_all, out_all, up_all, gate_all, down_all)
    tokens, width = stream.shape

    def turn(at, by, count):
        return lax.rem(at + by + count, count)

    def piece(which, owner, row, count):
        block_rows, block_cols = own[which].shape
        if BY_ROWS[which]:
            return full[which].at[pl.ds(pl.multiple_of(owner * block_rows + row, 16), count), :]
        return full[which].at[pl.ds(pl.multiple_of(row, 16), count),
                              pl.ds(pl.multiple_of(owner * block_cols, 128), block_cols)]

    def span(number, step, way):
        which, chunk = PIECES[number]
        rows = own[which].shape[0]
        cut = rows % (CHUNKS[which] * reps * 2 * 16) == 0
        count = rows // CHUNKS[which] if cut else (rows, 0)[chunk]
        row = chunk * (rows // CHUNKS[which])
        count = count // reps
        row = row + my_rep * count
        if step == half:
            count = count // 2
            row = row + way * count
        return which, row, count

    def empty(number):
        return span(number, 1, 0)[2] == 0

    def ring(number, step, way):
        which, row, count = span(number, step, way)
        sign = 1 - 2 * way
        owner = turn(me, -sign * (step - 1), fs)
        if step == 1:
            source = own[which].at[pl.ds(pl.multiple_of(row, 16), count), :]
        else:
            source = piece(which, owner, row, count)
        return pltpu.make_async_remote_copy(
            src_ref=source, dst_ref=piece(which, owner, row, count),
            send_sem=ring_send.at[number, step - 1, way],
            recv_sem=ring_recv.at[number, step - 1, way],
            device_id={"fs": turn(me, sign, fs)}, device_id_type=MESH)

    def forward(number, step, way, peer):
        which, row, count = span(number, step, way)
        block = piece(which, turn(me, -(1 - 2 * way) * step, fs), row, count)
        return pltpu.make_async_remote_copy(
            src_ref=block, dst_ref=block,
            send_sem=fwd_send.at[number, peer - 1, step - 1, way],
            recv_sem=fwd_recv.at[number, peer - 1, step - 1, way],
            device_id={"rep": turn(my_rep, peer, reps)}, device_id_type=MESH)

    def begin(*numbers):
        for number in numbers:
            if not empty(number):
                for way in (0, 1):
                    ring(number, 1, way).start()

    def advance(number, step):
        if empty(number):
            return
        for way in (0, 1):
            ring(number, step, way).wait_recv()
            if step < half:
                ring(number, step + 1, way).start()
            for peer in range(1, reps):
                forward(number, step, way, peer).start()

    def early(*numbers):
        for number in numbers:
            for step in range(1, half):
                advance(number, step)

    def late(*numbers):
        for number in numbers:
            advance(number, half)

    def arrived(*numbers):
        for number in numbers:
            if PIECES[number][1] == 0:
                keeps[PIECES[number][0]].wait()
            if empty(number):
                continue
            for step in range(1, half + 1):
                for way in (0, 1):
                    for peer in range(1, reps):
                        forward(number, step, way, peer).wait()

    def tp_copy(stage, offset, source, target):
        return pltpu.make_async_remote_copy(
            src_ref=source, dst_ref=target,
            send_sem=tp_send.at[stage, offset - 1], recv_sem=tp_recv.at[stage, offset - 1],
            device_id={"tp": turn(my_tp, offset, tp)}, device_id_type=MESH)

    def feature_cols(owner):
        return pl.ds(pl.multiple_of(owner * width, 128), width)

    barrier = pltpu.get_barrier_semaphore()
    greeted = 0
    for name, at, count, offsets in (
            ("fs", me, fs, (1, -1)),
            ("tp", my_tp, tp, range(1, tp)),
            ("rep", my_rep, reps, range(1, reps))):
        for offset in offsets:
            pl.semaphore_signal(barrier, inc=1, device_id={name: turn(at, offset, count)},
                                device_id_type=MESH)
            greeted += 1
    pl.semaphore_wait(barrier, greeted)

    begin(0, 1)
    stream_sends = []
    for offset in range(1, tp):
        copy = tp_copy(0, offset, stream, rows_all.at[:, feature_cols(my_tp)])
        copy.start()
        stream_sends.append(copy)
    keeps = []
    for which in range(len(own)):
        keep = pltpu.make_async_copy(
            own[which], piece(which, me, 0, own[which].shape[0]), own_sem.at[which])
        keep.start()
        keeps.append(keep)
    keep_stream = pltpu.make_async_copy(
        stream, rows_all.at[:, feature_cols(my_tp)], keep_sem)
    keep_stream.start()
    early(0, 1)
    begin(2, 3, 4)
    late(0, 1)

    def norm_into(source, gain, target):
        tile = 64

        def body(i, carry):
            at = pl.ds(pl.multiple_of(i * tile, tile), tile)
            wide = source[at, :].astype(jnp.float32)
            mean = jnp.mean(wide * wide, axis=-1, keepdims=True)
            target[at, :] = (wide * lax.rsqrt(mean + EPSILON)
                             * gain[...].astype(jnp.float32)).astype(jnp.bfloat16)
            return carry

        lax.fori_loop(0, tokens // tile, body, 0)

    keep_stream.wait()
    for copy in stream_sends:
        copy.wait()
    norm_into(rows_all, mix_gain, normed)
    arrived(0)

    local_groups, group_dim = pool_w.shape[0], pool_w.shape[1]
    at_row = lax.broadcasted_iota(jnp.int32, (SEQ, SEQ), 0)
    at_col = lax.broadcasted_iota(jnp.int32, (SEQ, SEQ), 1)
    insides, inverses = [], []
    for g in range(local_groups):
        group = my_tp * local_groups + g
        level = lax.div(4 * group, local_groups * tp)
        reach = jnp.int32(2)
        for bit in range(1, 4):
            reach = jnp.where(level >= bit, jnp.int32(2 << bit), reach)
        inside = (at_col <= at_row) & (at_col > at_row - reach)
        insides.append(jnp.where(inside, 1.0, 0.0).astype(jnp.bfloat16))
        inverses.append(jnp.minimum(at_row + 1, reach).astype(jnp.float32)[:, :1])

    def mix(i, carry):
        at = pl.ds(pl.multiple_of(i * SEQ, SEQ), SEQ)
        pooled = jnp.dot(normed[at, :], in_all[...],
                         preferred_element_type=jnp.float32).astype(jnp.bfloat16)
        for g in range(local_groups):
            cols = slice(g * group_dim, (g + 1) * group_dim)
            part = pooled[:, cols]
            sums = jnp.dot(insides[g], part, preferred_element_type=jnp.float32)
            contrast = (sums / inverses[g] - part.astype(jnp.float32)).astype(jnp.bfloat16)
            mixed = jnp.dot(contrast, pool_w[g], preferred_element_type=jnp.float32)
            group_out[at, cols] = (mixed * scale[:, cols].astype(jnp.float32)).astype(jnp.bfloat16)
        return carry

    lax.fori_loop(0, tokens // SEQ, mix, 0)

    arrived(1)
    early(2)

    def spread(operand, weights, stage, sends, tile):
        def block(owner, target):
            def body(i, carry):
                at = pl.ds(pl.multiple_of(i * tile, tile), tile)
                target[at, :] = jnp.dot(operand[at, :], weights[:, feature_cols(owner)],
                                        preferred_element_type=jnp.float32).astype(jnp.bfloat16)
                return carry
            lax.fori_loop(0, tokens // tile, body, 0)

        copies = []
        recv = mix_recv if stage == 1 else ffn_recv
        for offset in sorted(range(1, tp), key=lambda o: -min(o, tp - o)):
            block(turn(my_tp, offset, tp), sends.at[offset - 1])
            copy = tp_copy(stage, offset, sends.at[offset - 1], recv.at[offset - 1])
            copy.start()
            copies.append(copy)
        block(my_tp, sends.at[tp - 1])
        return copies

    def gather_sum(base, recv, sends, target):
        tile = 64

        def body(i, carry):
            at = pl.ds(pl.multiple_of(i * tile, tile), tile)
            total = sends[tp - 1, at, :].astype(jnp.float32)
            for k in range(tp - 1):
                total = total + recv[k, at, :].astype(jnp.float32)
            target[at, :] = (base[at, :].astype(jnp.float32) + total).astype(jnp.bfloat16)
            return carry

        lax.fori_loop(0, tokens // tile, body, 0)

    mix_copies = spread(group_out, out_all, 1, mix_send, tokens // 2)
    early(3)
    begin(5)
    for copy in mix_copies:
        copy.wait()
    gather_sum(stream, mix_recv, mix_send, middle)
    keep_middle = pltpu.make_async_copy(middle, mid_all.at[:, feature_cols(my_tp)], keep_sem)
    keep_middle.start()
    middle_copies = []
    for offset in range(1, tp):
        copy = tp_copy(2, offset, middle, mid_all.at[:, feature_cols(my_tp)])
        copy.start()
        middle_copies.append(copy)
    early(4)
    begin(6, 7)
    late(2, 3)
    keep_middle.wait()
    for copy in middle_copies:
        copy.wait()
    norm_into(mid_all, ffn_gain, normed)
    early(5)
    late(4)
    early(6)
    late(5)
    early(7)
    late(6)
    arrived(2, 3, 4, 5)
    tile = tokens // 2

    def gated(i, carry):
        at = pl.ds(pl.multiple_of(i * tile, tile), tile)
        values = normed[at, :]
        gate = jnp.dot(values, gate_all[...], preferred_element_type=jnp.float32)
        up = jnp.dot(values, up_all[...], preferred_element_type=jnp.float32)
        hidden[at, :] = (gate / (1.0 + jnp.exp(-gate)) * up).astype(jnp.bfloat16)
        return carry

    lax.fori_loop(0, tokens // tile, gated, 0)
    late(7)
    arrived(6, 7)
    ffn_copies = spread(hidden, down_all, 3, ffn_send, tokens // 2)
    for number in range(len(PIECES)):
        if not empty(number):
            for step in range(1, half + 1):
                for way in (0, 1):
                    ring(number, step, way).wait_send()
    for copy in ffn_copies:
        copy.wait()
    gather_sum(middle, ffn_recv, ffn_send, result)


def ring_on_device(sizes, stream, in_weight, pool_weight, pool_scale, out_weight,
              mix_gain, ffn_gain, gate_weight, up_weight, down_weight):
    reps, fs, tp = sizes
    half = fs // 2
    tokens, width = stream.shape
    features = width * tp
    own = (in_weight, out_weight, up_weight, gate_weight, down_weight)
    full = [pltpu.VMEM((w.shape[0] * fs, w.shape[1]) if by_rows else (w.shape[0], w.shape[1] * fs),
                       jnp.bfloat16) for w, by_rows in zip(own, BY_ROWS)]
    units = gate_weight.shape[1]
    bf = jnp.bfloat16
    vmem = pl.BlockSpec(memory_space=pltpu.VMEM)
    hbm = pl.BlockSpec(memory_space=pl.ANY)
    dma = pltpu.SemaphoreType.DMA
    flops = 2 * tokens * (2 * features * in_weight.shape[1] + 3 * features * units)
    return pl.pallas_call(
        functools.partial(ring_kernel, sizes),
        out_shape=jax.ShapeDtypeStruct(stream.shape, bf),
        in_specs=[vmem] + [hbm] * 5 + [vmem] * 4,
        out_specs=vmem,
        scratch_shapes=full + [
            pltpu.VMEM((tokens, features), bf),
            pltpu.VMEM((tokens, features), bf),
            pltpu.VMEM((tokens, in_weight.shape[1]), bf),
            pltpu.VMEM((tokens, units), bf),
            pltpu.VMEM((tokens, width), bf),
            pltpu.VMEM((tokens, features), bf),
            pltpu.VMEM((tp, tokens, width), bf),
            pltpu.VMEM((tp - 1, tokens, width), bf),
            pltpu.VMEM((tp, tokens, width), bf),
            pltpu.VMEM((tp - 1, tokens, width), bf),
            dma((len(PIECES), half, 2)),
            dma((len(PIECES), half, 2)),
            dma((len(PIECES), max(reps - 1, 1), half, 2)),
            dma((len(PIECES), max(reps - 1, 1), half, 2)),
            dma((len(own),)),
            dma((4, tp - 1)),
            dma((4, tp - 1)),
            dma(()),
        ],
        compiler_params=pltpu.CompilerParams(
            collective_id=0, has_side_effects=True, vmem_limit_bytes=64 * 1024 * 1024 - 65536),
        cost_estimate=pl.CostEstimate(flops=flops, bytes_accessed=flops // 512, transcendentals=0),
    )(stream, in_weight, out_weight, up_weight, gate_weight, down_weight, pool_weight,
      pool_scale.reshape(1, -1), mix_gain.reshape(1, -1), ffn_gain.reshape(1, -1))


IN, OUT, UP, GATE, DOWN = range(5)
LANES = 128


def pair_kernel(sizes, stream, in_w, out_w, up_w, gate_w, down_w, pool_w, scale,
                mix_gain, ffn_gain, result,
                in_all, out_all, up_all, gate_all, down_all,
                rows_all, normed, group_out, hidden, gate_acts, up_acts, mid_all, normed_ffn,
                pool_sib, scale_sib,
                mix_own, mix_send, mix_recv, ffn_own, ffn_send, ffn_recv, pair_send, pair_recv,
                stage, cross_send, cross_recv, cross_own, late_send, late_recv,
                last_send, last_recv,
                z_send, z_recv, pass_send, y_send, y_recv, d_send, d_recv, own_sem,
                in_send, in_recv, pool_send, pool_recv, mix_sems, mid_send, mid_recv,
                x_send, x_recv, p_send, p_recv, l_send, l_recv, c_send, c_recv, late_sems):
    reps, fs, tp = sizes
    y, z, lane_id = lax.axis_index("rep"), lax.axis_index("fs"), lax.axis_index("tp")
    x, core = lax.div(lane_id, 2), lax.rem(lane_id, 2)
    own = (in_w, out_w, up_w, gate_w, down_w)
    full = (in_all, out_all, up_all, gate_all, down_all)
    tokens, width = stream.shape
    rows = tokens // 2
    wide = 2 * width
    seat, pair = lax.rem(z, 2), lax.div(z, 2)
    peer = z + 1 - 2 * seat
    near = jnp.where(pair == 0, 2, 1)
    far = jnp.where(pair == 0, 3, 0)
    inner = (z == 1) | (z == 2)
    f32, bf16 = jnp.float32, jnp.bfloat16

    blocks = gate_w.shape[1] // LANES
    few, many = blocks // 2, blocks - blocks // 2

    SIB = {"tp": lane_id + 1 - 2 * core}
    XPEER = {"tp": lane_id + 2 - 4 * x}
    XSIB = {"tp": 2 * (1 - x) + 1 - core}
    YPEER = {"rep": 1 - y}
    ZPEER = {"fs": peer}

    def at_least(value, multiple):
        return pl.multiple_of(value, multiple)

    def remote(source, target, send, recv, device):
        return pltpu.make_async_remote_copy(
            src_ref=source, dst_ref=target, send_sem=send, recv_sem=recv,
            device_id=device, device_id_type=MESH)

    def sized(which, roomy, act):
        if which in (IN, OUT) or few == many:
            act(many)
            return

        @pl.when(roomy)
        def _():
            act(many)

        @pl.when(jnp.logical_not(roomy))
        def _():
            act(few)

    slot_of = {IN: 0, OUT: 1, GATE: 2, UP: 3, DOWN: 5}

    def role_of(source):
        return jnp.where(source == peer, 0, jnp.where(source == near, 1,
                         jnp.where(source == far, 2, 3)))

    def flow(which, part, role):
        return 3 * (slot_of[which] + (part or 0)) + role

    def beside_flow(which, source, half, part):
        if which != DOWN:
            return 4 * (IN, OUT, GATE, UP).index(which) + role_of(source)
        if source is z:
            return 16 + half
        return 18 + 3 * role_of(source) + (0 if part is None else 1 + part)

    def extent(which):
        return own[which].shape[1 if which == DOWN else 0]

    def half_span(which, half, part=None):
        size = extent(which) // 2
        if half is None:
            return 0, 2 * size
        if part is None:
            return half * size, size
        return half * size + part * (size // 2), size // 2

    def parts(which):
        return (0, 1) if which in (UP, DOWN) else (None,)

    def place(which, source, span, core_at, count):
        block_rows, block_cols = own[which].shape
        ref = full[which]
        start, size = span
        if which == OUT:
            return ref.at[pl.ds(at_least(core_at * block_rows + start, 16), size),
                          pl.ds(at_least(source * block_cols, LANES), block_cols)]
        if which == IN:
            return ref.at[pl.ds(at_least(source * block_rows + start, 16), size),
                          pl.ds(at_least(core_at * block_cols, LANES), block_cols)]
        first = core_at * (count * LANES)
        if which == DOWN:
            return ref.at[pl.ds(at_least(first, LANES), count * LANES),
                          pl.ds(at_least(source * block_cols + start, LANES), size)]
        return ref.at[pl.ds(at_least(source * block_rows + start, 16), size),
                      pl.ds(at_least(first, LANES), count * LANES)]

    def held(which, span, roomy, count):
        ref = own[which]
        start, size = span
        if which in (IN, OUT):
            return ref.at[pl.ds(at_least(start, 16), size), :]
        first = jnp.where(roomy, 0, many * LANES)
        if which == DOWN:
            return ref.at[pl.ds(at_least(first, LANES), count * LANES),
                          pl.ds(at_least(start, LANES), size)]
        return ref.at[pl.ds(at_least(start, 16), size),
                      pl.ds(at_least(first, LANES), count * LANES)]

    def z_copies(which, dest, step, only=None):
        roomy = (dest == 1) | (dest == 2)

        def act(n):
            for part in parts(which) if only is None else (only,):
                span = half_span(which, y, part)
                there = jnp.where(dest == peer, 0, jnp.where(inner, 1, 2))
                copy = remote(held(which, span, roomy, n), place(which, z, span, core, n),
                              z_send.at[flow(which, part, role_of(dest))],
                              z_recv.at[flow(which, part, there)], {"fs": dest})
                {"start": copy.start, "send": copy.wait_send}[step]()
        sized(which, roomy, act)

    def z_start(which, dest, only=None):
        z_copies(which, dest, "start", only)

    def z_sent(which, dest):
        z_copies(which, dest, "send")

    def z_pass(which, source):
        block = place(which, source, half_span(which, y), core, many)
        return remote(block, block, pass_send.at[which, lax.rem(source, 2)],
                      z_recv.at[flow(which, None, role_of(source))], ZPEER)

    def arrived(which, source, part):
        def act(n):
            block = place(which, source, half_span(which, y, part), core, n)
            at = flow(which, part, role_of(source))
            remote(block, block, y_send.at[at], z_recv.at[at], YPEER).wait_recv()
        sized(which, inner, act)

    def across(which, source, part, step):
        def act(n):
            half = 1 - y if step == "recv" else y
            block = place(which, source, half_span(which, half, part), core, n)
            at = flow(which, part, role_of(source))
            copy = remote(block, block, y_send.at[at], y_recv.at[at], YPEER)
            {"start": copy.start, "recv": copy.wait_recv, "send": copy.wait_send}[step]()
        sized(which, inner, act)

    def beside(which, source, half, step, mine=False, part=None):
        at = beside_flow(which, source, half, part)
        whose = 1 - core if step == "recv" else core

        def act(n):
            span = half_span(which, half, part)
            block = place(which, source, span, whose, n)
            start = held(which, span, inner, n) if mine else block
            copy = remote(start, block, d_send.at[at], d_recv.at[at], SIB)
            {"start": copy.start, "recv": copy.wait_recv, "send": copy.wait_send}[step]()
        sized(which, inner, act)

    def keep(which, step):
        def act(n):
            span = half_span(which, None)
            copy = pltpu.make_async_copy(held(which, span, inner, n),
                                         place(which, z, span, core, n), own_sem.at[which])
            {"start": copy.start, "wait": copy.wait}[step]()
        sized(which, inner, act)

    def relay(which, source, only=None):
        for part in parts(which):
            if only is None or part == only:
                arrived(which, source, part)
                across(which, source, part, "start")

    def share(which, source):
        for part in parts(which):
            across(which, source, part, "recv")
        beside(which, source, None, "start")

    def feature_cols(owner):
        return pl.ds(at_least(owner * width, LANES), width)

    def token_rows(half):
        return pl.ds(at_least(half * rows, 16), rows)

    def stream_copy(number, device, half):
        return remote(stream.at[token_rows(half), :], rows_all.at[:, feature_cols(lane_id)],
                      in_send.at[number], in_recv.at[number], device)

    barrier = pltpu.get_barrier_semaphore()
    greeted = 0
    for device in (SIB, XPEER, XSIB, YPEER, ZPEER, {"fs": near}, {"fs": far}):
        pl.semaphore_signal(barrier, inc=1, device_id=device, device_id_type=MESH)
        greeted += 1
    pl.semaphore_wait(barrier, greeted)

    outer = jnp.logical_not(inner)
    z_start(IN, near)
    z_start(IN, peer)
    stream_copies = [stream_copy(0, XPEER, core), stream_copy(1, XSIB, 1 - core),
                     stream_copy(2, SIB, 1 - core)]
    for copy in stream_copies:
        copy.start()
    z_start(OUT, near)
    z_start(OUT, peer)
    keep(IN, "start")
    beside(IN, z, None, "start", mine=True)
    pool_copy = remote(pool_w, pool_sib, pool_send.at[0], pool_recv.at[0], SIB)
    scale_copy = remote(scale, scale_sib, pool_send.at[1], pool_recv.at[1], SIB)
    pool_copy.start()
    scale_copy.start()

    @pl.when(inner)
    def _():
        z_start(GATE, near)
        z_start(GATE, far)
        z_start(UP, near)

    @pl.when(outer)
    def _():
        z_start(GATE, peer)
        z_start(GATE, far)
        z_start(UP, far)
        z_start(UP, peer)

    for which in (OUT, GATE, UP, DOWN):
        keep(which, "start")
        for half in (0, 1) if which == DOWN else (None,):
            beside(which, z, half, "start", mine=True)

    rows_all[:, feature_cols(lane_id)] = stream[token_rows(core), :]

    def take(which):
        relay(which, peer)
        for source in (near, far):
            arrived(which, source, None)

            @pl.when(inner)
            def _():
                z_pass(which, source).start()
            across(which, source, None, "start")

    take(IN)

    @pl.when(inner)
    def _():
        take(OUT)

    def norm_into(source, gain, target, first, count):
        tile = 64

        def body(i, carry):
            at = pl.ds(at_least(first + i * tile, tile), tile)
            values = source[at, :].astype(f32)
            mean = jnp.mean(values * values, axis=-1, keepdims=True)
            target[at, :] = (values * lax.rsqrt(mean + EPSILON)
                             * gain[...].astype(f32).reshape(1, -1)).astype(bf16)
            return carry

        lax.fori_loop(0, count // tile, body, 0)

    for copy in stream_copies:
        copy.wait()
    norm_into(rows_all, mix_gain, normed, 0, rows)
    for source in (peer, near, far):
        share(IN, source)

    @pl.when(outer)
    def _():
        take(OUT)

    pool_copy.wait()
    scale_copy.wait()
    for source in (z, peer, near, far):
        beside(IN, source, None, "recv")
    keep(IN, "wait")

    local_groups, group_dim = pool_w.shape[0], pool_w.shape[1]
    at_row = lax.broadcasted_iota(jnp.int32, (SEQ, SEQ), 0)
    at_col = lax.broadcasted_iota(jnp.int32, (SEQ, SEQ), 1)
    pooled = jnp.dot(normed[...], in_all[...], preferred_element_type=f32).astype(bf16)
    for g in range(2 * local_groups):
        owner, place_in = divmod(g, local_groups)
        group = x * 2 * local_groups + g
        level = lax.div(4 * group, local_groups * tp)
        reach = jnp.int32(2)
        for bit in range(1, 4):
            reach = jnp.where(level >= bit, jnp.int32(2 << bit), reach)
        inside = jnp.where((at_col <= at_row) & (at_col > at_row - reach), 1.0, 0.0).astype(bf16)
        counts = jnp.minimum(at_row + 1, reach).astype(f32)[:, :1]
        is_own = core == owner
        cols = slice(g * group_dim, (g + 1) * group_dim)
        own_cols = slice(place_in * group_dim, (place_in + 1) * group_dim)
        weight = jnp.where(is_own, pool_w[place_in], pool_sib[place_in])
        factor = jnp.where(is_own, scale[own_cols].astype(f32).reshape(1, -1),
                           scale_sib[own_cols].astype(f32).reshape(1, -1))
        for s in range(rows // SEQ):
            at = slice(s * SEQ, (s + 1) * SEQ)
            part = pooled[at, cols]
            sums = jnp.dot(inside, part, preferred_element_type=f32)
            contrast = (sums / counts - part.astype(f32)).astype(bf16)
            mixed = jnp.dot(contrast, weight, preferred_element_type=f32)
            group_out[at, cols] = (mixed * factor).astype(bf16)

    for source in (peer, near, far):
        share(OUT, source)
    for source in (z, peer, near, far):
        beside(OUT, source, None, "recv")
    keep(OUT, "wait")

    def half_cols(owner):
        return pl.ds(at_least(owner * wide, LANES), wide)

    mix_send[...] = jnp.dot(group_out[...], out_all[:, half_cols(1 - x)],
                            preferred_element_type=f32).astype(bf16)
    mix_copy = remote(mix_send, mix_recv, mix_sems.at[0], mix_sems.at[1], XPEER)
    mix_copy.start()
    mix_own[...] = jnp.dot(group_out[...], out_all[:, half_cols(x)], preferred_element_type=f32)

    @pl.when(inner)
    def _():
        relay(GATE, peer)
        relay(GATE, near)

    @pl.when(outer)
    def _():
        relay(GATE, far)

    mix_copy.wait()
    mid_rows = pl.ds(at_least(seat * rows, 16), rows)
    mid_all[mid_rows, half_cols(x)] = (
        rows_all[:, half_cols(x)].astype(f32) + (mix_own[...] + mix_recv[...].astype(f32))).astype(bf16)

    def mid_copy(number, block, device):
        view = mid_all.at[pl.ds(at_least(block * rows, 16), rows), half_cols(x)]
        return remote(view, view, mid_send.at[number], mid_recv.at[number], device)

    to_pair, to_x, to_x_later = mid_copy(0, seat, ZPEER), mid_copy(1, seat, XPEER), mid_copy(2, 1 - seat, XPEER)
    to_pair.start()
    to_x.start()

    @pl.when(inner)
    def _():
        z_start(GATE, peer)
        z_start(UP, peer)
        z_start(DOWN, near, 0)
        z_start(UP, far)
        z_start(DOWN, far)
        z_start(DOWN, near, 1)
        share(GATE, peer)
        share(GATE, near)
        relay(UP, peer)
        relay(UP, near)

    @pl.when(outer)
    def _():
        z_start(GATE, near)
        z_start(UP, near)
        share(GATE, far)
        relay(UP, far)
        relay(GATE, near)

    to_pair.wait_recv()
    to_x_later.start()

    @pl.when(inner)
    def _():
        z_start(DOWN, peer)
        share(UP, peer)
        relay(DOWN, near, 0)

    @pl.when(outer)
    def _():
        z_start(DOWN, peer)
        z_start(DOWN, near)
        z_start(DOWN, far)
        share(UP, far)
        share(GATE, near)

    to_x.wait_recv()
    norm_into(mid_all, ffn_gain, normed_ffn, seat * rows, rows)

    @pl.when(inner)
    def _():
        share(UP, near)
        relay(GATE, far)

    @pl.when(outer)
    def _():
        relay(GATE, peer)

    to_x_later.wait_recv()
    norm_into(mid_all, ffn_gain, normed_ffn, (1 - seat) * rows, rows)

    depth = gate_all.shape[0] // 2
    pair_at = pl.ds(at_least(pair * depth, LANES), depth)
    cross_at = pl.ds(at_least((1 - pair) * depth, LANES), depth)
    early_at = pl.ds(at_least(jnp.where(inner, pair, 1 - pair) * depth, LANES), depth)
    later_at = pl.ds(at_least(jnp.where(inner, 1 - pair, pair) * depth, LANES), depth)
    tile = rows

    def by_tiles(body):
        def all_tiles(count):
            wide_units = 2 * count * LANES

            def step(i, carry):
                body(pl.ds(at_least(i * tile, tile), tile), wide_units)
                return carry
            lax.fori_loop(0, 2 * rows // tile, step, 0)
        sized(UP, inner, all_tiles)

    def partial_dot(at, depth_at, weights, n):
        return jnp.dot(normed_ffn[at, depth_at], weights[depth_at, :n], preferred_element_type=f32)

    def gate_first(at, n):
        gate_acts[at, :n] = partial_dot(at, early_at, gate_all, n)

    def gate_second(at, n):
        gate = gate_acts[at, :n] + partial_dot(at, later_at, gate_all, n)
        gate_acts[at, :n] = gate / (1.0 + jnp.exp(-gate))

    def up_first(at, n):
        up_acts[at, :n] = partial_dot(at, pair_at, up_all, n)

    def up_second(at, n):
        up = up_acts[at, :n] + partial_dot(at, cross_at, up_all, n)
        hidden[at, :n] = (gate_acts[at, :n] * up).astype(bf16)

    keep(GATE, "wait")
    for source in (jnp.where(inner, z, far), jnp.where(inner, peer, near)):
        beside(GATE, source, None, "recv")
    by_tiles(gate_first)

    @pl.when(inner)
    def _():
        relay(UP, far)
        share(GATE, far)

    @pl.when(outer)
    def _():
        relay(UP, peer)
        share(GATE, peer)

    for source in (jnp.where(inner, near, z), jnp.where(inner, far, peer)):
        beside(GATE, source, None, "recv")
    by_tiles(gate_second)

    @pl.when(outer)
    def _():
        share(UP, peer)
        relay(UP, near)

    keep(UP, "wait")
    for source in (z, peer):
        beside(UP, source, None, "recv")
    by_tiles(up_first)
    relay(DOWN, peer)

    @pl.when(inner)
    def _():
        share(UP, far)

    @pl.when(outer)
    def _():
        share(UP, near)

    beside(DOWN, peer, y, "start")
    for source in (near, far):
        beside(UP, source, None, "recv")
    by_tiles(up_second)

    sub = width // 2
    order = (z, peer, far, near)
    keeps_early = x == pair

    def half_of(turn):
        return y if turn == 0 else 1 - y

    half_sub = sub // 2

    def piece_cols(o, turn, part):
        start = order[o] * width + half_of(turn) * sub
        if part is None:
            return pl.ds(at_least(start, LANES), sub)
        return pl.ds(at_least(start + part * half_sub, LANES), half_sub)

    def lanes(part):
        return slice(0, sub) if part is None else slice(part * half_sub, (part + 1) * half_sub)

    ours = pl.ds(at_least(seat * rows, 16), rows)
    theirs = pl.ds(at_least((1 - seat) * rows, 16), rows)

    OWN, PEER, FAR, NEAR = range(4)

    def kept(o):
        return keeps_early if o < FAR else jnp.logical_not(keeps_early)

    def column_block(o, turn, part, n):
        values = jnp.dot(hidden[:, :n], down_all[:n, piece_cols(o, turn, part)],
                         preferred_element_type=f32)
        if o == NEAR:
            stage[:, lanes(part)] = values
            cross_send[turn, :, lanes(part)] = stage[theirs, lanes(part)].astype(bf16)
            cross_copy(turn, part).start()
            cross_own[turn, :, lanes(part)] = stage[ours, lanes(part)]
            return
        slot = 2 * (o % 2) + turn

        @pl.when(kept(o))
        def _():
            ffn_own[slot] = values

        @pl.when(jnp.logical_not(kept(o)))
        def _():
            ffn_send[slot] = values.astype(bf16)
            x_copy(slot, 0).start()
            x_copy(slot, 1).start()

    def cross_copy(turn, part):
        at, number = lanes(part), turn + (part or 0)
        return remote(cross_send.at[turn, :, at], cross_recv.at[turn, :, at],
                      c_send.at[number], c_recv.at[number], ZPEER)

    def late_copy(turn, part):
        at, number = lanes(part), turn + (part or 0)
        return remote(late_send.at[turn, :, at], late_recv.at[turn, :, at],
                      late_sems.at[0, number], late_sems.at[1, number], XPEER)

    def combine(turn, part=None):
        at = lanes(part)
        cross_copy(turn, part).wait_recv()

        @pl.when(keeps_early)
        def _():
            late_send[turn, :, at] = (cross_own[turn, :, at]
                                      + cross_recv[turn, :, at].astype(f32)).astype(bf16)
            late_copy(turn, part).start()

    def x_copy(slot, mine):
        at = ours if mine else theirs
        return remote(ffn_send.at[slot, at, :], ffn_recv.at[slot, at, :],
                      x_send.at[slot, mine], x_recv.at[slot, mine], XPEER)

    def pair_copy(o, turn):
        quarter, half = lax.rem(order[o], 2), half_of(turn)
        return remote(pair_send.at[quarter, half], pair_recv.at[quarter, half],
                      p_send.at[quarter, half], p_recv.at[quarter, half], ZPEER)

    def fold(o, turn):
        slot = 2 * (o % 2) + turn
        quarter, half = lax.rem(order[o], 2), half_of(turn)

        @pl.when(kept(o))
        def _():
            x_copy(slot, 0).wait_recv()
            pair_send[quarter, half] = (ffn_own[slot, theirs, :]
                                        + ffn_recv[slot, theirs, :].astype(f32)).astype(bf16)
            pair_copy(o, turn).start()

    def last_copy(half):
        return remote(last_send.at[half], last_recv.at[half], l_send.at[half], l_recv.at[half], SIB)

    def finish(o, turn, total):
        quarter, half = lax.rem(order[o], 2), half_of(turn)
        value = (mid_all[ours, piece_cols(o, turn, None)].astype(f32) + total).astype(bf16)

        @pl.when(quarter == core)
        def _():
            result[token_rows(core), pl.ds(at_least(half * sub, LANES), sub)] = value

        @pl.when(quarter != core)
        def _():
            last_send[half] = value
            last_copy(half).start()

    def settle(o, turn):
        slot = 2 * (o % 2) + turn
        quarter, half = lax.rem(order[o], 2), half_of(turn)

        @pl.when(kept(o))
        def _():
            if o == NEAR:
                for part in block_parts(o, turn):
                    late_copy(turn, part).wait_recv()
                finish(o, turn, cross_own[turn] + cross_recv[turn].astype(f32)
                       + late_recv[turn].astype(f32))
            else:
                x_copy(slot, 1).wait_recv()
                pair_copy(o, turn).wait_recv()
                finish(o, turn, ffn_own[slot, ours, :] + ffn_recv[slot, ours, :].astype(f32)
                       + pair_recv[quarter, half].astype(f32))

    def block_parts(o, turn):
        return (0, 1) if (o, turn) == (NEAR, 1) else (None,)

    def pour(source, only=None):
        for part in parts(DOWN):
            if only is None or part == only:
                across(DOWN, source, part, "recv")
                beside(DOWN, source, 1 - y, "start", part=part)

    def ready(o, turn, only=None):
        if o == 0 or turn == 0:
            beside(DOWN, order[o], half_of(turn), "recv")
            return
        for part in parts(DOWN):
            if only is None or part == only:
                beside(DOWN, order[o], 1 - y, "recv", part=part)

    def bring(o, only=None):
        relay(DOWN, order[o], only)
        beside(DOWN, order[o], y, "start")

    def block(o, turn, count, part=None):
        ready(o, turn, part)
        column_block(o, turn, part, 2 * count * LANES)

    keep(DOWN, "wait")

    @pl.when(outer)
    def _():
        block(OWN, 0, few)
        block(OWN, 1, few)
        block(PEER, 0, few)
        pour(peer)
        bring(FAR)
        block(PEER, 1, few)
        block(FAR, 0, few)
        fold(OWN, 0)
        bring(NEAR)
        pour(far)
        block(FAR, 1, few)
        fold(OWN, 1)
        block(NEAR, 0, few)
        fold(FAR, 0)
        pour(near, 0)
        block(NEAR, 1, few, 0)
        fold(PEER, 0)
        pour(near, 1)
        block(NEAR, 1, few, 1)

    @pl.when(inner)
    def _():
        block(OWN, 0, many)
        block(OWN, 1, many)
        block(PEER, 0, many)
        bring(FAR)
        pour(peer)
        block(PEER, 1, many)
        block(FAR, 0, many)
        fold(OWN, 0)
        pour(far)
        block(FAR, 1, many)
        fold(OWN, 1)
        bring(NEAR, 1)
        block(NEAR, 0, many)
        fold(FAR, 0)
        pour(near, 0)
        block(NEAR, 1, many, 0)
        fold(PEER, 0)
        pour(near, 1)
        block(NEAR, 1, many, 1)

    fold(FAR, 1)
    combine(0)
    combine(1, 0)
    fold(PEER, 1)
    combine(1, 1)
    for o in (OWN, FAR, PEER, NEAR):
        for turn in (0, 1):
            settle(o, turn)

    for half in (0, 1):
        last_copy(half).wait()
        result[token_rows(1 - core), half * sub:(half + 1) * sub] = last_recv[half]

    for which in range(5):
        z_sent(which, peer)
        z_sent(which, near)
        if which not in (IN, OUT):
            z_sent(which, far)
        else:
            @pl.when(inner)
            def _():
                for source in (near, far):
                    z_pass(which, source).wait_send()
        for source in (peer, near, far):
            for part in parts(which):
                across(which, source, part, "send")
        if which != DOWN:
            for source in order:
                beside(which, source, None, "send")
            continue
        for half in (0, 1):
            beside(which, z, half, "send")
        for source in order[1:]:
            beside(which, source, y, "send")
            for part in parts(which):
                beside(which, source, 1 - y, "send", part=part)
    for copy in (to_pair, to_x, to_x_later):
        copy.wait_send()
    near_pieces = [(turn, part) for turn in (0, 1) for part in block_parts(NEAR, turn)]
    for turn, part in near_pieces:
        cross_copy(turn, part).wait_send()

    @pl.when(keeps_early)
    def _():
        for turn in (0, 1):
            for mine in (0, 1):
                x_copy(turn, mine).wait_send()
            for o in (OWN, PEER):
                pair_copy(o, turn).wait_send()
        for turn, part in near_pieces:
            late_copy(turn, part).wait_send()

    @pl.when(jnp.logical_not(keeps_early))
    def _():
        for slot in range(4):
            for mine in (0, 1):
                x_copy(slot, mine).wait_send()
        for turn in (0, 1):
            pair_copy(FAR, turn).wait_send()


def pairs_fit(sizes, stream, in_weight, pool_weight, out_weight, gate_weight, down_weight):
    reps, fs, tp = sizes
    tokens, width = stream.shape
    return (reps == 2 and fs == 4 and tp == 4 and tokens % (2 * SEQ) == 0
            and width % (4 * LANES) == 0 and gate_weight.shape[1] % LANES == 0
            and in_weight.shape[1] % LANES == 0 and in_weight.shape[0] % 32 == 0
            and out_weight.shape[0] % 32 == 0 and gate_weight.shape[0] % 64 == 0
            and down_weight.shape[1] == width)


def pair_on_device(sizes, stream, in_weight, pool_weight, pool_scale, out_weight,
                   mix_gain, ffn_gain, gate_weight, up_weight, down_weight):
    if not pairs_fit(sizes, stream, in_weight, pool_weight, out_weight, gate_weight, down_weight):
        return ring_on_device(sizes, stream, in_weight, pool_weight, pool_scale, out_weight,
                              mix_gain, ffn_gain, gate_weight, up_weight, down_weight)
    reps, fs, tp = sizes
    tokens, width = stream.shape
    rows, sub = tokens // 2, width // 2
    features = width * tp
    channels = in_weight.shape[1]
    blocks = gate_weight.shape[1] // LANES
    units = 2 * LANES * (blocks - blocks // 2)
    bf, f32 = jnp.bfloat16, jnp.float32
    vmem = pl.BlockSpec(memory_space=pltpu.VMEM)
    hbm = pl.BlockSpec(memory_space=pl.ANY)
    dma = pltpu.SemaphoreType.DMA
    flops = 2 * tokens * (2 * features * channels + 3 * features * gate_weight.shape[1])
    return pl.pallas_call(
        functools.partial(pair_kernel, sizes),
        out_shape=jax.ShapeDtypeStruct(stream.shape, bf),
        in_specs=[vmem] + [hbm] * 5 + [vmem] * 4,
        out_specs=vmem,
        scratch_shapes=[
            pltpu.VMEM((in_weight.shape[0] * fs, 2 * channels), bf),
            pltpu.VMEM((2 * out_weight.shape[0], out_weight.shape[1] * fs), bf),
            pltpu.VMEM((up_weight.shape[0] * fs, units), bf),
            pltpu.VMEM((gate_weight.shape[0] * fs, units), bf),
            pltpu.VMEM((units, down_weight.shape[1] * fs), bf),
            pltpu.VMEM((rows, features), bf),
            pltpu.VMEM((rows, features), bf),
            pltpu.VMEM((rows, 2 * channels), bf),
            pltpu.VMEM((2 * rows, units), bf),
            pltpu.VMEM((2 * rows, units), f32),
            pltpu.VMEM((2 * rows, units), f32),
            pltpu.VMEM((2 * rows, features), bf),
            pltpu.VMEM((2 * rows, features), bf),
            pltpu.VMEM(pool_weight.shape, bf),
            pltpu.VMEM((channels,), bf),
            pltpu.VMEM((rows, 2 * width), f32),
            pltpu.VMEM((rows, 2 * width), bf),
            pltpu.VMEM((rows, 2 * width), bf),
            pltpu.VMEM((4, 2 * rows, sub), f32),
            pltpu.VMEM((4, 2 * rows, sub), bf),
            pltpu.VMEM((4, 2 * rows, sub), bf),
            pltpu.VMEM((2, 2, rows, sub), bf),
            pltpu.VMEM((2, 2, rows, sub), bf),
            pltpu.VMEM((2 * rows, sub), f32),
            pltpu.VMEM((2, rows, sub), bf),
            pltpu.VMEM((2, rows, sub), bf),
            pltpu.VMEM((2, rows, sub), f32),
            pltpu.VMEM((2, rows, sub), bf),
            pltpu.VMEM((2, rows, sub), bf),
            pltpu.VMEM((2, rows, sub), bf),
            pltpu.VMEM((2, rows, sub), bf),
            dma((21,)), dma((21,)), dma((2, 2)), dma((21,)), dma((21,)),
            dma((27,)), dma((27,)), dma((5,)),
            dma((3,)), dma((3,)), dma((2,)), dma((2,)), dma((2,)), dma((3,)), dma((3,)),
            dma((4, 2)), dma((4, 2)), dma((2, 2)), dma((2, 2)), dma((2,)), dma((2,)),
            dma((3,)), dma((3,)), dma((2, 3)),
        ],
        compiler_params=pltpu.CompilerParams(
            collective_id=0, has_side_effects=True, vmem_limit_bytes=64 * 1024 * 1024 - 65536),
        cost_estimate=pl.CostEstimate(flops=flops, bytes_accessed=flops // 512, transcendentals=0),
    )(stream, in_weight, out_weight, up_weight, gate_weight, down_weight, pool_weight,
      pool_scale, mix_gain, ffn_gain)


def solution(mesh):
    sizes = tuple(mesh.shape[name] for name in ("rep", "fs", "tp"))
    return jax.shard_map(
        functools.partial(pair_on_device, sizes),
        mesh=mesh,
        in_specs=(
            P(("rep", "fs"), "tp"),
            P("fs", "tp"),
            P("tp", None, None),
            P("tp"),
            P("tp", "fs"),
            P(),
            P(),
            P("fs", "tp"),
            P("fs", "tp"),
            P("tp", "fs"),
        ),
        out_specs=P(("rep", "fs"), "tp"),
        check_vma=False,
    )
```

```python
import functools

import jax
import jax.numpy as jnp
from jax import lax
from jax.experimental import pallas as pl
from jax.experimental.pallas import tpu as pltpu
from jax.sharding import PartitionSpec as P

SEQ = 128
EPSILON = 1e-06
MESH = pl.DeviceIdType.MESH
BY_ROWS = (True, False, True, True, False)
PIECES = ((0, 0), (1, 0), (2, 0), (3, 0), (2, 1), (3, 1), (4, 0), (4, 1))
CHUNKS = (1, 1, 2, 2, 2)


def ring_kernel(sizes, stream, in_w, out_w, up_w, gate_w, down_w, pool_w, scale,
           mix_gain, ffn_gain, result,
           in_all, out_all, up_all, gate_all, down_all,
           rows_all, normed, group_out, hidden, middle, mid_all,
           mix_send, mix_recv, ffn_send, ffn_recv,
           ring_send, ring_recv, fwd_send, fwd_recv, own_sem,
           tp_send, tp_recv, keep_sem):
    reps, fs, tp = sizes
    half = fs // 2
    my_rep, me, my_tp = lax.axis_index("rep"), lax.axis_index("fs"), lax.axis_index("tp")
    own = (in_w, out_w, up_w, gate_w, down_w)
    full = (in_all, out_all, up_all, gate_all, down_all)
    tokens, width = stream.shape

    def turn(at, by, count):
        return lax.rem(at + by + count, count)

    def piece(which, owner, row, count):
        block_rows, block_cols = own[which].shape
        if BY_ROWS[which]:
            return full[which].at[pl.ds(pl.multiple_of(owner * block_rows + row, 16), count), :]
        return full[which].at[pl.ds(pl.multiple_of(row, 16), count),
                              pl.ds(pl.multiple_of(owner * block_cols, 128), block_cols)]

    def span(number, step, way):
        which, chunk = PIECES[number]
        rows = own[which].shape[0]
        cut = rows % (CHUNKS[which] * reps * 2 * 16) == 0
        count = rows // CHUNKS[which] if cut else (rows, 0)[chunk]
        row = chunk * (rows // CHUNKS[which])
        count = count // reps
        row = row + my_rep * count
        if step == half:
            count = count // 2
            row = row + way * count
        return which, row, count

    def empty(number):
        return span(number, 1, 0)[2] == 0

    def ring(number, step, way):
        which, row, count = span(number, step, way)
        sign = 1 - 2 * way
        owner = turn(me, -sign * (step - 1), fs)
        if step == 1:
            source = own[which].at[pl.ds(pl.multiple_of(row, 16), count), :]
        else:
            source = piece(which, owner, row, count)
        return pltpu.make_async_remote_copy(
            src_ref=source, dst_ref=piece(which, owner, row, count),
            send_sem=ring_send.at[number, step - 1, way],
            recv_sem=ring_recv.at[number, step - 1, way],
            device_id={"fs": turn(me, sign, fs)}, device_id_type=MESH)

    def forward(number, step, way, peer):
        which, row, count = span(number, step, way)
        block = piece(which, turn(me, -(1 - 2 * way) * step, fs), row, count)
        return pltpu.make_async_remote_copy(
            src_ref=block, dst_ref=block,
            send_sem=fwd_send.at[number, peer - 1, step - 1, way],
            recv_sem=fwd_recv.at[number, peer - 1, step - 1, way],
            device_id={"rep": turn(my_rep, peer, reps)}, device_id_type=MESH)

    def begin(*numbers):
        for number in numbers:
            if not empty(number):
                for way in (0, 1):
                    ring(number, 1, way).start()

    def advance(number, step):
        if empty(number):
            return
        for way in (0, 1):
            ring(number, step, way).wait_recv()
            if step < half:
                ring(number, step + 1, way).start()
            for peer in range(1, reps):
                forward(number, step, way, peer).start()

    def early(*numbers):
        for number in numbers:
            for step in range(1, half):
                advance(number, step)

    def late(*numbers):
        for number in numbers:
            advance(number, half)

    def arrived(*numbers):
        for number in numbers:
            if PIECES[number][1] == 0:
                keeps[PIECES[number][0]].wait()
            if empty(number):
                continue
            for step in range(1, half + 1):
                for way in (0, 1):
                    for peer in range(1, reps):
                        forward(number, step, way, peer).wait()

    def tp_copy(stage, offset, source, target):
        return pltpu.make_async_remote_copy(
            src_ref=source, dst_ref=target,
            send_sem=tp_send.at[stage, offset - 1], recv_sem=tp_recv.at[stage, offset - 1],
            device_id={"tp": turn(my_tp, offset, tp)}, device_id_type=MESH)

    def feature_cols(owner):
        return pl.ds(pl.multiple_of(owner * width, 128), width)

    barrier = pltpu.get_barrier_semaphore()
    greeted = 0
    for name, at, count, offsets in (
            ("fs", me, fs, (1, -1)),
            ("tp", my_tp, tp, range(1, tp)),
            ("rep", my_rep, reps, range(1, reps))):
        for offset in offsets:
            pl.semaphore_signal(barrier, inc=1, device_id={name: turn(at, offset, count)},
                                device_id_type=MESH)
            greeted += 1
    pl.semaphore_wait(barrier, greeted)

    begin(0, 1)
    stream_sends = []
    for offset in range(1, tp):
        copy = tp_copy(0, offset, stream, rows_all.at[:, feature_cols(my_tp)])
        copy.start()
        stream_sends.append(copy)
    keeps = []
    for which in range(len(own)):
        keep = pltpu.make_async_copy(
            own[which], piece(which, me, 0, own[which].shape[0]), own_sem.at[which])
        keep.start()
        keeps.append(keep)
    keep_stream = pltpu.make_async_copy(
        stream, rows_all.at[:, feature_cols(my_tp)], keep_sem)
    keep_stream.start()
    early(0, 1)
    begin(2, 3, 4)
    late(0, 1)

    def norm_into(source, gain, target):
        tile = 64

        def body(i, carry):
            at = pl.ds(pl.multiple_of(i * tile, tile), tile)
            wide = source[at, :].astype(jnp.float32)
            mean = jnp.mean(wide * wide, axis=-1, keepdims=True)
            target[at, :] = (wide * lax.rsqrt(mean + EPSILON)
                             * gain[...].astype(jnp.float32)).astype(jnp.bfloat16)
            return carry

        lax.fori_loop(0, tokens // tile, body, 0)

    keep_stream.wait()
    for copy in stream_sends:
        copy.wait()
    norm_into(rows_all, mix_gain, normed)
    arrived(0)

    local_groups, group_dim = pool_w.shape[0], pool_w.shape[1]
    at_row = lax.broadcasted_iota(jnp.int32, (SEQ, SEQ), 0)
    at_col = lax.broadcasted_iota(jnp.int32, (SEQ, SEQ), 1)
    insides, inverses = [], []
    for g in range(local_groups):
        group = my_tp * local_groups + g
        level = lax.div(4 * group, local_groups * tp)
        reach = jnp.int32(2)
        for bit in range(1, 4):
            reach = jnp.where(level >= bit, jnp.int32(2 << bit), reach)
        inside = (at_col <= at_row) & (at_col > at_row - reach)
        insides.append(jnp.where(inside, 1.0, 0.0).astype(jnp.bfloat16))
        inverses.append(jnp.minimum(at_row + 1, reach).astype(jnp.float32)[:, :1])

    def mix(i, carry):
        at = pl.ds(pl.multiple_of(i * SEQ, SEQ), SEQ)
        pooled = jnp.dot(normed[at, :], in_all[...],
                         preferred_element_type=jnp.float32).astype(jnp.bfloat16)
        for g in range(local_groups):
            cols = slice(g * group_dim, (g + 1) * group_dim)
            part = pooled[:, cols]
            sums = jnp.dot(insides[g], part, preferred_element_type=jnp.float32)
            contrast = (sums / inverses[g] - part.astype(jnp.float32)).astype(jnp.bfloat16)
            mixed = jnp.dot(contrast, pool_w[g], preferred_element_type=jnp.float32)
            group_out[at, cols] = (mixed * scale[:, cols].astype(jnp.float32)).astype(jnp.bfloat16)
        return carry

    lax.fori_loop(0, tokens // SEQ, mix, 0)

    arrived(1)
    early(2)

    def spread(operand, weights, stage, sends, tile):
        def block(owner, target):
            def body(i, carry):
                at = pl.ds(pl.multiple_of(i * tile, tile), tile)
                target[at, :] = jnp.dot(operand[at, :], weights[:, feature_cols(owner)],
                                        preferred_element_type=jnp.float32).astype(jnp.bfloat16)
                return carry
            lax.fori_loop(0, tokens // tile, body, 0)

        copies = []
        recv = mix_recv if stage == 1 else ffn_recv
        for offset in sorted(range(1, tp), key=lambda o: -min(o, tp - o)):
            block(turn(my_tp, offset, tp), sends.at[offset - 1])
            copy = tp_copy(stage, offset, sends.at[offset - 1], recv.at[offset - 1])
            copy.start()
            copies.append(copy)
        block(my_tp, sends.at[tp - 1])
        return copies

    def gather_sum(base, recv, sends, target):
        tile = 64

        def body(i, carry):
            at = pl.ds(pl.multiple_of(i * tile, tile), tile)
            total = sends[tp - 1, at, :].astype(jnp.float32)
            for k in range(tp - 1):
                total = total + recv[k, at, :].astype(jnp.float32)
            target[at, :] = (base[at, :].astype(jnp.float32) + total).astype(jnp.bfloat16)
            return carry

        lax.fori_loop(0, tokens // tile, body, 0)

    mix_copies = spread(group_out, out_all, 1, mix_send, tokens // 2)
    early(3)
    begin(5)
    for copy in mix_copies:
        copy.wait()
    gather_sum(stream, mix_recv, mix_send, middle)
    keep_middle = pltpu.make_async_copy(middle, mid_all.at[:, feature_cols(my_tp)], keep_sem)
    keep_middle.start()
    middle_copies = []
    for offset in range(1, tp):
        copy = tp_copy(2, offset, middle, mid_all.at[:, feature_cols(my_tp)])
        copy.start()
        middle_copies.append(copy)
    early(4)
    begin(6, 7)
    late(2, 3)
    keep_middle.wait()
    for copy in middle_copies:
        copy.wait()
    norm_into(mid_all, ffn_gain, normed)
    early(5)
    late(4)
    early(6)
    late(5)
    early(7)
    late(6)
    arrived(2, 3, 4, 5)
    tile = tokens // 2

    def gated(i, carry):
        at = pl.ds(pl.multiple_of(i * tile, tile), tile)
        values = normed[at, :]
        gate = jnp.dot(values, gate_all[...], preferred_element_type=jnp.float32)
        up = jnp.dot(values, up_all[...], preferred_element_type=jnp.float32)
        hidden[at, :] = (gate / (1.0 + jnp.exp(-gate)) * up).astype(jnp.bfloat16)
        return carry

    lax.fori_loop(0, tokens // tile, gated, 0)
    late(7)
    arrived(6, 7)
    ffn_copies = spread(hidden, down_all, 3, ffn_send, tokens // 2)
    for number in range(len(PIECES)):
        if not empty(number):
            for step in range(1, half + 1):
                for way in (0, 1):
                    ring(number, step, way).wait_send()
    for copy in ffn_copies:
        copy.wait()
    gather_sum(middle, ffn_recv, ffn_send, result)


def ring_on_device(sizes, stream, in_weight, pool_weight, pool_scale, out_weight,
              mix_gain, ffn_gain, gate_weight, up_weight, down_weight):
    reps, fs, tp = sizes
    half = fs // 2
    tokens, width = stream.shape
    features = width * tp
    own = (in_weight, out_weight, up_weight, gate_weight, down_weight)
    full = [pltpu.VMEM((w.shape[0] * fs, w.shape[1]) if by_rows else (w.shape[0], w.shape[1] * fs),
                       jnp.bfloat16) for w, by_rows in zip(own, BY_ROWS)]
    units = gate_weight.shape[1]
    bf = jnp.bfloat16
    vmem = pl.BlockSpec(memory_space=pltpu.VMEM)
    hbm = pl.BlockSpec(memory_space=pl.ANY)
    dma = pltpu.SemaphoreType.DMA
    flops = 2 * tokens * (2 * features * in_weight.shape[1] + 3 * features * units)
    return pl.pallas_call(
        functools.partial(ring_kernel, sizes),
        out_shape=jax.ShapeDtypeStruct(stream.shape, bf),
        in_specs=[vmem] + [hbm] * 5 + [vmem] * 4,
        out_specs=vmem,
        scratch_shapes=full + [
            pltpu.VMEM((tokens, features), bf),
            pltpu.VMEM((tokens, features), bf),
            pltpu.VMEM((tokens, in_weight.shape[1]), bf),
            pltpu.VMEM((tokens, units), bf),
            pltpu.VMEM((tokens, width), bf),
            pltpu.VMEM((tokens, features), bf),
            pltpu.VMEM((tp, tokens, width), bf),
            pltpu.VMEM((tp - 1, tokens, width), bf),
            pltpu.VMEM((tp, tokens, width), bf),
            pltpu.VMEM((tp - 1, tokens, width), bf),
            dma((len(PIECES), half, 2)),
            dma((len(PIECES), half, 2)),
            dma((len(PIECES), max(reps - 1, 1), half, 2)),
            dma((len(PIECES), max(reps - 1, 1), half, 2)),
            dma((len(own),)),
            dma((4, tp - 1)),
            dma((4, tp - 1)),
            dma(()),
        ],
        compiler_params=pltpu.CompilerParams(
            collective_id=0, has_side_effects=True, vmem_limit_bytes=64 * 1024 * 1024 - 65536),
        cost_estimate=pl.CostEstimate(flops=flops, bytes_accessed=flops // 512, transcendentals=0),
    )(stream, in_weight, out_weight, up_weight, gate_weight, down_weight, pool_weight,
      pool_scale.reshape(1, -1), mix_gain.reshape(1, -1), ffn_gain.reshape(1, -1))


IN, OUT, UP, GATE, DOWN = range(5)
LANES = 128


def pair_kernel(sizes, stream, in_w, out_w, up_w, gate_w, down_w, pool_in, scale_in,
                mix_gain_in, ffn_gain_in, result,
                in_all, out_all, up_all, gate_all, down_all,
                rows_all, normed, group_out, hidden, gate_acts, up_acts, mid_all, normed_ffn,
                pool_w, scale, mix_gain, ffn_gain, pool_sib, scale_sib,
                mix_own, mix_send, mix_recv, ffn_own, ffn_send, ffn_recv, pair_send, pair_recv,
                stage, cross_send, cross_recv, cross_own, late_send, late_recv,
                last_send, last_recv,
                z_send, z_recv, pass_send, y_send, y_recv, d_send, d_recv, own_sem,
                in_send, in_recv, pool_send, pool_recv, mix_sems, mid_send, mid_recv,
                x_send, x_recv, p_send, p_recv, l_send, l_recv, c_send, c_recv, late_sems):
    reps, fs, tp = sizes
    y, z, lane_id = lax.axis_index("rep"), lax.axis_index("fs"), lax.axis_index("tp")
    x, core = lax.div(lane_id, 2), lax.rem(lane_id, 2)
    own = (in_w, out_w, up_w, gate_w, down_w)
    full = (in_all, out_all, up_all, gate_all, down_all)
    tokens, width = stream.shape
    rows = tokens // 2
    wide = 2 * width
    seat, pair = lax.rem(z, 2), lax.div(z, 2)
    peer = z + 1 - 2 * seat
    near = jnp.where(pair == 0, 2, 1)
    far = jnp.where(pair == 0, 3, 0)
    inner = (z == 1) | (z == 2)
    f32, bf16 = jnp.float32, jnp.bfloat16

    blocks = gate_w.shape[1] // LANES
    few, many = blocks // 2, blocks - blocks // 2

    SIB = {"tp": lane_id + 1 - 2 * core}
    XPEER = {"tp": lane_id + 2 - 4 * x}
    XSIB = {"tp": 2 * (1 - x) + 1 - core}
    YPEER = {"rep": 1 - y}
    ZPEER = {"fs": peer}

    def at_least(value, multiple):
        return pl.multiple_of(value, multiple)

    def remote(source, target, send, recv, device):
        return pltpu.make_async_remote_copy(
            src_ref=source, dst_ref=target, send_sem=send, recv_sem=recv,
            device_id=device, device_id_type=MESH)

    def sized(which, roomy, act):
        if which in (IN, OUT) or few == many:
            act(many)
            return

        @pl.when(roomy)
        def _():
            act(many)

        @pl.when(jnp.logical_not(roomy))
        def _():
            act(few)

    slot_of = {IN: 0, OUT: 1, GATE: 2, UP: 3, DOWN: 5}

    def role_of(source):
        return jnp.where(source == peer, 0, jnp.where(source == near, 1,
                         jnp.where(source == far, 2, 3)))

    def flow(which, part, role):
        return 3 * (slot_of[which] + (part or 0)) + role

    def beside_flow(which, source, half, part):
        if which != DOWN:
            return 4 * (IN, OUT, GATE, UP).index(which) + role_of(source)
        if source is z:
            return 16 + half
        return 18 + 3 * role_of(source) + (0 if part is None else 1 + part)

    def extent(which):
        return own[which].shape[1 if which == DOWN else 0]

    def half_span(which, half, part=None):
        size = extent(which) // 2
        if half is None:
            return 0, 2 * size
        if part is None:
            return half * size, size
        return half * size + min(part, 1) * (size // 2), size // 2

    def unit_rows(part, count):
        upper = count - count // 2
        return {1: (0, upper), 2: (upper, count - upper)}.get(part, (0, count))

    def parts(which):
        return {UP: (0, 1), DOWN: (0, 1, 2)}.get(which, (None,))

    def place(which, source, span, core_at, count, part=None):
        block_rows, block_cols = own[which].shape
        ref = full[which]
        start, size = span
        if which == OUT:
            return ref.at[pl.ds(at_least(core_at * block_rows + start, 16), size),
                          pl.ds(at_least(source * block_cols, LANES), block_cols)]
        if which == IN:
            return ref.at[pl.ds(at_least(source * block_rows + start, 16), size),
                          pl.ds(at_least(core_at * block_cols, LANES), block_cols)]
        first = core_at * (count * LANES)
        if which == DOWN:
            skip, taken = unit_rows(part, count)
            return ref.at[pl.ds(at_least(first + skip * LANES, LANES), taken * LANES),
                          pl.ds(at_least(source * block_cols + start, LANES), size)]
        return ref.at[pl.ds(at_least(source * block_rows + start, 16), size),
                      pl.ds(at_least(first, LANES), count * LANES)]

    def held(which, span, roomy, count, part=None):
        ref = own[which]
        start, size = span
        if which in (IN, OUT):
            return ref.at[pl.ds(at_least(start, 16), size), :]
        first = jnp.where(roomy, 0, many * LANES)
        if which == DOWN:
            skip, taken = unit_rows(part, count)
            return ref.at[pl.ds(at_least(first + skip * LANES, LANES), taken * LANES),
                          pl.ds(at_least(start, LANES), size)]
        return ref.at[pl.ds(at_least(start, 16), size),
                      pl.ds(at_least(first, LANES), count * LANES)]

    def z_copies(which, dest, step, only=None):
        roomy = (dest == 1) | (dest == 2)

        def act(n):
            for part in parts(which) if only is None else only:
                span = half_span(which, y, part)
                there = jnp.where(dest == peer, 0, jnp.where(inner, 1, 2))
                copy = remote(held(which, span, roomy, n, part),
                              place(which, z, span, core, n, part),
                              z_send.at[flow(which, part, role_of(dest))],
                              z_recv.at[flow(which, part, there)], {"fs": dest})
                {"start": copy.start, "send": copy.wait_send}[step]()
        sized(which, roomy, act)

    def z_start(which, dest, only=None):
        z_copies(which, dest, "start", only)

    def z_sent(which, dest):
        z_copies(which, dest, "send")

    def z_pass(which, source):
        block = place(which, source, half_span(which, y), core, many)
        return remote(block, block, pass_send.at[which, lax.rem(source, 2)],
                      z_recv.at[flow(which, None, role_of(source))], ZPEER)

    def arrived(which, source, part):
        def act(n):
            block = place(which, source, half_span(which, y, part), core, n, part)
            at = flow(which, part, role_of(source))
            remote(block, block, y_send.at[at], z_recv.at[at], YPEER).wait_recv()
        sized(which, inner, act)

    def across(which, source, part, step):
        def act(n):
            half = 1 - y if step == "recv" else y
            block = place(which, source, half_span(which, half, part), core, n, part)
            at = flow(which, part, role_of(source))
            copy = remote(block, block, y_send.at[at], y_recv.at[at], YPEER)
            {"start": copy.start, "recv": copy.wait_recv, "send": copy.wait_send}[step]()
        sized(which, inner, act)

    def beside(which, source, half, step, mine=False, part=None):
        at = beside_flow(which, source, half, part)
        whose = 1 - core if step == "recv" else core

        def act(n):
            span = half_span(which, half, part)
            block = place(which, source, span, whose, n)
            start = held(which, span, inner, n) if mine else block
            copy = remote(start, block, d_send.at[at], d_recv.at[at], SIB)
            {"start": copy.start, "recv": copy.wait_recv, "send": copy.wait_send}[step]()
        sized(which, inner, act)

    def keep(which, step):
        def act(n):
            span = half_span(which, None)
            copy = pltpu.make_async_copy(held(which, span, inner, n),
                                         place(which, z, span, core, n), own_sem.at[which])
            {"start": copy.start, "wait": copy.wait}[step]()
        sized(which, inner, act)

    def relay(which, source, only=None):
        for part in parts(which):
            if only is None or part in only:
                arrived(which, source, part)
                across(which, source, part, "start")

    def share(which, source):
        for part in parts(which):
            across(which, source, part, "recv")
        beside(which, source, None, "start")

    def feature_cols(owner):
        return pl.ds(at_least(owner * width, LANES), width)

    def token_rows(half):
        return pl.ds(at_least(half * rows, 16), rows)

    def stream_copy(number, device, half):
        return remote(stream.at[token_rows(half), :], rows_all.at[:, feature_cols(lane_id)],
                      in_send.at[number], in_recv.at[number], device)

    small_copies = [pltpu.make_async_copy(source, target, own_sem.at[6 + number])
                    for number, (source, target) in enumerate((
                        (mix_gain_in, mix_gain), (ffn_gain_in, ffn_gain),
                        (pool_in, pool_w), (scale_in, scale)))]
    for copy in small_copies:
        copy.start()

    barrier = pltpu.get_barrier_semaphore()
    greeted = 0
    for device in (SIB, XPEER, XSIB, YPEER, ZPEER, {"fs": near}, {"fs": far}):
        pl.semaphore_signal(barrier, inc=1, device_id=device, device_id_type=MESH)
        greeted += 1
    pl.semaphore_wait(barrier, greeted)

    outer = jnp.logical_not(inner)
    z_start(IN, near)
    z_start(IN, peer)
    stream_copies = [stream_copy(0, XPEER, core), stream_copy(1, XSIB, 1 - core),
                     stream_copy(2, SIB, 1 - core)]
    for copy in stream_copies:
        copy.start()
    z_start(OUT, near)
    z_start(OUT, peer)
    keep(IN, "start")
    beside(IN, z, None, "start", mine=True)
    pool_copy = remote(pool_in, pool_sib, pool_send.at[0], pool_recv.at[0], SIB)
    scale_copy = remote(scale_in, scale_sib, pool_send.at[1], pool_recv.at[1], SIB)
    pool_copy.start()
    scale_copy.start()

    @pl.when(inner)
    def _():
        z_start(GATE, near)
        z_start(GATE, far)
        z_start(UP, near)

    @pl.when(outer)
    def _():
        z_start(GATE, peer)
        z_start(GATE, far)
        z_start(UP, far)
        z_start(UP, peer)

    for which in (OUT, GATE, UP, DOWN):
        keep(which, "start")
        for half in (0, 1) if which == DOWN else (None,):
            beside(which, z, half, "start", mine=True)

    own_rows = pltpu.make_async_copy(stream.at[token_rows(core), :],
                                     rows_all.at[:, feature_cols(lane_id)], own_sem.at[5])
    own_rows.start()

    def take(which):
        relay(which, peer)
        for source in (near, far):
            arrived(which, source, None)

            @pl.when(inner)
            def _():
                z_pass(which, source).start()
            across(which, source, None, "start")

    take(IN)

    @pl.when(inner)
    def _():
        take(OUT)

    def norm_into(source, gain, target, first, count):
        tile = 64

        def body(i, carry):
            at = pl.ds(at_least(first + i * tile, tile), tile)
            values = source[at, :].astype(f32)
            mean = jnp.mean(values * values, axis=-1, keepdims=True)
            target[at, :] = (values * lax.rsqrt(mean + EPSILON)
                             * gain[...].astype(f32).reshape(1, -1)).astype(bf16)
            return carry

        lax.fori_loop(0, count // tile, body, 0)

    own_rows.wait()
    for copy in small_copies:
        copy.wait()
    for copy in stream_copies:
        copy.wait()
    norm_into(rows_all, mix_gain, normed, 0, rows)
    for source in (peer, near, far):
        share(IN, source)

    @pl.when(outer)
    def _():
        take(OUT)

    pool_copy.wait()
    scale_copy.wait()
    for source in (z, peer, near, far):
        beside(IN, source, None, "recv")
    keep(IN, "wait")

    local_groups, group_dim = pool_w.shape[0], pool_w.shape[1]
    at_row = lax.broadcasted_iota(jnp.int32, (SEQ, SEQ), 0)
    at_col = lax.broadcasted_iota(jnp.int32, (SEQ, SEQ), 1)
    pooled = jnp.dot(normed[...], in_all[...], preferred_element_type=f32).astype(bf16)
    for g in range(2 * local_groups):
        owner, place_in = divmod(g, local_groups)
        group = x * 2 * local_groups + g
        level = lax.div(4 * group, local_groups * tp)
        reach = jnp.int32(2)
        for bit in range(1, 4):
            reach = jnp.where(level >= bit, jnp.int32(2 << bit), reach)
        inside = jnp.where((at_col <= at_row) & (at_col > at_row - reach), 1.0, 0.0).astype(bf16)
        counts = jnp.minimum(at_row + 1, reach).astype(f32)[:, :1]
        is_own = core == owner
        cols = slice(g * group_dim, (g + 1) * group_dim)
        own_cols = slice(place_in * group_dim, (place_in + 1) * group_dim)
        weight = jnp.where(is_own, pool_w[place_in], pool_sib[place_in])
        factor = jnp.where(is_own, scale[own_cols].astype(f32).reshape(1, -1),
                           scale_sib[own_cols].astype(f32).reshape(1, -1))
        for s in range(rows // SEQ):
            at = slice(s * SEQ, (s + 1) * SEQ)
            part = pooled[at, cols]
            sums = jnp.dot(inside, part, preferred_element_type=f32)
            contrast = (sums / counts - part.astype(f32)).astype(bf16)
            mixed = jnp.dot(contrast, weight, preferred_element_type=f32)
            group_out[at, cols] = (mixed * factor).astype(bf16)

    for source in (peer, near, far):
        share(OUT, source)
    for source in (z, peer, near, far):
        beside(OUT, source, None, "recv")
    keep(OUT, "wait")

    def half_cols(owner):
        return pl.ds(at_least(owner * wide, LANES), wide)

    mix_send[...] = jnp.dot(group_out[...], out_all[:, half_cols(1 - x)],
                            preferred_element_type=f32).astype(bf16)
    mix_copy = remote(mix_send, mix_recv, mix_sems.at[0], mix_sems.at[1], XPEER)
    mix_copy.start()
    mix_own[...] = jnp.dot(group_out[...], out_all[:, half_cols(x)], preferred_element_type=f32)

    @pl.when(inner)
    def _():
        relay(GATE, peer)
        relay(GATE, near)

    @pl.when(outer)
    def _():
        relay(GATE, far)

    mix_copy.wait()
    mid_rows = pl.ds(at_least(seat * rows, 16), rows)
    mid_all[mid_rows, half_cols(x)] = (
        rows_all[:, half_cols(x)].astype(f32) + (mix_own[...] + mix_recv[...].astype(f32))).astype(bf16)

    def mid_copy(number, block, device):
        view = mid_all.at[pl.ds(at_least(block * rows, 16), rows), half_cols(x)]
        return remote(view, view, mid_send.at[number], mid_recv.at[number], device)

    to_pair, to_x, to_x_later = mid_copy(0, seat, ZPEER), mid_copy(1, seat, XPEER), mid_copy(2, 1 - seat, XPEER)
    to_pair.start()
    to_x.start()

    @pl.when(inner)
    def _():
        z_start(GATE, peer)
        z_start(UP, peer)
        z_start(DOWN, near, (0,))
        z_start(UP, far)
        z_start(DOWN, far)
        z_start(DOWN, near, (1, 2))
        share(GATE, peer)
        share(GATE, near)
        relay(UP, peer)
        relay(UP, near)

    @pl.when(outer)
    def _():
        z_start(GATE, near)
        z_start(UP, near)
        share(GATE, far)
        relay(UP, far)
        relay(GATE, near)

    to_pair.wait_recv()
    to_x_later.start()

    @pl.when(inner)
    def _():
        z_start(DOWN, peer)
        share(UP, peer)
        relay(DOWN, near, (0,))

    @pl.when(outer)
    def _():
        z_start(DOWN, peer)
        z_start(DOWN, near)
        z_start(DOWN, far)
        share(UP, far)
        share(GATE, near)

    to_x.wait_recv()
    norm_into(mid_all, ffn_gain, normed_ffn, seat * rows, rows)

    @pl.when(inner)
    def _():
        share(UP, near)
        relay(GATE, far)

    @pl.when(outer)
    def _():
        relay(GATE, peer)

    to_x_later.wait_recv()
    norm_into(mid_all, ffn_gain, normed_ffn, (1 - seat) * rows, rows)

    depth = gate_all.shape[0] // 2
    pair_at = pl.ds(at_least(pair * depth, LANES), depth)
    cross_at = pl.ds(at_least((1 - pair) * depth, LANES), depth)
    early_at = pl.ds(at_least(jnp.where(inner, pair, 1 - pair) * depth, LANES), depth)
    later_at = pl.ds(at_least(jnp.where(inner, 1 - pair, pair) * depth, LANES), depth)
    tile = rows

    def by_tiles(body):
        def all_tiles(count):
            wide_units = 2 * count * LANES

            def step(i, carry):
                body(pl.ds(at_least(i * tile, tile), tile), wide_units)
                return carry
            lax.fori_loop(0, 2 * rows // tile, step, 0)
        sized(UP, inner, all_tiles)

    def partial_dot(at, depth_at, weights, n):
        return jnp.dot(normed_ffn[at, depth_at], weights[depth_at, :n], preferred_element_type=f32)

    def gate_first(at, n):
        gate_acts[at, :n] = partial_dot(at, early_at, gate_all, n)

    def gate_second(at, n):
        gate = gate_acts[at, :n] + partial_dot(at, later_at, gate_all, n)
        gate_acts[at, :n] = gate / (1.0 + jnp.exp(-gate))

    def up_first(at, n):
        up_acts[at, :n] = partial_dot(at, pair_at, up_all, n)

    def up_second(at, n):
        up = up_acts[at, :n] + partial_dot(at, cross_at, up_all, n)
        hidden[at, :n] = (gate_acts[at, :n] * up).astype(bf16)

    keep(GATE, "wait")
    for source in (jnp.where(inner, z, far), jnp.where(inner, peer, near)):
        beside(GATE, source, None, "recv")
    by_tiles(gate_first)

    @pl.when(inner)
    def _():
        relay(UP, far)
        share(GATE, far)

    @pl.when(outer)
    def _():
        relay(UP, peer)
        share(GATE, peer)

    for source in (jnp.where(inner, near, z), jnp.where(inner, far, peer)):
        beside(GATE, source, None, "recv")
    by_tiles(gate_second)

    @pl.when(outer)
    def _():
        share(UP, peer)
        relay(UP, near)

    keep(UP, "wait")
    for source in (z, peer):
        beside(UP, source, None, "recv")
    by_tiles(up_first)

    relay(DOWN, peer)

    @pl.when(inner)
    def _():
        share(UP, far)

    @pl.when(outer)
    def _():
        share(UP, near)

    beside(DOWN, peer, y, "start")

    for source in (near, far):
        beside(UP, source, None, "recv")
    by_tiles(up_second)

    sub = width // 2
    order = (z, peer, far, near)
    keeps_early = x == pair

    def half_of(turn):
        return y if turn == 0 else 1 - y

    half_sub = sub // 2

    def piece_cols(o, turn, part):
        start = order[o] * width + half_of(turn) * sub
        if part is None:
            return pl.ds(at_least(start, LANES), sub)
        return pl.ds(at_least(start + part * half_sub, LANES), half_sub)

    def lanes(part):
        return slice(0, sub) if part is None else slice(part * half_sub, (part + 1) * half_sub)

    ours = pl.ds(at_least(seat * rows, 16), rows)
    theirs = pl.ds(at_least((1 - seat) * rows, 16), rows)

    OWN, PEER, FAR, NEAR = range(4)

    def kept(o):
        return keeps_early if o < FAR else jnp.logical_not(keeps_early)

    def column_block(o, turn, part, n):
        values = jnp.dot(hidden[:, :n], down_all[:n, piece_cols(o, turn, part)],
                         preferred_element_type=f32)
        if o == NEAR:
            stage[:, lanes(part)] = values
            cross_send[turn, :, lanes(part)] = stage[theirs, lanes(part)].astype(bf16)
            cross_copy(turn, part).start()
            cross_own[turn, :, lanes(part)] = stage[ours, lanes(part)]
            return
        slot = 2 * (o % 2) + turn

        @pl.when(kept(o))
        def _():
            ffn_own[slot] = values

        @pl.when(jnp.logical_not(kept(o)))
        def _():
            ffn_send[slot] = values.astype(bf16)
            x_copy(slot, 0).start()
            x_copy(slot, 1).start()

    def cross_copy(turn, part):
        at, number = lanes(part), turn + (part or 0)
        return remote(cross_send.at[turn, :, at], cross_recv.at[turn, :, at],
                      c_send.at[number], c_recv.at[number], ZPEER)

    def late_copy(turn, part):
        at, number = lanes(part), turn + (part or 0)
        return remote(late_send.at[turn, :, at], late_recv.at[turn, :, at],
                      late_sems.at[0, number], late_sems.at[1, number], XPEER)

    def combine(turn, part=None):
        at = lanes(part)
        cross_copy(turn, part).wait_recv()

        @pl.when(keeps_early)
        def _():
            late_send[turn, :, at] = (cross_own[turn, :, at]
                                      + cross_recv[turn, :, at].astype(f32)).astype(bf16)
            late_copy(turn, part).start()

    def x_copy(slot, mine):
        at = ours if mine else theirs
        return remote(ffn_send.at[slot, at, :], ffn_recv.at[slot, at, :],
                      x_send.at[slot, mine], x_recv.at[slot, mine], XPEER)

    def pair_copy(o, turn):
        quarter, half = lax.rem(order[o], 2), half_of(turn)
        return remote(pair_send.at[quarter, half], pair_recv.at[quarter, half],
                      p_send.at[quarter, half], p_recv.at[quarter, half], ZPEER)

    def fold(o, turn):
        slot = 2 * (o % 2) + turn
        quarter, half = lax.rem(order[o], 2), half_of(turn)

        @pl.when(kept(o))
        def _():
            x_copy(slot, 0).wait_recv()
            pair_send[quarter, half] = (ffn_own[slot, theirs, :]
                                        + ffn_recv[slot, theirs, :].astype(f32)).astype(bf16)
            pair_copy(o, turn).start()

    def last_copy(half):
        return remote(last_send.at[half], last_recv.at[half], l_send.at[half], l_recv.at[half], SIB)

    def finish(o, turn, total):
        quarter, half = lax.rem(order[o], 2), half_of(turn)
        value = (mid_all[ours, piece_cols(o, turn, None)].astype(f32) + total).astype(bf16)

        @pl.when(quarter == core)
        def _():
            result[token_rows(core), pl.ds(at_least(half * sub, LANES), sub)] = value

        @pl.when(quarter != core)
        def _():
            last_send[half] = value
            last_copy(half).start()

    def settle(o, turn):
        slot = 2 * (o % 2) + turn
        quarter, half = lax.rem(order[o], 2), half_of(turn)

        @pl.when(kept(o))
        def _():
            if o == NEAR:
                for part in block_parts(o, turn):
                    late_copy(turn, part).wait_recv()
                finish(o, turn, cross_own[turn] + cross_recv[turn].astype(f32)
                       + late_recv[turn].astype(f32))
            else:
                x_copy(slot, 1).wait_recv()
                pair_copy(o, turn).wait_recv()
                finish(o, turn, ffn_own[slot, ours, :] + ffn_recv[slot, ours, :].astype(f32)
                       + pair_recv[quarter, half].astype(f32))

    def block_parts(o, turn):
        return (0, 1) if (o, turn) == (NEAR, 1) else (None,)

    def pour(source, only=None):
        for part in (0, 1):
            if only is None or part == only:
                for piece in (0,) if part == 0 else (1, 2):
                    across(DOWN, source, piece, "recv")
                beside(DOWN, source, 1 - y, "start", part=part)

    def ready(o, turn, only=None):
        if o == 0 or turn == 0:
            beside(DOWN, order[o], half_of(turn), "recv")
            return
        for part in (0, 1):
            if only is None or part == only:
                beside(DOWN, order[o], 1 - y, "recv", part=part)

    def bring(o, only=None):
        relay(DOWN, order[o], only)
        beside(DOWN, order[o], y, "start")

    def block(o, turn, count, part=None):
        ready(o, turn, part)
        column_block(o, turn, part, 2 * count * LANES)

    keep(DOWN, "wait")

    @pl.when(outer)
    def _():
        block(OWN, 0, few)
        block(OWN, 1, few)
        block(PEER, 0, few)
        pour(peer)
        relay(DOWN, far, (0,))
        block(PEER, 1, few)
        bring(FAR, (1, 2))
        block(FAR, 0, few)
        fold(OWN, 0)
        bring(NEAR)
        pour(far)
        block(FAR, 1, few)
        fold(OWN, 1)
        block(NEAR, 0, few)
        fold(FAR, 0)
        pour(near, 0)
        block(NEAR, 1, few, 0)
        fold(PEER, 0)
        pour(near, 1)
        block(NEAR, 1, few, 1)

    @pl.when(inner)
    def _():
        block(OWN, 0, many)
        block(OWN, 1, many)
        block(PEER, 0, many)
        bring(FAR)
        pour(peer)
        block(PEER, 1, many)
        block(FAR, 0, many)
        fold(OWN, 0)
        pour(far)
        relay(DOWN, near, (1,))
        block(FAR, 1, many)
        fold(OWN, 1)
        bring(NEAR, (2,))
        block(NEAR, 0, many)
        fold(FAR, 0)
        pour(near, 0)
        block(NEAR, 1, many, 0)
        fold(PEER, 0)
        pour(near, 1)
        block(NEAR, 1, many, 1)

    fold(FAR, 1)
    combine(0)
    combine(1, 0)
    fold(PEER, 1)
    combine(1, 1)
    for o in (OWN, FAR, PEER, NEAR):
        for turn in (0, 1):
            settle(o, turn)

    for half in (0, 1):
        last_copy(half).wait()
        result[token_rows(1 - core), half * sub:(half + 1) * sub] = last_recv[half]

    for which in range(5):
        z_sent(which, peer)
        z_sent(which, near)
        if which not in (IN, OUT):
            z_sent(which, far)
        else:
            @pl.when(inner)
            def _():
                for source in (near, far):
                    z_pass(which, source).wait_send()
        for source in (peer, near, far):
            for part in parts(which):
                across(which, source, part, "send")
        if which != DOWN:
            for source in order:
                beside(which, source, None, "send")
            continue
        for half in (0, 1):
            beside(which, z, half, "send")
        for source in order[1:]:
            beside(which, source, y, "send")
            for part in (0, 1):
                beside(which, source, 1 - y, "send", part=part)
    for copy in (to_pair, to_x, to_x_later):
        copy.wait_send()
    near_pieces = [(turn, part) for turn in (0, 1) for part in block_parts(NEAR, turn)]
    for turn, part in near_pieces:
        cross_copy(turn, part).wait_send()

    @pl.when(keeps_early)
    def _():
        for turn in (0, 1):
            for mine in (0, 1):
                x_copy(turn, mine).wait_send()
            for o in (OWN, PEER):
                pair_copy(o, turn).wait_send()
        for turn, part in near_pieces:
            late_copy(turn, part).wait_send()

    @pl.when(jnp.logical_not(keeps_early))
    def _():
        for slot in range(4):
            for mine in (0, 1):
                x_copy(slot, mine).wait_send()
        for turn in (0, 1):
            pair_copy(FAR, turn).wait_send()


def pairs_fit(sizes, stream, in_weight, pool_weight, out_weight, gate_weight, down_weight):
    reps, fs, tp = sizes
    tokens, width = stream.shape
    return (reps == 2 and fs == 4 and tp == 4 and tokens % (2 * SEQ) == 0
            and width % (4 * LANES) == 0 and gate_weight.shape[1] % LANES == 0
            and in_weight.shape[1] % LANES == 0 and in_weight.shape[0] % 32 == 0
            and out_weight.shape[0] % 32 == 0 and gate_weight.shape[0] % 64 == 0
            and down_weight.shape[1] == width)


def pair_on_device(sizes, stream, in_weight, pool_weight, pool_scale, out_weight,
                   mix_gain, ffn_gain, gate_weight, up_weight, down_weight):
    if not pairs_fit(sizes, stream, in_weight, pool_weight, out_weight, gate_weight, down_weight):
        return ring_on_device(sizes, stream, in_weight, pool_weight, pool_scale, out_weight,
                              mix_gain, ffn_gain, gate_weight, up_weight, down_weight)
    reps, fs, tp = sizes
    tokens, width = stream.shape
    rows, sub = tokens // 2, width // 2
    features = width * tp
    channels = in_weight.shape[1]
    blocks = gate_weight.shape[1] // LANES
    units = 2 * LANES * (blocks - blocks // 2)
    bf, f32 = jnp.bfloat16, jnp.float32
    vmem = pl.BlockSpec(memory_space=pltpu.VMEM)
    hbm = pl.BlockSpec(memory_space=pltpu.HBM)
    dma = pltpu.SemaphoreType.DMA
    flops = 2 * tokens * (2 * features * channels + 3 * features * gate_weight.shape[1])
    return pl.pallas_call(
        functools.partial(pair_kernel, sizes),
        out_shape=jax.ShapeDtypeStruct(stream.shape, bf),
        in_specs=[hbm] * 10,
        out_specs=vmem,
        scratch_shapes=[
            pltpu.VMEM((in_weight.shape[0] * fs, 2 * channels), bf),
            pltpu.VMEM((2 * out_weight.shape[0], out_weight.shape[1] * fs), bf),
            pltpu.VMEM((up_weight.shape[0] * fs, units), bf),
            pltpu.VMEM((gate_weight.shape[0] * fs, units), bf),
            pltpu.VMEM((units, down_weight.shape[1] * fs), bf),
            pltpu.VMEM((rows, features), bf),
            pltpu.VMEM((rows, features), bf),
            pltpu.VMEM((rows, 2 * channels), bf),
            pltpu.VMEM((2 * rows, units), bf),
            pltpu.VMEM((2 * rows, units), f32),
            pltpu.VMEM((2 * rows, units), f32),
            pltpu.VMEM((2 * rows, features), bf),
            pltpu.VMEM((2 * rows, features), bf),
            pltpu.VMEM(pool_weight.shape, bf),
            pltpu.VMEM((channels,), bf),
            pltpu.VMEM(mix_gain.shape, bf),
            pltpu.VMEM(ffn_gain.shape, bf),
            pltpu.VMEM(pool_weight.shape, bf),
            pltpu.VMEM((channels,), bf),
            pltpu.VMEM((rows, 2 * width), f32),
            pltpu.VMEM((rows, 2 * width), bf),
            pltpu.VMEM((rows, 2 * width), bf),
            pltpu.VMEM((4, 2 * rows, sub), f32),
            pltpu.VMEM((4, 2 * rows, sub), bf),
            pltpu.VMEM((4, 2 * rows, sub), bf),
            pltpu.VMEM((2, 2, rows, sub), bf),
            pltpu.VMEM((2, 2, rows, sub), bf),
            pltpu.VMEM((2 * rows, sub), f32),
            pltpu.VMEM((2, rows, sub), bf),
            pltpu.VMEM((2, rows, sub), bf),
            pltpu.VMEM((2, rows, sub), f32),
            pltpu.VMEM((2, rows, sub), bf),
            pltpu.VMEM((2, rows, sub), bf),
            pltpu.VMEM((2, rows, sub), bf),
            pltpu.VMEM((2, rows, sub), bf),
            dma((24,)), dma((24,)), dma((2, 2)), dma((24,)), dma((24,)),
            dma((27,)), dma((27,)), dma((10,)),
            dma((3,)), dma((3,)), dma((2,)), dma((2,)), dma((2,)), dma((3,)), dma((3,)),
            dma((4, 2)), dma((4, 2)), dma((2, 2)), dma((2, 2)), dma((2,)), dma((2,)),
            dma((3,)), dma((3,)), dma((2, 3)),
        ],
        compiler_params=pltpu.CompilerParams(
            collective_id=0, has_side_effects=True, vmem_limit_bytes=52 * 1024 * 1024),
        cost_estimate=pl.CostEstimate(flops=flops, bytes_accessed=flops // 512, transcendentals=0),
    )(*[pltpu.with_memory_space_constraint(v, pltpu.HBM) for v in (
        stream, in_weight, out_weight, up_weight, gate_weight, down_weight, pool_weight,
        pool_scale, mix_gain, ffn_gain)])


def solution(mesh):
    sizes = tuple(mesh.shape[name] for name in ("rep", "fs", "tp"))
    return jax.shard_map(
        functools.partial(pair_on_device, sizes),
        mesh=mesh,
        in_specs=(
            P(("rep", "fs"), "tp"),
            P("fs", "tp"),
            P("tp", None, None),
            P("tp"),
            P("tp", "fs"),
            P(),
            P(),
            P("fs", "tp"),
            P("fs", "tp"),
            P("tp", "fs"),
        ),
        out_specs=P(("rep", "fs"), "tp"),
        check_vma=False,
    )
```

```python
import functools

import jax
import jax.numpy as jnp
from jax import lax
from jax.experimental import pallas as pl
from jax.experimental.pallas import tpu as pltpu
from jax.sharding import PartitionSpec as P

SEQ = 128
EPSILON = 1e-06
MESH = pl.DeviceIdType.MESH
BY_ROWS = (True, False, True, True, False)
PIECES = ((0, 0), (1, 0), (2, 0), (3, 0), (2, 1), (3, 1), (4, 0), (4, 1))
CHUNKS = (1, 1, 2, 2, 2)


def ring_kernel(sizes, stream, in_w, out_w, up_w, gate_w, down_w, pool_w, scale,
           mix_gain, ffn_gain, result,
           in_all, out_all, up_all, gate_all, down_all,
           rows_all, normed, group_out, hidden, middle, mid_all,
           mix_send, mix_recv, ffn_send, ffn_recv,
           ring_send, ring_recv, fwd_send, fwd_recv, own_sem,
           tp_send, tp_recv, keep_sem):
    reps, fs, tp = sizes
    half = fs // 2
    my_rep, me, my_tp = lax.axis_index("rep"), lax.axis_index("fs"), lax.axis_index("tp")
    own = (in_w, out_w, up_w, gate_w, down_w)
    full = (in_all, out_all, up_all, gate_all, down_all)
    tokens, width = stream.shape

    def turn(at, by, count):
        return lax.rem(at + by + count, count)

    def piece(which, owner, row, count):
        block_rows, block_cols = own[which].shape
        if BY_ROWS[which]:
            return full[which].at[pl.ds(pl.multiple_of(owner * block_rows + row, 16), count), :]
        return full[which].at[pl.ds(pl.multiple_of(row, 16), count),
                              pl.ds(pl.multiple_of(owner * block_cols, 128), block_cols)]

    def span(number, step, way):
        which, chunk = PIECES[number]
        rows = own[which].shape[0]
        cut = rows % (CHUNKS[which] * reps * 2 * 16) == 0
        count = rows // CHUNKS[which] if cut else (rows, 0)[chunk]
        row = chunk * (rows // CHUNKS[which])
        count = count // reps
        row = row + my_rep * count
        if step == half:
            count = count // 2
            row = row + way * count
        return which, row, count

    def empty(number):
        return span(number, 1, 0)[2] == 0

    def ring(number, step, way):
        which, row, count = span(number, step, way)
        sign = 1 - 2 * way
        owner = turn(me, -sign * (step - 1), fs)
        if step == 1:
            source = own[which].at[pl.ds(pl.multiple_of(row, 16), count), :]
        else:
            source = piece(which, owner, row, count)
        return pltpu.make_async_remote_copy(
            src_ref=source, dst_ref=piece(which, owner, row, count),
            send_sem=ring_send.at[number, step - 1, way],
            recv_sem=ring_recv.at[number, step - 1, way],
            device_id={"fs": turn(me, sign, fs)}, device_id_type=MESH)

    def forward(number, step, way, peer):
        which, row, count = span(number, step, way)
        block = piece(which, turn(me, -(1 - 2 * way) * step, fs), row, count)
        return pltpu.make_async_remote_copy(
            src_ref=block, dst_ref=block,
            send_sem=fwd_send.at[number, peer - 1, step - 1, way],
            recv_sem=fwd_recv.at[number, peer - 1, step - 1, way],
            device_id={"rep": turn(my_rep, peer, reps)}, device_id_type=MESH)

    def begin(*numbers):
        for number in numbers:
            if not empty(number):
                for way in (0, 1):
                    ring(number, 1, way).start()

    def advance(number, step):
        if empty(number):
            return
        for way in (0, 1):
            ring(number, step, way).wait_recv()
            if step < half:
                ring(number, step + 1, way).start()
            for peer in range(1, reps):
                forward(number, step, way, peer).start()

    def early(*numbers):
        for number in numbers:
            for step in range(1, half):
                advance(number, step)

    def late(*numbers):
        for number in numbers:
            advance(number, half)

    def arrived(*numbers):
        for number in numbers:
            if PIECES[number][1] == 0:
                keeps[PIECES[number][0]].wait()
            if empty(number):
                continue
            for step in range(1, half + 1):
                for way in (0, 1):
                    for peer in range(1, reps):
                        forward(number, step, way, peer).wait()

    def tp_copy(stage, offset, source, target):
        return pltpu.make_async_remote_copy(
            src_ref=source, dst_ref=target,
            send_sem=tp_send.at[stage, offset - 1], recv_sem=tp_recv.at[stage, offset - 1],
            device_id={"tp": turn(my_tp, offset, tp)}, device_id_type=MESH)

    def feature_cols(owner):
        return pl.ds(pl.multiple_of(owner * width, 128), width)

    barrier = pltpu.get_barrier_semaphore()
    greeted = 0
    for name, at, count, offsets in (
            ("fs", me, fs, (1, -1)),
            ("tp", my_tp, tp, range(1, tp)),
            ("rep", my_rep, reps, range(1, reps))):
        for offset in offsets:
            pl.semaphore_signal(barrier, inc=1, device_id={name: turn(at, offset, count)},
                                device_id_type=MESH)
            greeted += 1
    pl.semaphore_wait(barrier, greeted)

    begin(0, 1)
    stream_sends = []
    for offset in range(1, tp):
        copy = tp_copy(0, offset, stream, rows_all.at[:, feature_cols(my_tp)])
        copy.start()
        stream_sends.append(copy)
    keeps = []
    for which in range(len(own)):
        keep = pltpu.make_async_copy(
            own[which], piece(which, me, 0, own[which].shape[0]), own_sem.at[which])
        keep.start()
        keeps.append(keep)
    keep_stream = pltpu.make_async_copy(
        stream, rows_all.at[:, feature_cols(my_tp)], keep_sem)
    keep_stream.start()
    early(0, 1)
    begin(2, 3, 4)
    late(0, 1)

    def norm_into(source, gain, target):
        tile = 64

        def body(i, carry):
            at = pl.ds(pl.multiple_of(i * tile, tile), tile)
            wide = source[at, :].astype(jnp.float32)
            mean = jnp.mean(wide * wide, axis=-1, keepdims=True)
            target[at, :] = (wide * lax.rsqrt(mean + EPSILON)
                             * gain[...].astype(jnp.float32)).astype(jnp.bfloat16)
            return carry

        lax.fori_loop(0, tokens // tile, body, 0)

    keep_stream.wait()
    for copy in stream_sends:
        copy.wait()
    norm_into(rows_all, mix_gain, normed)
    arrived(0)

    local_groups, group_dim = pool_w.shape[0], pool_w.shape[1]
    at_row = lax.broadcasted_iota(jnp.int32, (SEQ, SEQ), 0)
    at_col = lax.broadcasted_iota(jnp.int32, (SEQ, SEQ), 1)
    insides, inverses = [], []
    for g in range(local_groups):
        group = my_tp * local_groups + g
        level = lax.div(4 * group, local_groups * tp)
        reach = jnp.int32(2)
        for bit in range(1, 4):
            reach = jnp.where(level >= bit, jnp.int32(2 << bit), reach)
        inside = (at_col <= at_row) & (at_col > at_row - reach)
        insides.append(jnp.where(inside, 1.0, 0.0).astype(jnp.bfloat16))
        inverses.append(jnp.minimum(at_row + 1, reach).astype(jnp.float32)[:, :1])

    def mix(i, carry):
        at = pl.ds(pl.multiple_of(i * SEQ, SEQ), SEQ)
        pooled = jnp.dot(normed[at, :], in_all[...],
                         preferred_element_type=jnp.float32).astype(jnp.bfloat16)
        for g in range(local_groups):
            cols = slice(g * group_dim, (g + 1) * group_dim)
            part = pooled[:, cols]
            sums = jnp.dot(insides[g], part, preferred_element_type=jnp.float32)
            contrast = (sums / inverses[g] - part.astype(jnp.float32)).astype(jnp.bfloat16)
            mixed = jnp.dot(contrast, pool_w[g], preferred_element_type=jnp.float32)
            group_out[at, cols] = (mixed * scale[:, cols].astype(jnp.float32)).astype(jnp.bfloat16)
        return carry

    lax.fori_loop(0, tokens // SEQ, mix, 0)

    arrived(1)
    early(2)

    def spread(operand, weights, stage, sends, tile):
        def block(owner, target):
            def body(i, carry):
                at = pl.ds(pl.multiple_of(i * tile, tile), tile)
                target[at, :] = jnp.dot(operand[at, :], weights[:, feature_cols(owner)],
                                        preferred_element_type=jnp.float32).astype(jnp.bfloat16)
                return carry
            lax.fori_loop(0, tokens // tile, body, 0)

        copies = []
        recv = mix_recv if stage == 1 else ffn_recv
        for offset in sorted(range(1, tp), key=lambda o: -min(o, tp - o)):
            block(turn(my_tp, offset, tp), sends.at[offset - 1])
            copy = tp_copy(stage, offset, sends.at[offset - 1], recv.at[offset - 1])
            copy.start()
            copies.append(copy)
        block(my_tp, sends.at[tp - 1])
        return copies

    def gather_sum(base, recv, sends, target):
        tile = 64

        def body(i, carry):
            at = pl.ds(pl.multiple_of(i * tile, tile), tile)
            total = sends[tp - 1, at, :].astype(jnp.float32)
            for k in range(tp - 1):
                total = total + recv[k, at, :].astype(jnp.float32)
            target[at, :] = (base[at, :].astype(jnp.float32) + total).astype(jnp.bfloat16)
            return carry

        lax.fori_loop(0, tokens // tile, body, 0)

    mix_copies = spread(group_out, out_all, 1, mix_send, tokens // 2)
    early(3)
    begin(5)
    for copy in mix_copies:
        copy.wait()
    gather_sum(stream, mix_recv, mix_send, middle)
    keep_middle = pltpu.make_async_copy(middle, mid_all.at[:, feature_cols(my_tp)], keep_sem)
    keep_middle.start()
    middle_copies = []
    for offset in range(1, tp):
        copy = tp_copy(2, offset, middle, mid_all.at[:, feature_cols(my_tp)])
        copy.start()
        middle_copies.append(copy)
    early(4)
    begin(6, 7)
    late(2, 3)
    keep_middle.wait()
    for copy in middle_copies:
        copy.wait()
    norm_into(mid_all, ffn_gain, normed)
    early(5)
    late(4)
    early(6)
    late(5)
    early(7)
    late(6)
    arrived(2, 3, 4, 5)
    tile = tokens // 2

    def gated(i, carry):
        at = pl.ds(pl.multiple_of(i * tile, tile), tile)
        values = normed[at, :]
        gate = jnp.dot(values, gate_all[...], preferred_element_type=jnp.float32)
        up = jnp.dot(values, up_all[...], preferred_element_type=jnp.float32)
        hidden[at, :] = (gate / (1.0 + jnp.exp(-gate)) * up).astype(jnp.bfloat16)
        return carry

    lax.fori_loop(0, tokens // tile, gated, 0)
    late(7)
    arrived(6, 7)
    ffn_copies = spread(hidden, down_all, 3, ffn_send, tokens // 2)
    for number in range(len(PIECES)):
        if not empty(number):
            for step in range(1, half + 1):
                for way in (0, 1):
                    ring(number, step, way).wait_send()
    for copy in ffn_copies:
        copy.wait()
    gather_sum(middle, ffn_recv, ffn_send, result)


def ring_on_device(sizes, stream, in_weight, pool_weight, pool_scale, out_weight,
              mix_gain, ffn_gain, gate_weight, up_weight, down_weight):
    reps, fs, tp = sizes
    half = fs // 2
    tokens, width = stream.shape
    features = width * tp
    own = (in_weight, out_weight, up_weight, gate_weight, down_weight)
    full = [pltpu.VMEM((w.shape[0] * fs, w.shape[1]) if by_rows else (w.shape[0], w.shape[1] * fs),
                       jnp.bfloat16) for w, by_rows in zip(own, BY_ROWS)]
    units = gate_weight.shape[1]
    bf = jnp.bfloat16
    vmem = pl.BlockSpec(memory_space=pltpu.VMEM)
    hbm = pl.BlockSpec(memory_space=pl.ANY)
    dma = pltpu.SemaphoreType.DMA
    flops = 2 * tokens * (2 * features * in_weight.shape[1] + 3 * features * units)
    return pl.pallas_call(
        functools.partial(ring_kernel, sizes),
        out_shape=jax.ShapeDtypeStruct(stream.shape, bf),
        in_specs=[vmem] + [hbm] * 5 + [vmem] * 4,
        out_specs=vmem,
        scratch_shapes=full + [
            pltpu.VMEM((tokens, features), bf),
            pltpu.VMEM((tokens, features), bf),
            pltpu.VMEM((tokens, in_weight.shape[1]), bf),
            pltpu.VMEM((tokens, units), bf),
            pltpu.VMEM((tokens, width), bf),
            pltpu.VMEM((tokens, features), bf),
            pltpu.VMEM((tp, tokens, width), bf),
            pltpu.VMEM((tp - 1, tokens, width), bf),
            pltpu.VMEM((tp, tokens, width), bf),
            pltpu.VMEM((tp - 1, tokens, width), bf),
            dma((len(PIECES), half, 2)),
            dma((len(PIECES), half, 2)),
            dma((len(PIECES), max(reps - 1, 1), half, 2)),
            dma((len(PIECES), max(reps - 1, 1), half, 2)),
            dma((len(own),)),
            dma((4, tp - 1)),
            dma((4, tp - 1)),
            dma(()),
        ],
        compiler_params=pltpu.CompilerParams(
            collective_id=0, has_side_effects=True, vmem_limit_bytes=64 * 1024 * 1024 - 65536),
        cost_estimate=pl.CostEstimate(flops=flops, bytes_accessed=flops // 512, transcendentals=0),
    )(stream, in_weight, out_weight, up_weight, gate_weight, down_weight, pool_weight,
      pool_scale.reshape(1, -1), mix_gain.reshape(1, -1), ffn_gain.reshape(1, -1))


IN, OUT, UP, GATE, DOWN = range(5)
LANES = 128


def pair_kernel(sizes, stream, in_w, out_w, up_w, gate_w, down_w, pool_in, scale_in,
                mix_gain_in, ffn_gain_in, result,
                in_all, out_all, up_all, gate_all, down_all,
                rows_all, normed, group_out, hidden, gate_acts, up_acts, mid_all, normed_ffn,
                pool_w, scale, mix_gain, ffn_gain, pool_sib, scale_sib,
                mix_own, mix_send, mix_recv, ffn_own, ffn_send, ffn_recv, pair_send, pair_recv,
                stage, cross_send, cross_recv, cross_own, late_send, late_recv,
                last_send, last_recv,
                z_send, z_recv, pass_send, y_send, y_recv, d_send, d_recv, own_sem,
                in_send, in_recv, pool_send, pool_recv, mix_sems, mid_send, mid_recv,
                x_send, x_recv, p_send, p_recv, l_send, l_recv, c_send, c_recv, late_sems):
    reps, fs, tp = sizes
    y, z, lane_id = lax.axis_index("rep"), lax.axis_index("fs"), lax.axis_index("tp")
    x, core = lax.div(lane_id, 2), lax.rem(lane_id, 2)
    own = (in_w, out_w, up_w, gate_w, down_w)
    full = (in_all, out_all, up_all, gate_all, down_all)
    tokens, width = stream.shape
    rows = tokens // 2
    wide = 2 * width
    seat, pair = lax.rem(z, 2), lax.div(z, 2)
    peer = z + 1 - 2 * seat
    near = jnp.where(pair == 0, 2, 1)
    far = jnp.where(pair == 0, 3, 0)
    inner = (z == 1) | (z == 2)
    f32, bf16 = jnp.float32, jnp.bfloat16

    blocks = gate_w.shape[1] // LANES
    few, many = blocks // 2, blocks - blocks // 2

    SIB = {"tp": lane_id + 1 - 2 * core}
    XPEER = {"tp": lane_id + 2 - 4 * x}
    XSIB = {"tp": 2 * (1 - x) + 1 - core}
    YPEER = {"rep": 1 - y}
    ZPEER = {"fs": peer}

    def at_least(value, multiple):
        return pl.multiple_of(value, multiple)

    def remote(source, target, send, recv, device):
        return pltpu.make_async_remote_copy(
            src_ref=source, dst_ref=target, send_sem=send, recv_sem=recv,
            device_id=device, device_id_type=MESH)

    def sized(which, roomy, act):
        if which in (IN, OUT) or few == many:
            act(many)
            return

        @pl.when(roomy)
        def _():
            act(many)

        @pl.when(jnp.logical_not(roomy))
        def _():
            act(few)

    slot_of = {IN: 0, OUT: 1, GATE: 2, UP: 3, DOWN: 5}

    def role_of(source):
        return jnp.where(source == peer, 0, jnp.where(source == near, 1,
                         jnp.where(source == far, 2, 3)))

    def flow(which, part, role):
        return 3 * (slot_of[which] + (part or 0)) + role

    def beside_flow(which, source, half, part):
        if which != DOWN:
            return 4 * (IN, OUT, GATE, UP).index(which) + role_of(source)
        if source is z:
            return 16 + half
        return 18 + 3 * role_of(source) + (0 if part is None else 1 + part)

    def extent(which):
        return own[which].shape[1 if which == DOWN else 0]

    def half_span(which, half, part=None):
        size = extent(which) // 2
        if half is None:
            return 0, 2 * size
        if part is None:
            return half * size, size
        return half * size + min(part, 1) * (size // 2), size // 2

    def unit_rows(part, count):
        upper = count - count // 2
        return {1: (0, upper), 2: (upper, count - upper)}.get(part, (0, count))

    def parts(which):
        return {UP: (0, 1), DOWN: (0, 1, 2)}.get(which, (None,))

    def place(which, source, span, core_at, count, part=None):
        block_rows, block_cols = own[which].shape
        ref = full[which]
        start, size = span
        if which == OUT:
            return ref.at[pl.ds(at_least(core_at * block_rows + start, 16), size),
                          pl.ds(at_least(source * block_cols, LANES), block_cols)]
        if which == IN:
            return ref.at[pl.ds(at_least(source * block_rows + start, 16), size),
                          pl.ds(at_least(core_at * block_cols, LANES), block_cols)]
        first = core_at * (count * LANES)
        if which == DOWN:
            skip, taken = unit_rows(part, count)
            return ref.at[pl.ds(at_least(first + skip * LANES, LANES), taken * LANES),
                          pl.ds(at_least(source * block_cols + start, LANES), size)]
        return ref.at[pl.ds(at_least(source * block_rows + start, 16), size),
                      pl.ds(at_least(first, LANES), count * LANES)]

    def held(which, span, roomy, count, part=None):
        ref = own[which]
        start, size = span
        if which in (IN, OUT):
            return ref.at[pl.ds(at_least(start, 16), size), :]
        first = jnp.where(roomy, 0, many * LANES)
        if which == DOWN:
            skip, taken = unit_rows(part, count)
            return ref.at[pl.ds(at_least(first + skip * LANES, LANES), taken * LANES),
                          pl.ds(at_least(start, LANES), size)]
        return ref.at[pl.ds(at_least(start, 16), size),
                      pl.ds(at_least(first, LANES), count * LANES)]

    def z_copies(which, dest, step, only=None):
        roomy = (dest == 1) | (dest == 2)

        def act(n):
            for part in parts(which) if only is None else only:
                span = half_span(which, y, part)
                there = jnp.where(dest == peer, 0, jnp.where(inner, 1, 2))
                copy = remote(held(which, span, roomy, n, part),
                              place(which, z, span, core, n, part),
                              z_send.at[flow(which, part, role_of(dest))],
                              z_recv.at[flow(which, part, there)], {"fs": dest})
                {"start": copy.start, "send": copy.wait_send}[step]()
        sized(which, roomy, act)

    def z_start(which, dest, only=None):
        z_copies(which, dest, "start", only)

    def z_sent(which, dest):
        z_copies(which, dest, "send")

    def z_pass(which, source):
        block = place(which, source, half_span(which, y), core, many)
        return remote(block, block, pass_send.at[which, lax.rem(source, 2)],
                      z_recv.at[flow(which, None, role_of(source))], ZPEER)

    def arrived(which, source, part):
        def act(n):
            block = place(which, source, half_span(which, y, part), core, n, part)
            at = flow(which, part, role_of(source))
            remote(block, block, y_send.at[at], z_recv.at[at], YPEER).wait_recv()
        sized(which, inner, act)

    def across(which, source, part, step):
        def act(n):
            half = 1 - y if step == "recv" else y
            block = place(which, source, half_span(which, half, part), core, n, part)
            at = flow(which, part, role_of(source))
            copy = remote(block, block, y_send.at[at], y_recv.at[at], YPEER)
            {"start": copy.start, "recv": copy.wait_recv, "send": copy.wait_send}[step]()
        sized(which, inner, act)

    def beside(which, source, half, step, mine=False, part=None):
        at = beside_flow(which, source, half, part)
        whose = 1 - core if step == "recv" else core

        def act(n):
            span = half_span(which, half, part)
            block = place(which, source, span, whose, n)
            start = held(which, span, inner, n) if mine else block
            copy = remote(start, block, d_send.at[at], d_recv.at[at], SIB)
            {"start": copy.start, "recv": copy.wait_recv, "send": copy.wait_send}[step]()
        sized(which, inner, act)

    def keep(which, step):
        def act(n):
            span = half_span(which, None)
            copy = pltpu.make_async_copy(held(which, span, inner, n),
                                         place(which, z, span, core, n), own_sem.at[which])
            {"start": copy.start, "wait": copy.wait}[step]()
        sized(which, inner, act)

    def relay(which, source, only=None):
        for part in parts(which):
            if only is None or part in only:
                arrived(which, source, part)
                across(which, source, part, "start")

    def share(which, source):
        for part in parts(which):
            across(which, source, part, "recv")
        beside(which, source, None, "start")

    def feature_cols(owner):
        return pl.ds(at_least(owner * width, LANES), width)

    def token_rows(half):
        return pl.ds(at_least(half * rows, 16), rows)

    def stream_copy(number, device, half):
        return remote(stream.at[token_rows(half), :], rows_all.at[:, feature_cols(lane_id)],
                      in_send.at[number], in_recv.at[number], device)

    small_copies = [pltpu.make_async_copy(source, target, own_sem.at[6 + number])
                    for number, (source, target) in enumerate((
                        (mix_gain_in, mix_gain), (ffn_gain_in, ffn_gain),
                        (pool_in, pool_w), (scale_in, scale)))]
    for copy in small_copies:
        copy.start()

    barrier = pltpu.get_barrier_semaphore()
    greeted = 0
    for device in (SIB, XPEER, XSIB, YPEER, ZPEER, {"fs": near}, {"fs": far}):
        pl.semaphore_signal(barrier, inc=1, device_id=device, device_id_type=MESH)
        greeted += 1
    pl.semaphore_wait(barrier, greeted)

    outer = jnp.logical_not(inner)
    z_start(IN, near)
    z_start(IN, peer)
    stream_copies = [stream_copy(0, XPEER, core), stream_copy(1, XSIB, 1 - core),
                     stream_copy(2, SIB, 1 - core)]
    for copy in stream_copies:
        copy.start()
    z_start(OUT, near)
    z_start(OUT, peer)
    keep(IN, "start")
    beside(IN, z, None, "start", mine=True)
    pool_copy = remote(pool_in, pool_sib, pool_send.at[0], pool_recv.at[0], SIB)
    scale_copy = remote(scale_in, scale_sib, pool_send.at[1], pool_recv.at[1], SIB)
    pool_copy.start()
    scale_copy.start()

    @pl.when(inner)
    def _():
        z_start(GATE, near)
        z_start(GATE, far)
        z_start(UP, near)

    @pl.when(outer)
    def _():
        z_start(GATE, peer)
        z_start(GATE, far)
        z_start(UP, far)
        z_start(UP, peer)

    for which in (OUT, GATE, UP, DOWN):
        keep(which, "start")
        for half in (0, 1) if which == DOWN else (None,):
            beside(which, z, half, "start", mine=True)

    own_rows = pltpu.make_async_copy(stream.at[token_rows(core), :],
                                     rows_all.at[:, feature_cols(lane_id)], own_sem.at[5])
    own_rows.start()

    def take(which):
        relay(which, peer)
        for source in (near, far):
            arrived(which, source, None)

            @pl.when(inner)
            def _():
                z_pass(which, source).start()
            across(which, source, None, "start")

    take(IN)

    @pl.when(inner)
    def _():
        take(OUT)

    def norm_into(source, gain, target, first, count):
        tile = 64

        def body(i, carry):
            at = pl.ds(at_least(first + i * tile, tile), tile)
            values = source[at, :].astype(f32)
            mean = jnp.mean(values * values, axis=-1, keepdims=True)
            target[at, :] = (values * lax.rsqrt(mean + EPSILON)
                             * gain[...].astype(f32).reshape(1, -1)).astype(bf16)
            return carry

        lax.fori_loop(0, count // tile, body, 0)

    own_rows.wait()
    for copy in small_copies:
        copy.wait()
    for copy in stream_copies:
        copy.wait()
    norm_into(rows_all, mix_gain, normed, 0, rows)
    for source in (peer, near, far):
        share(IN, source)

    @pl.when(outer)
    def _():
        take(OUT)

    pool_copy.wait()
    scale_copy.wait()
    for source in (z, peer, near, far):
        beside(IN, source, None, "recv")
    keep(IN, "wait")

    local_groups, group_dim = pool_w.shape[0], pool_w.shape[1]
    at_row = lax.broadcasted_iota(jnp.int32, (SEQ, SEQ), 0)
    at_col = lax.broadcasted_iota(jnp.int32, (SEQ, SEQ), 1)
    pooled = jnp.dot(normed[...], in_all[...], preferred_element_type=f32).astype(bf16)
    for g in range(2 * local_groups):
        owner, place_in = divmod(g, local_groups)
        group = x * 2 * local_groups + g
        level = lax.div(4 * group, local_groups * tp)
        reach = jnp.int32(2)
        for bit in range(1, 4):
            reach = jnp.where(level >= bit, jnp.int32(2 << bit), reach)
        inside = jnp.where((at_col <= at_row) & (at_col > at_row - reach), 1.0, 0.0).astype(bf16)
        counts = jnp.minimum(at_row + 1, reach).astype(f32)[:, :1]
        is_own = core == owner
        cols = slice(g * group_dim, (g + 1) * group_dim)
        own_cols = slice(place_in * group_dim, (place_in + 1) * group_dim)
        weight = jnp.where(is_own, pool_w[place_in], pool_sib[place_in])
        factor = jnp.where(is_own, scale[own_cols].astype(f32).reshape(1, -1),
                           scale_sib[own_cols].astype(f32).reshape(1, -1))
        for s in range(rows // SEQ):
            at = slice(s * SEQ, (s + 1) * SEQ)
            part = pooled[at, cols]
            sums = jnp.dot(inside, part, preferred_element_type=f32)
            contrast = (sums / counts - part.astype(f32)).astype(bf16)
            mixed = jnp.dot(contrast, weight, preferred_element_type=f32)
            group_out[at, cols] = (mixed * factor).astype(bf16)

    for source in (peer, near, far):
        share(OUT, source)
    for source in (z, peer, near, far):
        beside(OUT, source, None, "recv")
    keep(OUT, "wait")

    def half_cols(owner):
        return pl.ds(at_least(owner * wide, LANES), wide)

    mix_send[...] = jnp.dot(group_out[...], out_all[:, half_cols(1 - x)],
                            preferred_element_type=f32).astype(bf16)
    mix_copy = remote(mix_send, mix_recv, mix_sems.at[0], mix_sems.at[1], XPEER)
    mix_copy.start()
    mix_own[...] = jnp.dot(group_out[...], out_all[:, half_cols(x)], preferred_element_type=f32)

    @pl.when(inner)
    def _():
        relay(GATE, peer)
        relay(GATE, near)

    @pl.when(outer)
    def _():
        relay(GATE, far)

    mix_copy.wait()
    mid_rows = pl.ds(at_least(seat * rows, 16), rows)
    mid_all[mid_rows, half_cols(x)] = (
        rows_all[:, half_cols(x)].astype(f32) + (mix_own[...] + mix_recv[...].astype(f32))).astype(bf16)

    def mid_copy(number, block, device):
        view = mid_all.at[pl.ds(at_least(block * rows, 16), rows), half_cols(x)]
        return remote(view, view, mid_send.at[number], mid_recv.at[number], device)

    to_pair, to_x, to_x_later = mid_copy(0, seat, ZPEER), mid_copy(1, seat, XPEER), mid_copy(2, 1 - seat, XPEER)
    to_pair.start()
    to_x.start()

    @pl.when(inner)
    def _():
        z_start(GATE, peer)
        z_start(UP, peer)
        z_start(DOWN, near, (0,))
        z_start(UP, far)
        z_start(DOWN, far)
        z_start(DOWN, near, (1, 2))
        share(GATE, peer)
        share(GATE, near)
        relay(UP, peer)
        relay(UP, near)

    @pl.when(outer)
    def _():
        z_start(GATE, near)
        z_start(UP, near)
        share(GATE, far)
        relay(UP, far)
        relay(GATE, near)

    to_pair.wait_recv()
    to_x_later.start()

    @pl.when(inner)
    def _():
        z_start(DOWN, peer)
        share(UP, peer)
        relay(DOWN, near, (0,))

    @pl.when(outer)
    def _():
        z_start(DOWN, peer)
        z_start(DOWN, near)
        z_start(DOWN, far)
        share(UP, far)
        share(GATE, near)

    to_x.wait_recv()
    norm_into(mid_all, ffn_gain, normed_ffn, seat * rows, rows)

    @pl.when(inner)
    def _():
        share(UP, near)
        relay(GATE, far)

    @pl.when(outer)
    def _():
        relay(GATE, peer)

    to_x_later.wait_recv()
    norm_into(mid_all, ffn_gain, normed_ffn, (1 - seat) * rows, rows)

    depth = gate_all.shape[0] // 2
    pair_at = pl.ds(at_least(pair * depth, LANES), depth)
    cross_at = pl.ds(at_least((1 - pair) * depth, LANES), depth)
    early_at = pl.ds(at_least(jnp.where(inner, pair, 1 - pair) * depth, LANES), depth)
    later_at = pl.ds(at_least(jnp.where(inner, 1 - pair, pair) * depth, LANES), depth)
    tile = rows

    def by_tiles(body):
        def all_tiles(count):
            wide_units = 2 * count * LANES

            def step(i, carry):
                body(pl.ds(at_least(i * tile, tile), tile), wide_units)
                return carry
            lax.fori_loop(0, 2 * rows // tile, step, 0)
        sized(UP, inner, all_tiles)

    def partial_dot(at, depth_at, weights, n):
        return jnp.dot(normed_ffn[at, depth_at], weights[depth_at, :n], preferred_element_type=f32)

    def gate_first(at, n):
        gate_acts[at, :n] = partial_dot(at, early_at, gate_all, n)

    def gate_second(at, n):
        gate = gate_acts[at, :n] + partial_dot(at, later_at, gate_all, n)
        gate_acts[at, :n] = gate / (1.0 + jnp.exp(-gate))

    def up_first(at, n):
        up_acts[at, :n] = partial_dot(at, pair_at, up_all, n)

    def up_second(at, n):
        up = up_acts[at, :n] + partial_dot(at, cross_at, up_all, n)
        hidden[at, :n] = (gate_acts[at, :n] * up).astype(bf16)

    keep(GATE, "wait")
    for source in (jnp.where(inner, z, far), jnp.where(inner, peer, near)):
        beside(GATE, source, None, "recv")
    by_tiles(gate_first)

    @pl.when(inner)
    def _():
        relay(UP, far)
        share(GATE, far)

    @pl.when(outer)
    def _():
        relay(UP, peer)
        share(GATE, peer)

    for source in (jnp.where(inner, near, z), jnp.where(inner, far, peer)):
        beside(GATE, source, None, "recv")
    by_tiles(gate_second)

    @pl.when(outer)
    def _():
        share(UP, peer)
        relay(UP, near)

    keep(UP, "wait")
    for source in (z, peer):
        beside(UP, source, None, "recv")
    by_tiles(up_first)

    relay(DOWN, peer)

    @pl.when(inner)
    def _():
        share(UP, far)

    @pl.when(outer)
    def _():
        share(UP, near)

    beside(DOWN, peer, y, "start")

    for source in (near, far):
        beside(UP, source, None, "recv")
    by_tiles(up_second)

    sub = width // 2
    order = (z, peer, far, near)
    keeps_early = x == pair

    def half_of(turn):
        return y if turn == 0 else 1 - y

    half_sub = sub // 2

    def piece_cols(o, turn, part):
        start = order[o] * width + half_of(turn) * sub
        if part is None:
            return pl.ds(at_least(start, LANES), sub)
        return pl.ds(at_least(start + part * half_sub, LANES), half_sub)

    def lanes(part):
        return slice(0, sub) if part is None else slice(part * half_sub, (part + 1) * half_sub)

    ours = pl.ds(at_least(seat * rows, 16), rows)
    theirs = pl.ds(at_least((1 - seat) * rows, 16), rows)

    OWN, PEER, FAR, NEAR = range(4)

    def kept(o):
        return keeps_early if o < FAR else jnp.logical_not(keeps_early)

    def column_block(o, turn, part, n):
        values = jnp.dot(hidden[:, :n], down_all[:n, piece_cols(o, turn, part)],
                         preferred_element_type=f32)
        if (o, turn) == (NEAR, 1):
            stage[:, lanes(part)] = values
            cross_send[turn, :, lanes(part)] = stage[theirs, lanes(part)].astype(bf16)
            cross_copy(turn, part).start()
            cross_own[turn, :, lanes(part)] = stage[ours, lanes(part)]
            return
        slot = 2 * (o % 2) + turn

        @pl.when(kept(o))
        def _():
            ffn_own[slot] = values

        @pl.when(jnp.logical_not(kept(o)))
        def _():
            ffn_send[slot] = values.astype(bf16)
            x_copy(slot, 0).start()
            x_copy(slot, 1).start()

    def cross_copy(turn, part):
        at, number = lanes(part), turn + (part or 0)
        return remote(cross_send.at[turn, :, at], cross_recv.at[turn, :, at],
                      c_send.at[number], c_recv.at[number], ZPEER)

    def late_copy(turn, part):
        at, number = lanes(part), turn + (part or 0)
        return remote(late_send.at[turn, :, at], late_recv.at[turn, :, at],
                      late_sems.at[0, number], late_sems.at[1, number], XPEER)

    def combine(turn, part=None):
        at = lanes(part)
        cross_copy(turn, part).wait_recv()

        @pl.when(keeps_early)
        def _():
            late_send[turn, :, at] = (cross_own[turn, :, at]
                                      + cross_recv[turn, :, at].astype(f32)).astype(bf16)
            late_copy(turn, part).start()

    def x_copy(slot, mine):
        at = ours if mine else theirs
        return remote(ffn_send.at[slot, at, :], ffn_recv.at[slot, at, :],
                      x_send.at[slot, mine], x_recv.at[slot, mine], XPEER)

    def pair_copy(o, turn):
        quarter, half = lax.rem(order[o], 2), half_of(turn)
        return remote(pair_send.at[quarter, half], pair_recv.at[quarter, half],
                      p_send.at[quarter, half], p_recv.at[quarter, half], ZPEER)

    def fold(o, turn):
        slot = 2 * (o % 2) + turn
        quarter, half = lax.rem(order[o], 2), half_of(turn)

        @pl.when(kept(o))
        def _():
            x_copy(slot, 0).wait_recv()
            pair_send[quarter, half] = (ffn_own[slot, theirs, :]
                                        + ffn_recv[slot, theirs, :].astype(f32)).astype(bf16)
            pair_copy(o, turn).start()

    def last_copy(half):
        return remote(last_send.at[half], last_recv.at[half], l_send.at[half], l_recv.at[half], SIB)

    def finish(o, turn, total):
        quarter, half = lax.rem(order[o], 2), half_of(turn)
        value = (mid_all[ours, piece_cols(o, turn, None)].astype(f32) + total).astype(bf16)

        @pl.when(quarter == core)
        def _():
            result[token_rows(core), pl.ds(at_least(half * sub, LANES), sub)] = value

        @pl.when(quarter != core)
        def _():
            last_send[half] = value
            last_copy(half).start()

    def settle(o, turn):
        slot = 2 * (o % 2) + turn
        quarter, half = lax.rem(order[o], 2), half_of(turn)

        @pl.when(kept(o))
        def _():
            if (o, turn) == (NEAR, 1):
                for part in block_parts(o, turn):
                    late_copy(turn, part).wait_recv()
                finish(o, turn, cross_own[turn] + cross_recv[turn].astype(f32)
                       + late_recv[turn].astype(f32))
            else:
                x_copy(slot, 1).wait_recv()
                pair_copy(o, turn).wait_recv()
                finish(o, turn, ffn_own[slot, ours, :] + ffn_recv[slot, ours, :].astype(f32)
                       + pair_recv[quarter, half].astype(f32))

    def block_parts(o, turn):
        return (0, 1) if (o, turn) == (NEAR, 1) else (None,)

    def pour(source, only=None):
        for part in (0, 1):
            if only is None or part == only:
                for piece in (0,) if part == 0 else (1, 2):
                    across(DOWN, source, piece, "recv")
                beside(DOWN, source, 1 - y, "start", part=part)

    def ready(o, turn, only=None):
        if o == 0 or turn == 0:
            beside(DOWN, order[o], half_of(turn), "recv")
            return
        for part in (0, 1):
            if only is None or part == only:
                beside(DOWN, order[o], 1 - y, "recv", part=part)

    def bring(o, only=None):
        relay(DOWN, order[o], only)
        beside(DOWN, order[o], y, "start")

    def block(o, turn, count, part=None):
        ready(o, turn, part)
        column_block(o, turn, part, 2 * count * LANES)

    keep(DOWN, "wait")

    @pl.when(outer)
    def _():
        block(OWN, 0, few)
        block(OWN, 1, few)
        block(PEER, 0, few)
        pour(peer)
        relay(DOWN, far, (0,))
        block(PEER, 1, few)
        bring(FAR, (1, 2))
        block(FAR, 0, few)
        fold(OWN, 0)
        bring(NEAR)
        pour(far)
        block(FAR, 1, few)
        fold(OWN, 1)
        block(NEAR, 0, few)
        fold(FAR, 0)
        pour(near, 0)
        block(NEAR, 1, few, 0)
        fold(PEER, 0)
        pour(near, 1)
        block(NEAR, 1, few, 1)

    @pl.when(inner)
    def _():
        block(OWN, 0, many)
        block(OWN, 1, many)
        block(PEER, 0, many)
        bring(FAR)
        pour(peer)
        block(PEER, 1, many)
        block(FAR, 0, many)
        fold(OWN, 0)
        pour(far)
        relay(DOWN, near, (1,))
        block(FAR, 1, many)
        fold(OWN, 1)
        bring(NEAR, (2,))
        block(NEAR, 0, many)
        fold(FAR, 0)
        pour(near, 0)
        block(NEAR, 1, many, 0)
        fold(PEER, 0)
        pour(near, 1)
        block(NEAR, 1, many, 1)

    fold(FAR, 1)
    combine(1, 0)
    fold(PEER, 1)
    fold(NEAR, 0)
    combine(1, 1)
    for o in (OWN, FAR, PEER, NEAR):
        for turn in (0, 1):
            settle(o, turn)

    for half in (0, 1):
        last_copy(half).wait()
        result[token_rows(1 - core), half * sub:(half + 1) * sub] = last_recv[half]

    for which in range(5):
        z_sent(which, peer)
        z_sent(which, near)
        if which not in (IN, OUT):
            z_sent(which, far)
        else:
            @pl.when(inner)
            def _():
                for source in (near, far):
                    z_pass(which, source).wait_send()
        for source in (peer, near, far):
            for part in parts(which):
                across(which, source, part, "send")
        if which != DOWN:
            for source in order:
                beside(which, source, None, "send")
            continue
        for half in (0, 1):
            beside(which, z, half, "send")
        for source in order[1:]:
            beside(which, source, y, "send")
            for part in (0, 1):
                beside(which, source, 1 - y, "send", part=part)
    for copy in (to_pair, to_x, to_x_later):
        copy.wait_send()
    near_pieces = [(1, part) for part in block_parts(NEAR, 1)]
    for turn, part in near_pieces:
        cross_copy(turn, part).wait_send()

    @pl.when(keeps_early)
    def _():
        for slot in range(3):
            for mine in (0, 1):
                x_copy(slot, mine).wait_send()
        for turn in (0, 1):
            for o in (OWN, PEER):
                pair_copy(o, turn).wait_send()
        for turn, part in near_pieces:
            late_copy(turn, part).wait_send()

    @pl.when(jnp.logical_not(keeps_early))
    def _():
        for slot in range(4):
            for mine in (0, 1):
                x_copy(slot, mine).wait_send()
        for o, turn in ((FAR, 0), (FAR, 1), (NEAR, 0)):
            pair_copy(o, turn).wait_send()


def pairs_fit(sizes, stream, in_weight, pool_weight, out_weight, gate_weight, down_weight):
    reps, fs, tp = sizes
    tokens, width = stream.shape
    return (reps == 2 and fs == 4 and tp == 4 and tokens % (2 * SEQ) == 0
            and width % (4 * LANES) == 0 and gate_weight.shape[1] % LANES == 0
            and in_weight.shape[1] % LANES == 0 and in_weight.shape[0] % 32 == 0
            and out_weight.shape[0] % 32 == 0 and gate_weight.shape[0] % 64 == 0
            and down_weight.shape[1] == width)


def pair_on_device(sizes, stream, in_weight, pool_weight, pool_scale, out_weight,
                   mix_gain, ffn_gain, gate_weight, up_weight, down_weight):
    if not pairs_fit(sizes, stream, in_weight, pool_weight, out_weight, gate_weight, down_weight):
        return ring_on_device(sizes, stream, in_weight, pool_weight, pool_scale, out_weight,
                              mix_gain, ffn_gain, gate_weight, up_weight, down_weight)
    reps, fs, tp = sizes
    tokens, width = stream.shape
    rows, sub = tokens // 2, width // 2
    features = width * tp
    channels = in_weight.shape[1]
    blocks = gate_weight.shape[1] // LANES
    units = 2 * LANES * (blocks - blocks // 2)
    bf, f32 = jnp.bfloat16, jnp.float32
    vmem = pl.BlockSpec(memory_space=pltpu.VMEM)
    hbm = pl.BlockSpec(memory_space=pltpu.HBM)
    dma = pltpu.SemaphoreType.DMA
    flops = 2 * tokens * (2 * features * channels + 3 * features * gate_weight.shape[1])
    return pl.pallas_call(
        functools.partial(pair_kernel, sizes),
        out_shape=jax.ShapeDtypeStruct(stream.shape, bf),
        in_specs=[hbm] * 10,
        out_specs=vmem,
        scratch_shapes=[
            pltpu.VMEM((in_weight.shape[0] * fs, 2 * channels), bf),
            pltpu.VMEM((2 * out_weight.shape[0], out_weight.shape[1] * fs), bf),
            pltpu.VMEM((up_weight.shape[0] * fs, units), bf),
            pltpu.VMEM((gate_weight.shape[0] * fs, units), bf),
            pltpu.VMEM((units, down_weight.shape[1] * fs), bf),
            pltpu.VMEM((rows, features), bf),
            pltpu.VMEM((rows, features), bf),
            pltpu.VMEM((rows, 2 * channels), bf),
            pltpu.VMEM((2 * rows, units), bf),
            pltpu.VMEM((2 * rows, units), f32),
            pltpu.VMEM((2 * rows, units), f32),
            pltpu.VMEM((2 * rows, features), bf),
            pltpu.VMEM((2 * rows, features), bf),
            pltpu.VMEM(pool_weight.shape, bf),
            pltpu.VMEM((channels,), bf),
            pltpu.VMEM(mix_gain.shape, bf),
            pltpu.VMEM(ffn_gain.shape, bf),
            pltpu.VMEM(pool_weight.shape, bf),
            pltpu.VMEM((channels,), bf),
            pltpu.VMEM((rows, 2 * width), f32),
            pltpu.VMEM((rows, 2 * width), bf),
            pltpu.VMEM((rows, 2 * width), bf),
            pltpu.VMEM((4, 2 * rows, sub), f32),
            pltpu.VMEM((4, 2 * rows, sub), bf),
            pltpu.VMEM((4, 2 * rows, sub), bf),
            pltpu.VMEM((2, 2, rows, sub), bf),
            pltpu.VMEM((2, 2, rows, sub), bf),
            pltpu.VMEM((2 * rows, sub), f32),
            pltpu.VMEM((2, rows, sub), bf),
            pltpu.VMEM((2, rows, sub), bf),
            pltpu.VMEM((2, rows, sub), f32),
            pltpu.VMEM((2, rows, sub), bf),
            pltpu.VMEM((2, rows, sub), bf),
            pltpu.VMEM((2, rows, sub), bf),
            pltpu.VMEM((2, rows, sub), bf),
            dma((24,)), dma((24,)), dma((2, 2)), dma((24,)), dma((24,)),
            dma((27,)), dma((27,)), dma((10,)),
            dma((3,)), dma((3,)), dma((2,)), dma((2,)), dma((2,)), dma((3,)), dma((3,)),
            dma((4, 2)), dma((4, 2)), dma((2, 2)), dma((2, 2)), dma((2,)), dma((2,)),
            dma((3,)), dma((3,)), dma((2, 3)),
        ],
        compiler_params=pltpu.CompilerParams(
            collective_id=0, has_side_effects=True, vmem_limit_bytes=52 * 1024 * 1024),
        cost_estimate=pl.CostEstimate(flops=flops, bytes_accessed=flops // 512, transcendentals=0),
    )(*[pltpu.with_memory_space_constraint(v, pltpu.HBM) for v in (
        stream, in_weight, out_weight, up_weight, gate_weight, down_weight, pool_weight,
        pool_scale, mix_gain, ffn_gain)])


def solution(mesh):
    sizes = tuple(mesh.shape[name] for name in ("rep", "fs", "tp"))
    return jax.shard_map(
        functools.partial(pair_on_device, sizes),
        mesh=mesh,
        in_specs=(
            P(("rep", "fs"), "tp"),
            P("fs", "tp"),
            P("tp", None, None),
            P("tp"),
            P("tp", "fs"),
            P(),
            P(),
            P("fs", "tp"),
            P("fs", "tp"),
            P("tp", "fs"),
        ),
        out_specs=P(("rep", "fs"), "tp"),
        check_vma=False,
    )
```

```python
import functools

import jax
import jax.numpy as jnp
from jax import lax
from jax.experimental import pallas as pl
from jax.experimental.pallas import tpu as pltpu
from jax.sharding import PartitionSpec as P

SEQ = 128
EPSILON = 1e-06
MESH = pl.DeviceIdType.MESH
BY_ROWS = (True, False, True, True, False)
PIECES = ((0, 0), (1, 0), (2, 0), (3, 0), (2, 1), (3, 1), (4, 0), (4, 1))
CHUNKS = (1, 1, 2, 2, 2)


def ring_kernel(sizes, stream, in_w, out_w, up_w, gate_w, down_w, pool_w, scale,
           mix_gain, ffn_gain, result,
           in_all, out_all, up_all, gate_all, down_all,
           rows_all, normed, group_out, hidden, middle, mid_all,
           mix_send, mix_recv, ffn_send, ffn_recv,
           ring_send, ring_recv, fwd_send, fwd_recv, own_sem,
           tp_send, tp_recv, keep_sem):
    reps, fs, tp = sizes
    half = fs // 2
    my_rep, me, my_tp = lax.axis_index("rep"), lax.axis_index("fs"), lax.axis_index("tp")
    own = (in_w, out_w, up_w, gate_w, down_w)
    full = (in_all, out_all, up_all, gate_all, down_all)
    tokens, width = stream.shape

    def turn(at, by, count):
        return lax.rem(at + by + count, count)

    def piece(which, owner, row, count):
        block_rows, block_cols = own[which].shape
        if BY_ROWS[which]:
            return full[which].at[pl.ds(pl.multiple_of(owner * block_rows + row, 16), count), :]
        return full[which].at[pl.ds(pl.multiple_of(row, 16), count),
                              pl.ds(pl.multiple_of(owner * block_cols, 128), block_cols)]

    def span(number, step, way):
        which, chunk = PIECES[number]
        rows = own[which].shape[0]
        cut = rows % (CHUNKS[which] * reps * 2 * 16) == 0
        count = rows // CHUNKS[which] if cut else (rows, 0)[chunk]
        row = chunk * (rows // CHUNKS[which])
        count = count // reps
        row = row + my_rep * count
        if step == half:
            count = count // 2
            row = row + way * count
        return which, row, count

    def empty(number):
        return span(number, 1, 0)[2] == 0

    def ring(number, step, way):
        which, row, count = span(number, step, way)
        sign = 1 - 2 * way
        owner = turn(me, -sign * (step - 1), fs)
        if step == 1:
            source = own[which].at[pl.ds(pl.multiple_of(row, 16), count), :]
        else:
            source = piece(which, owner, row, count)
        return pltpu.make_async_remote_copy(
            src_ref=source, dst_ref=piece(which, owner, row, count),
            send_sem=ring_send.at[number, step - 1, way],
            recv_sem=ring_recv.at[number, step - 1, way],
            device_id={"fs": turn(me, sign, fs)}, device_id_type=MESH)

    def forward(number, step, way, peer):
        which, row, count = span(number, step, way)
        block = piece(which, turn(me, -(1 - 2 * way) * step, fs), row, count)
        return pltpu.make_async_remote_copy(
            src_ref=block, dst_ref=block,
            send_sem=fwd_send.at[number, peer - 1, step - 1, way],
            recv_sem=fwd_recv.at[number, peer - 1, step - 1, way],
            device_id={"rep": turn(my_rep, peer, reps)}, device_id_type=MESH)

    def begin(*numbers):
        for number in numbers:
            if not empty(number):
                for way in (0, 1):
                    ring(number, 1, way).start()

    def advance(number, step):
        if empty(number):
            return
        for way in (0, 1):
            ring(number, step, way).wait_recv()
            if step < half:
                ring(number, step + 1, way).start()
            for peer in range(1, reps):
                forward(number, step, way, peer).start()

    def early(*numbers):
        for number in numbers:
            for step in range(1, half):
                advance(number, step)

    def late(*numbers):
        for number in numbers:
            advance(number, half)

    def arrived(*numbers):
        for number in numbers:
            if PIECES[number][1] == 0:
                keeps[PIECES[number][0]].wait()
            if empty(number):
                continue
            for step in range(1, half + 1):
                for way in (0, 1):
                    for peer in range(1, reps):
                        forward(number, step, way, peer).wait()

    def tp_copy(stage, offset, source, target):
        return pltpu.make_async_remote_copy(
            src_ref=source, dst_ref=target,
            send_sem=tp_send.at[stage, offset - 1], recv_sem=tp_recv.at[stage, offset - 1],
            device_id={"tp": turn(my_tp, offset, tp)}, device_id_type=MESH)

    def feature_cols(owner):
        return pl.ds(pl.multiple_of(owner * width, 128), width)

    barrier = pltpu.get_barrier_semaphore()
    greeted = 0
    for name, at, count, offsets in (
            ("fs", me, fs, (1, -1)),
            ("tp", my_tp, tp, range(1, tp)),
            ("rep", my_rep, reps, range(1, reps))):
        for offset in offsets:
            pl.semaphore_signal(barrier, inc=1, device_id={name: turn(at, offset, count)},
                                device_id_type=MESH)
            greeted += 1
    pl.semaphore_wait(barrier, greeted)

    begin(0, 1)
    stream_sends = []
    for offset in range(1, tp):
        copy = tp_copy(0, offset, stream, rows_all.at[:, feature_cols(my_tp)])
        copy.start()
        stream_sends.append(copy)
    keeps = []
    for which in range(len(own)):
        keep = pltpu.make_async_copy(
            own[which], piece(which, me, 0, own[which].shape[0]), own_sem.at[which])
        keep.start()
        keeps.append(keep)
    keep_stream = pltpu.make_async_copy(
        stream, rows_all.at[:, feature_cols(my_tp)], keep_sem)
    keep_stream.start()
    early(0, 1)
    begin(2, 3, 4)
    late(0, 1)

    def norm_into(source, gain, target):
        tile = 64

        def body(i, carry):
            at = pl.ds(pl.multiple_of(i * tile, tile), tile)
            wide = source[at, :].astype(jnp.float32)
            mean = jnp.mean(wide * wide, axis=-1, keepdims=True)
            target[at, :] = (wide * lax.rsqrt(mean + EPSILON)
                             * gain[...].astype(jnp.float32)).astype(jnp.bfloat16)
            return carry

        lax.fori_loop(0, tokens // tile, body, 0)

    keep_stream.wait()
    for copy in stream_sends:
        copy.wait()
    norm_into(rows_all, mix_gain, normed)
    arrived(0)

    local_groups, group_dim = pool_w.shape[0], pool_w.shape[1]
    at_row = lax.broadcasted_iota(jnp.int32, (SEQ, SEQ), 0)
    at_col = lax.broadcasted_iota(jnp.int32, (SEQ, SEQ), 1)
    insides, inverses = [], []
    for g in range(local_groups):
        group = my_tp * local_groups + g
        level = lax.div(4 * group, local_groups * tp)
        reach = jnp.int32(2)
        for bit in range(1, 4):
            reach = jnp.where(level >= bit, jnp.int32(2 << bit), reach)
        inside = (at_col <= at_row) & (at_col > at_row - reach)
        insides.append(jnp.where(inside, 1.0, 0.0).astype(jnp.bfloat16))
        inverses.append(jnp.minimum(at_row + 1, reach).astype(jnp.float32)[:, :1])

    def mix(i, carry):
        at = pl.ds(pl.multiple_of(i * SEQ, SEQ), SEQ)
        pooled = jnp.dot(normed[at, :], in_all[...],
                         preferred_element_type=jnp.float32).astype(jnp.bfloat16)
        for g in range(local_groups):
            cols = slice(g * group_dim, (g + 1) * group_dim)
            part = pooled[:, cols]
            sums = jnp.dot(insides[g], part, preferred_element_type=jnp.float32)
            contrast = (sums / inverses[g] - part.astype(jnp.float32)).astype(jnp.bfloat16)
            mixed = jnp.dot(contrast, pool_w[g], preferred_element_type=jnp.float32)
            group_out[at, cols] = (mixed * scale[:, cols].astype(jnp.float32)).astype(jnp.bfloat16)
        return carry

    lax.fori_loop(0, tokens // SEQ, mix, 0)

    arrived(1)
    early(2)

    def spread(operand, weights, stage, sends, tile):
        def block(owner, target):
            def body(i, carry):
                at = pl.ds(pl.multiple_of(i * tile, tile), tile)
                target[at, :] = jnp.dot(operand[at, :], weights[:, feature_cols(owner)],
                                        preferred_element_type=jnp.float32).astype(jnp.bfloat16)
                return carry
            lax.fori_loop(0, tokens // tile, body, 0)

        copies = []
        recv = mix_recv if stage == 1 else ffn_recv
        for offset in sorted(range(1, tp), key=lambda o: -min(o, tp - o)):
            block(turn(my_tp, offset, tp), sends.at[offset - 1])
            copy = tp_copy(stage, offset, sends.at[offset - 1], recv.at[offset - 1])
            copy.start()
            copies.append(copy)
        block(my_tp, sends.at[tp - 1])
        return copies

    def gather_sum(base, recv, sends, target):
        tile = 64

        def body(i, carry):
            at = pl.ds(pl.multiple_of(i * tile, tile), tile)
            total = sends[tp - 1, at, :].astype(jnp.float32)
            for k in range(tp - 1):
                total = total + recv[k, at, :].astype(jnp.float32)
            target[at, :] = (base[at, :].astype(jnp.float32) + total).astype(jnp.bfloat16)
            return carry

        lax.fori_loop(0, tokens // tile, body, 0)

    mix_copies = spread(group_out, out_all, 1, mix_send, tokens // 2)
    early(3)
    begin(5)
    for copy in mix_copies:
        copy.wait()
    gather_sum(stream, mix_recv, mix_send, middle)
    keep_middle = pltpu.make_async_copy(middle, mid_all.at[:, feature_cols(my_tp)], keep_sem)
    keep_middle.start()
    middle_copies = []
    for offset in range(1, tp):
        copy = tp_copy(2, offset, middle, mid_all.at[:, feature_cols(my_tp)])
        copy.start()
        middle_copies.append(copy)
    early(4)
    begin(6, 7)
    late(2, 3)
    keep_middle.wait()
    for copy in middle_copies:
        copy.wait()
    norm_into(mid_all, ffn_gain, normed)
    early(5)
    late(4)
    early(6)
    late(5)
    early(7)
    late(6)
    arrived(2, 3, 4, 5)
    tile = tokens // 2

    def gated(i, carry):
        at = pl.ds(pl.multiple_of(i * tile, tile), tile)
        values = normed[at, :]
        gate = jnp.dot(values, gate_all[...], preferred_element_type=jnp.float32)
        up = jnp.dot(values, up_all[...], preferred_element_type=jnp.float32)
        hidden[at, :] = (gate / (1.0 + jnp.exp(-gate)) * up).astype(jnp.bfloat16)
        return carry

    lax.fori_loop(0, tokens // tile, gated, 0)
    late(7)
    arrived(6, 7)
    ffn_copies = spread(hidden, down_all, 3, ffn_send, tokens // 2)
    for number in range(len(PIECES)):
        if not empty(number):
            for step in range(1, half + 1):
                for way in (0, 1):
                    ring(number, step, way).wait_send()
    for copy in ffn_copies:
        copy.wait()
    gather_sum(middle, ffn_recv, ffn_send, result)


def ring_on_device(sizes, stream, in_weight, pool_weight, pool_scale, out_weight,
              mix_gain, ffn_gain, gate_weight, up_weight, down_weight):
    reps, fs, tp = sizes
    half = fs // 2
    tokens, width = stream.shape
    features = width * tp
    own = (in_weight, out_weight, up_weight, gate_weight, down_weight)
    full = [pltpu.VMEM((w.shape[0] * fs, w.shape[1]) if by_rows else (w.shape[0], w.shape[1] * fs),
                       jnp.bfloat16) for w, by_rows in zip(own, BY_ROWS)]
    units = gate_weight.shape[1]
    bf = jnp.bfloat16
    vmem = pl.BlockSpec(memory_space=pltpu.VMEM)
    hbm = pl.BlockSpec(memory_space=pl.ANY)
    dma = pltpu.SemaphoreType.DMA
    flops = 2 * tokens * (2 * features * in_weight.shape[1] + 3 * features * units)
    return pl.pallas_call(
        functools.partial(ring_kernel, sizes),
        out_shape=jax.ShapeDtypeStruct(stream.shape, bf),
        in_specs=[vmem] + [hbm] * 5 + [vmem] * 4,
        out_specs=vmem,
        scratch_shapes=full + [
            pltpu.VMEM((tokens, features), bf),
            pltpu.VMEM((tokens, features), bf),
            pltpu.VMEM((tokens, in_weight.shape[1]), bf),
            pltpu.VMEM((tokens, units), bf),
            pltpu.VMEM((tokens, width), bf),
            pltpu.VMEM((tokens, features), bf),
            pltpu.VMEM((tp, tokens, width), bf),
            pltpu.VMEM((tp - 1, tokens, width), bf),
            pltpu.VMEM((tp, tokens, width), bf),
            pltpu.VMEM((tp - 1, tokens, width), bf),
            dma((len(PIECES), half, 2)),
            dma((len(PIECES), half, 2)),
            dma((len(PIECES), max(reps - 1, 1), half, 2)),
            dma((len(PIECES), max(reps - 1, 1), half, 2)),
            dma((len(own),)),
            dma((4, tp - 1)),
            dma((4, tp - 1)),
            dma(()),
        ],
        compiler_params=pltpu.CompilerParams(
            collective_id=0, has_side_effects=True, vmem_limit_bytes=64 * 1024 * 1024 - 65536),
        cost_estimate=pl.CostEstimate(flops=flops, bytes_accessed=flops // 512, transcendentals=0),
    )(stream, in_weight, out_weight, up_weight, gate_weight, down_weight, pool_weight,
      pool_scale.reshape(1, -1), mix_gain.reshape(1, -1), ffn_gain.reshape(1, -1))


IN, OUT, UP, GATE, DOWN = range(5)
LANES = 128


def pair_kernel(sizes, stream, in_w, out_w, up_w, gate_w, down_w, pool_in, scale_in,
                mix_gain_in, ffn_gain_in, result,
                in_all, out_all, up_all, gate_all, down_all,
                rows_all, normed, group_out, hidden, gate_acts, up_acts, mid_all, normed_ffn,
                pool_w, scale, mix_gain, ffn_gain, pool_sib, scale_sib,
                mix_own, mix_send, mix_recv, ffn_own, ffn_send, ffn_recv, pair_send, pair_recv,
                stage, cross_send, cross_recv, cross_own, late_send, late_recv,
                last_send, last_recv,
                z_send, z_recv, pass_send, y_send, y_recv, d_send, d_recv, own_sem,
                in_send, in_recv, pool_send, pool_recv, mix_sems, mid_send, mid_recv,
                x_send, x_recv, p_send, p_recv, l_send, l_recv, c_send, c_recv, late_sems):
    reps, fs, tp = sizes
    y, z, lane_id = lax.axis_index("rep"), lax.axis_index("fs"), lax.axis_index("tp")
    x, core = lax.div(lane_id, 2), lax.rem(lane_id, 2)
    own = (in_w, out_w, up_w, gate_w, down_w)
    full = (in_all, out_all, up_all, gate_all, down_all)
    tokens, width = stream.shape
    rows = tokens // 2
    wide = 2 * width
    seat, pair = lax.rem(z, 2), lax.div(z, 2)
    peer = z + 1 - 2 * seat
    near = jnp.where(pair == 0, 2, 1)
    far = jnp.where(pair == 0, 3, 0)
    inner = (z == 1) | (z == 2)
    f32, bf16 = jnp.float32, jnp.bfloat16

    blocks = gate_w.shape[1] // LANES
    few, many = blocks // 2, blocks - blocks // 2

    SIB = {"tp": lane_id + 1 - 2 * core}
    XPEER = {"tp": lane_id + 2 - 4 * x}
    XSIB = {"tp": 2 * (1 - x) + 1 - core}
    YPEER = {"rep": 1 - y}
    ZPEER = {"fs": peer}

    def at_least(value, multiple):
        return pl.multiple_of(value, multiple)

    def remote(source, target, send, recv, device):
        return pltpu.make_async_remote_copy(
            src_ref=source, dst_ref=target, send_sem=send, recv_sem=recv,
            device_id=device, device_id_type=MESH)

    def sized(which, roomy, act):
        if which in (IN, OUT) or few == many:
            act(many)
            return

        @pl.when(roomy)
        def _():
            act(many)

        @pl.when(jnp.logical_not(roomy))
        def _():
            act(few)

    slot_of = {IN: 0, OUT: 1, GATE: 2, UP: 3, DOWN: 5}

    def role_of(source):
        return jnp.where(source == peer, 0, jnp.where(source == near, 1,
                         jnp.where(source == far, 2, 3)))

    def flow(which, part, role):
        return 3 * (slot_of[which] + (part or 0)) + role

    def beside_flow(which, source, half, part):
        if which != DOWN:
            return 4 * (IN, OUT, GATE, UP).index(which) + role_of(source)
        if source is z:
            return 16 + half
        return 18 + 3 * role_of(source) + (0 if part is None else 1 + part)

    def extent(which):
        return own[which].shape[1 if which == DOWN else 0]

    def half_span(which, half, part=None):
        size = extent(which) // 2
        if half is None:
            return 0, 2 * size
        if part is None:
            return half * size, size
        return half * size + min(part, 1) * (size // 2), size // 2

    def unit_rows(part, count):
        upper = count - count // 2
        return {1: (0, upper), 2: (upper, count - upper)}.get(part, (0, count))

    def parts(which):
        return {UP: (0, 1), DOWN: (0, 1, 2)}.get(which, (None,))

    def place(which, source, span, core_at, count, part=None):
        block_rows, block_cols = own[which].shape
        ref = full[which]
        start, size = span
        if which == OUT:
            return ref.at[pl.ds(at_least(core_at * block_rows + start, 16), size),
                          pl.ds(at_least(source * block_cols, LANES), block_cols)]
        if which == IN:
            return ref.at[pl.ds(at_least(source * block_rows + start, 16), size),
                          pl.ds(at_least(core_at * block_cols, LANES), block_cols)]
        first = core_at * (count * LANES)
        if which == DOWN:
            skip, taken = unit_rows(part, count)
            return ref.at[pl.ds(at_least(first + skip * LANES, LANES), taken * LANES),
                          pl.ds(at_least(source * block_cols + start, LANES), size)]
        return ref.at[pl.ds(at_least(source * block_rows + start, 16), size),
                      pl.ds(at_least(first, LANES), count * LANES)]

    def held(which, span, roomy, count, part=None):
        ref = own[which]
        start, size = span
        if which in (IN, OUT):
            return ref.at[pl.ds(at_least(start, 16), size), :]
        first = jnp.where(roomy, 0, many * LANES)
        if which == DOWN:
            skip, taken = unit_rows(part, count)
            return ref.at[pl.ds(at_least(first + skip * LANES, LANES), taken * LANES),
                          pl.ds(at_least(start, LANES), size)]
        return ref.at[pl.ds(at_least(start, 16), size),
                      pl.ds(at_least(first, LANES), count * LANES)]

    def z_copies(which, dest, step, only=None):
        roomy = (dest == 1) | (dest == 2)

        def act(n):
            for part in parts(which) if only is None else only:
                span = half_span(which, y, part)
                there = jnp.where(dest == peer, 0, jnp.where(inner, 1, 2))
                copy = remote(held(which, span, roomy, n, part),
                              place(which, z, span, core, n, part),
                              z_send.at[flow(which, part, role_of(dest))],
                              z_recv.at[flow(which, part, there)], {"fs": dest})
                {"start": copy.start, "send": copy.wait_send}[step]()
        sized(which, roomy, act)

    def z_start(which, dest, only=None):
        z_copies(which, dest, "start", only)

    def z_sent(which, dest):
        z_copies(which, dest, "send")

    def z_pass(which, source):
        block = place(which, source, half_span(which, y), core, many)
        return remote(block, block, pass_send.at[which, lax.rem(source, 2)],
                      z_recv.at[flow(which, None, role_of(source))], ZPEER)

    def arrived(which, source, part):
        def act(n):
            block = place(which, source, half_span(which, y, part), core, n, part)
            at = flow(which, part, role_of(source))
            remote(block, block, y_send.at[0], z_recv.at[at], YPEER).wait_recv()
        sized(which, inner, act)

    def across(which, source, part, step):
        def act(n):
            half = 1 - y if step == "recv" else y
            block = place(which, source, half_span(which, half, part), core, n, part)
            at = flow(which, part, role_of(source))
            copy = remote(block, block, y_send.at[0], y_recv.at[at], YPEER)
            {"start": copy.start, "recv": copy.wait_recv, "send": copy.wait_send}[step]()
        sized(which, inner, act)

    def beside(which, source, half, step, mine=False, part=None):
        at = beside_flow(which, source, half, part)
        whose = 1 - core if step == "recv" else core

        def act(n):
            span = half_span(which, half, part)
            block = place(which, source, span, whose, n)
            start = held(which, span, inner, n) if mine else block
            copy = remote(start, block, d_send.at[at], d_recv.at[at], SIB)
            {"start": copy.start, "recv": copy.wait_recv, "send": copy.wait_send}[step]()
        sized(which, inner, act)

    def keep(which, step):
        def act(n):
            span = half_span(which, None)
            copy = pltpu.make_async_copy(held(which, span, inner, n),
                                         place(which, z, span, core, n), own_sem.at[which])
            {"start": copy.start, "wait": copy.wait}[step]()
        sized(which, inner, act)

    def relay(which, source, only=None):
        for part in parts(which):
            if only is None or part in only:
                arrived(which, source, part)
                across(which, source, part, "start")

    def share(which, source):
        for part in parts(which):
            across(which, source, part, "recv")
        beside(which, source, None, "start")

    def feature_cols(owner):
        return pl.ds(at_least(owner * width, LANES), width)

    def token_rows(half):
        return pl.ds(at_least(half * rows, 16), rows)

    def stream_copy(number, device, half):
        return remote(stream.at[token_rows(half), :], rows_all.at[:, feature_cols(lane_id)],
                      in_send.at[number], in_recv.at[number], device)

    small_copies = [pltpu.make_async_copy(source, target, own_sem.at[6 + number])
                    for number, (source, target) in enumerate((
                        (mix_gain_in, mix_gain), (ffn_gain_in, ffn_gain),
                        (pool_in, pool_w), (scale_in, scale)))]
    for copy in small_copies:
        copy.start()

    barrier = pltpu.get_barrier_semaphore()
    greeted = 0
    for device in (SIB, XPEER, XSIB, YPEER, ZPEER, {"fs": near}, {"fs": far}):
        pl.semaphore_signal(barrier, inc=1, device_id=device, device_id_type=MESH)
        greeted += 1
    pl.semaphore_wait(barrier, greeted)

    outer = jnp.logical_not(inner)
    z_start(IN, near)
    z_start(IN, peer)
    stream_copies = [stream_copy(0, XPEER, core), stream_copy(1, XSIB, 1 - core),
                     stream_copy(2, SIB, 1 - core)]
    for copy in stream_copies:
        copy.start()
    z_start(OUT, near)
    z_start(OUT, peer)
    keep(IN, "start")
    beside(IN, z, None, "start", mine=True)
    pool_copy = remote(pool_in, pool_sib, pool_send.at[0], pool_recv.at[0], SIB)
    scale_copy = remote(scale_in, scale_sib, pool_send.at[1], pool_recv.at[1], SIB)
    pool_copy.start()
    scale_copy.start()

    @pl.when(inner)
    def _():
        z_start(GATE, near)
        z_start(GATE, far)
        z_start(UP, near)

    @pl.when(outer)
    def _():
        z_start(GATE, peer)
        z_start(GATE, far)
        z_start(UP, far)
        z_start(UP, peer)

    for which in (OUT, GATE, UP, DOWN):
        keep(which, "start")
        for half in (0, 1) if which == DOWN else (None,):
            beside(which, z, half, "start", mine=True)

    own_rows = pltpu.make_async_copy(stream.at[token_rows(core), :],
                                     rows_all.at[:, feature_cols(lane_id)], own_sem.at[5])
    own_rows.start()

    def take(which):
        relay(which, peer)
        for source in (near, far):
            arrived(which, source, None)

            @pl.when(inner)
            def _():
                z_pass(which, source).start()
            across(which, source, None, "start")

    take(IN)

    @pl.when(inner)
    def _():
        take(OUT)

    def norm_into(source, gain, target, first, count):
        tile = 64

        def body(i, carry):
            at = pl.ds(at_least(first + i * tile, tile), tile)
            values = source[at, :].astype(f32)
            mean = jnp.mean(values * values, axis=-1, keepdims=True)
            target[at, :] = (values * lax.rsqrt(mean + EPSILON)
                             * gain[...].astype(f32).reshape(1, -1)).astype(bf16)
            return carry

        lax.fori_loop(0, count // tile, body, 0)

    own_rows.wait()
    for copy in small_copies:
        copy.wait()
    for copy in stream_copies:
        copy.wait()
    norm_into(rows_all, mix_gain, normed, 0, rows)
    for source in (peer, near, far):
        share(IN, source)

    @pl.when(outer)
    def _():
        take(OUT)

    pool_copy.wait()
    scale_copy.wait()
    for source in (z, peer, near, far):
        beside(IN, source, None, "recv")
    keep(IN, "wait")

    local_groups, group_dim = pool_w.shape[0], pool_w.shape[1]
    at_row = lax.broadcasted_iota(jnp.int32, (SEQ, SEQ), 0)
    at_col = lax.broadcasted_iota(jnp.int32, (SEQ, SEQ), 1)
    pooled = jnp.dot(normed[...], in_all[...], preferred_element_type=f32).astype(bf16)
    for g in range(2 * local_groups):
        owner, place_in = divmod(g, local_groups)
        group = x * 2 * local_groups + g
        level = lax.div(4 * group, local_groups * tp)
        reach = jnp.int32(2)
        for bit in range(1, 4):
            reach = jnp.where(level >= bit, jnp.int32(2 << bit), reach)
        inside = jnp.where((at_col <= at_row) & (at_col > at_row - reach), 1.0, 0.0).astype(bf16)
        counts = jnp.minimum(at_row + 1, reach).astype(f32)[:, :1]
        is_own = core == owner
        cols = slice(g * group_dim, (g + 1) * group_dim)
        own_cols = slice(place_in * group_dim, (place_in + 1) * group_dim)
        weight = jnp.where(is_own, pool_w[place_in], pool_sib[place_in])
        factor = jnp.where(is_own, scale[own_cols].astype(f32).reshape(1, -1),
                           scale_sib[own_cols].astype(f32).reshape(1, -1))
        for s in range(rows // SEQ):
            at = slice(s * SEQ, (s + 1) * SEQ)
            part = pooled[at, cols]
            sums = jnp.dot(inside, part, preferred_element_type=f32)
            contrast = (sums / counts - part.astype(f32)).astype(bf16)
            mixed = jnp.dot(contrast, weight, preferred_element_type=f32)
            group_out[at, cols] = (mixed * factor).astype(bf16)

    for source in (peer, near, far):
        share(OUT, source)
    for source in (z, peer, near, far):
        beside(OUT, source, None, "recv")
    keep(OUT, "wait")

    def half_cols(owner):
        return pl.ds(at_least(owner * wide, LANES), wide)

    mix_send[...] = jnp.dot(group_out[...], out_all[:, half_cols(1 - x)],
                            preferred_element_type=f32).astype(bf16)
    mix_copy = remote(mix_send, mix_recv, mix_sems.at[0], mix_sems.at[1], XPEER)
    mix_copy.start()
    mix_own[...] = jnp.dot(group_out[...], out_all[:, half_cols(x)], preferred_element_type=f32)

    @pl.when(inner)
    def _():
        relay(GATE, peer)
        relay(GATE, near)

    @pl.when(outer)
    def _():
        relay(GATE, far)

    mix_copy.wait()
    mid_rows = pl.ds(at_least(seat * rows, 16), rows)
    mid_all[mid_rows, half_cols(x)] = (
        rows_all[:, half_cols(x)].astype(f32) + (mix_own[...] + mix_recv[...].astype(f32))).astype(bf16)

    def mid_copy(number, block, device):
        view = mid_all.at[pl.ds(at_least(block * rows, 16), rows), half_cols(x)]
        return remote(view, view, mid_send.at[number], mid_recv.at[number], device)

    to_pair, to_x, to_x_later = mid_copy(0, seat, ZPEER), mid_copy(1, seat, XPEER), mid_copy(2, 1 - seat, XPEER)
    to_pair.start()
    to_x.start()

    @pl.when(inner)
    def _():
        z_start(GATE, peer)
        z_start(UP, peer)
        z_start(DOWN, near, (0,))
        z_start(UP, far)
        z_start(DOWN, far)
        z_start(DOWN, near, (1, 2))
        share(GATE, peer)
        share(GATE, near)
        relay(UP, peer)
        relay(UP, near)

    @pl.when(outer)
    def _():
        z_start(GATE, near)
        z_start(UP, near)
        share(GATE, far)
        relay(UP, far)
        relay(GATE, near)

    to_pair.wait_recv()
    to_x_later.start()

    @pl.when(inner)
    def _():
        z_start(DOWN, peer)
        share(UP, peer)
        relay(DOWN, near, (0,))

    @pl.when(outer)
    def _():
        z_start(DOWN, peer)
        z_start(DOWN, near)
        z_start(DOWN, far)
        share(UP, far)
        share(GATE, near)

    to_x.wait_recv()
    norm_into(mid_all, ffn_gain, normed_ffn, seat * rows, rows)

    @pl.when(inner)
    def _():
        share(UP, near)
        relay(GATE, far)

    @pl.when(outer)
    def _():
        relay(GATE, peer)

    to_x_later.wait_recv()
    norm_into(mid_all, ffn_gain, normed_ffn, (1 - seat) * rows, rows)

    depth = gate_all.shape[0] // 2
    pair_at = pl.ds(at_least(pair * depth, LANES), depth)
    cross_at = pl.ds(at_least((1 - pair) * depth, LANES), depth)
    early_at = pl.ds(at_least(jnp.where(inner, pair, 1 - pair) * depth, LANES), depth)
    later_at = pl.ds(at_least(jnp.where(inner, 1 - pair, pair) * depth, LANES), depth)
    tile = rows

    def by_tiles(body):
        def all_tiles(count):
            wide_units = 2 * count * LANES

            def step(i, carry):
                body(pl.ds(at_least(i * tile, tile), tile), wide_units)
                return carry
            lax.fori_loop(0, 2 * rows // tile, step, 0)
        sized(UP, inner, all_tiles)

    def partial_dot(at, depth_at, weights, n):
        return jnp.dot(normed_ffn[at, depth_at], weights[depth_at, :n], preferred_element_type=f32)

    def gate_first(at, n):
        gate_acts[at, :n] = partial_dot(at, early_at, gate_all, n)

    def gate_second(at, n):
        gate = gate_acts[at, :n] + partial_dot(at, later_at, gate_all, n)
        gate_acts[at, :n] = gate / (1.0 + jnp.exp(-gate))

    def up_first(at, n):
        up_acts[at, :n] = partial_dot(at, pair_at, up_all, n)

    def up_second(at, n):
        up = up_acts[at, :n] + partial_dot(at, cross_at, up_all, n)
        hidden[at, :n] = (gate_acts[at, :n] * up).astype(bf16)

    keep(GATE, "wait")
    for source in (jnp.where(inner, z, far), jnp.where(inner, peer, near)):
        beside(GATE, source, None, "recv")
    by_tiles(gate_first)

    @pl.when(inner)
    def _():
        relay(UP, far)
        share(GATE, far)

    @pl.when(outer)
    def _():
        relay(UP, peer)
        share(GATE, peer)

    for source in (jnp.where(inner, near, z), jnp.where(inner, far, peer)):
        beside(GATE, source, None, "recv")
    by_tiles(gate_second)

    @pl.when(outer)
    def _():
        share(UP, peer)
        relay(UP, near)

    keep(UP, "wait")
    for source in (z, peer):
        beside(UP, source, None, "recv")
    by_tiles(up_first)

    relay(DOWN, peer)

    @pl.when(inner)
    def _():
        share(UP, far)

    @pl.when(outer)
    def _():
        share(UP, near)

    beside(DOWN, peer, y, "start")

    for source in (near, far):
        beside(UP, source, None, "recv")
    by_tiles(up_second)

    sub = width // 2
    order = (z, peer, far, near)
    keeps_early = x == pair

    def half_of(turn):
        return y if turn == 0 else 1 - y

    half_sub = sub // 2

    def piece_cols(o, turn, part):
        start = order[o] * width + half_of(turn) * sub
        if part is None:
            return pl.ds(at_least(start, LANES), sub)
        return pl.ds(at_least(start + part * half_sub, LANES), half_sub)

    def lanes(part):
        return slice(0, sub) if part is None else slice(part * half_sub, (part + 1) * half_sub)

    ours = pl.ds(at_least(seat * rows, 16), rows)
    theirs = pl.ds(at_least((1 - seat) * rows, 16), rows)

    OWN, PEER, FAR, NEAR = range(4)

    def kept(o):
        return keeps_early if o < FAR else jnp.logical_not(keeps_early)

    def column_block(o, turn, part, n):
        values = jnp.dot(hidden[:, :n], down_all[:n, piece_cols(o, turn, part)],
                         preferred_element_type=f32)
        if (o, turn) == (NEAR, 1):
            stage[:, lanes(part)] = values
            cross_send[turn, :, lanes(part)] = stage[theirs, lanes(part)].astype(bf16)
            cross_copy(turn, part).start()
            cross_own[turn, :, lanes(part)] = stage[ours, lanes(part)]
            return
        slot = 2 * (o % 2) + turn

        @pl.when(kept(o))
        def _():
            ffn_own[slot] = values

        @pl.when(jnp.logical_not(kept(o)))
        def _():
            ffn_send[slot] = values.astype(bf16)
            x_copy(slot, 0).start()
            x_copy(slot, 1).start()

    def cross_copy(turn, part):
        at, number = lanes(part), turn + (part or 0)
        return remote(cross_send.at[turn, :, at], cross_recv.at[turn, :, at],
                      c_send.at[number], c_recv.at[number], ZPEER)

    def late_copy(turn, part):
        at, number = lanes(part), turn + (part or 0)
        return remote(late_send.at[turn, :, at], late_recv.at[turn, :, at],
                      late_sems.at[0, number], late_sems.at[1, number], XPEER)

    def combine(turn, part=None):
        at = lanes(part)
        cross_copy(turn, part).wait_recv()

        @pl.when(keeps_early)
        def _():
            late_send[turn, :, at] = (cross_own[turn, :, at]
                                      + cross_recv[turn, :, at].astype(f32)).astype(bf16)
            late_copy(turn, part).start()

    def x_copy(slot, mine):
        at = ours if mine else theirs
        return remote(ffn_send.at[slot, at, :], ffn_recv.at[slot, at, :],
                      x_send.at[slot, mine], x_recv.at[slot, mine], XPEER)

    def pair_copy(o, turn):
        quarter, half = lax.rem(order[o], 2), half_of(turn)
        return remote(pair_send.at[quarter, half], pair_recv.at[quarter, half],
                      p_send.at[quarter, half], p_recv.at[quarter, half], ZPEER)

    def fold(o, turn):
        slot = 2 * (o % 2) + turn
        quarter, half = lax.rem(order[o], 2), half_of(turn)

        @pl.when(kept(o))
        def _():
            x_copy(slot, 0).wait_recv()
            pair_send[quarter, half] = (ffn_own[slot, theirs, :]
                                        + ffn_recv[slot, theirs, :].astype(f32)).astype(bf16)
            pair_copy(o, turn).start()

    def last_copy(half):
        return remote(last_send.at[half], last_recv.at[half], l_send.at[half], l_recv.at[half], SIB)

    def finish(o, turn, total):
        quarter, half = lax.rem(order[o], 2), half_of(turn)
        value = (mid_all[ours, piece_cols(o, turn, None)].astype(f32) + total).astype(bf16)

        @pl.when(quarter == core)
        def _():
            result[token_rows(core), pl.ds(at_least(half * sub, LANES), sub)] = value

        @pl.when(quarter != core)
        def _():
            last_send[half] = value
            last_copy(half).start()

    def settle(o, turn):
        slot = 2 * (o % 2) + turn
        quarter, half = lax.rem(order[o], 2), half_of(turn)

        @pl.when(kept(o))
        def _():
            if (o, turn) == (NEAR, 1):
                for part in block_parts(o, turn):
                    late_copy(turn, part).wait_recv()
                finish(o, turn, cross_own[turn] + cross_recv[turn].astype(f32)
                       + late_recv[turn].astype(f32))
            else:
                x_copy(slot, 1).wait_recv()
                pair_copy(o, turn).wait_recv()
                finish(o, turn, ffn_own[slot, ours, :] + ffn_recv[slot, ours, :].astype(f32)
                       + pair_recv[quarter, half].astype(f32))

    def block_parts(o, turn):
        return (0, 1) if (o, turn) == (NEAR, 1) else (None,)

    def pour(source, only=None):
        for part in (0, 1):
            if only is None or part == only:
                for piece in (0,) if part == 0 else (1, 2):
                    across(DOWN, source, piece, "recv")
                beside(DOWN, source, 1 - y, "start", part=part)

    def ready(o, turn, only=None):
        if o == 0 or turn == 0:
            beside(DOWN, order[o], half_of(turn), "recv")
            return
        for part in (0, 1):
            if only is None or part == only:
                beside(DOWN, order[o], 1 - y, "recv", part=part)

    def bring(o, only=None):
        relay(DOWN, order[o], only)
        beside(DOWN, order[o], y, "start")

    def block(o, turn, count, part=None):
        ready(o, turn, part)
        column_block(o, turn, part, 2 * count * LANES)

    keep(DOWN, "wait")

    @pl.when(outer)
    def _():
        block(OWN, 0, few)
        block(OWN, 1, few)
        block(PEER, 0, few)
        pour(peer)
        relay(DOWN, far, (0,))
        block(PEER, 1, few)
        bring(FAR, (1, 2))
        block(FAR, 0, few)
        fold(OWN, 0)
        bring(NEAR)
        pour(far)
        block(FAR, 1, few)
        fold(OWN, 1)
        block(NEAR, 0, few)
        fold(FAR, 0)
        pour(near, 0)
        block(NEAR, 1, few, 0)
        fold(PEER, 0)
        pour(near, 1)
        block(NEAR, 1, few, 1)

    @pl.when(inner)
    def _():
        block(OWN, 0, many)
        block(OWN, 1, many)
        block(PEER, 0, many)
        bring(FAR)
        pour(peer)
        block(PEER, 1, many)
        block(FAR, 0, many)
        fold(OWN, 0)
        pour(far)
        relay(DOWN, near, (1,))
        block(FAR, 1, many)
        fold(OWN, 1)
        bring(NEAR, (2,))
        block(NEAR, 0, many)
        fold(FAR, 0)
        pour(near, 0)
        block(NEAR, 1, many, 0)
        fold(PEER, 0)
        pour(near, 1)
        block(NEAR, 1, many, 1)

    fold(FAR, 1)
    combine(1, 0)
    fold(PEER, 1)
    fold(NEAR, 0)
    combine(1, 1)
    for o in (OWN, FAR, PEER, NEAR):
        for turn in (0, 1):
            settle(o, turn)

    for half in (0, 1):
        last_copy(half).wait()
        result[token_rows(1 - core), half * sub:(half + 1) * sub] = last_recv[half]

    for which in range(5):
        z_sent(which, peer)
        z_sent(which, near)
        if which not in (IN, OUT):
            z_sent(which, far)
        else:
            @pl.when(inner)
            def _():
                for source in (near, far):
                    z_pass(which, source).wait_send()
        if which != DOWN:
            for source in order:
                beside(which, source, None, "send")
            continue
        for half in (0, 1):
            beside(which, z, half, "send")
        for source in order[1:]:
            beside(which, source, y, "send")
            for part in (0, 1):
                beside(which, source, 1 - y, "send", part=part)

    def forwarded(count):
        elements = 3 * (in_w.shape[0] * in_w.shape[1] + out_w.shape[0] * out_w.shape[1]
                        + 2 * gate_w.shape[0] * count * LANES
                        + down_w.shape[1] * count * LANES) // 2
        view = down_all.at[pl.ds(0, elements // down_all.shape[1]), :]
        remote(view, view, y_send.at[0], y_recv.at[0], YPEER).wait_send()

    sized(UP, inner, forwarded)
    for copy in (to_pair, to_x, to_x_later):
        copy.wait_send()
    near_pieces = [(1, part) for part in block_parts(NEAR, 1)]
    for turn, part in near_pieces:
        cross_copy(turn, part).wait_send()

    @pl.when(keeps_early)
    def _():
        for slot in range(3):
            for mine in (0, 1):
                x_copy(slot, mine).wait_send()
        for turn in (0, 1):
            for o in (OWN, PEER):
                pair_copy(o, turn).wait_send()
        for turn, part in near_pieces:
            late_copy(turn, part).wait_send()

    @pl.when(jnp.logical_not(keeps_early))
    def _():
        for slot in range(4):
            for mine in (0, 1):
                x_copy(slot, mine).wait_send()
        for o, turn in ((FAR, 0), (FAR, 1), (NEAR, 0)):
            pair_copy(o, turn).wait_send()


def pairs_fit(sizes, stream, in_weight, pool_weight, out_weight, gate_weight, down_weight):
    reps, fs, tp = sizes
    tokens, width = stream.shape
    return (reps == 2 and fs == 4 and tp == 4 and tokens % (2 * SEQ) == 0
            and width % (4 * LANES) == 0 and gate_weight.shape[1] % LANES == 0
            and in_weight.shape[1] % LANES == 0 and in_weight.shape[0] % 32 == 0
            and out_weight.shape[0] % 32 == 0 and gate_weight.shape[0] % 64 == 0
            and down_weight.shape[1] == width)


def pair_on_device(sizes, stream, in_weight, pool_weight, pool_scale, out_weight,
                   mix_gain, ffn_gain, gate_weight, up_weight, down_weight):
    if not pairs_fit(sizes, stream, in_weight, pool_weight, out_weight, gate_weight, down_weight):
        return ring_on_device(sizes, stream, in_weight, pool_weight, pool_scale, out_weight,
                              mix_gain, ffn_gain, gate_weight, up_weight, down_weight)
    reps, fs, tp = sizes
    tokens, width = stream.shape
    rows, sub = tokens // 2, width // 2
    features = width * tp
    channels = in_weight.shape[1]
    blocks = gate_weight.shape[1] // LANES
    units = 2 * LANES * (blocks - blocks // 2)
    bf, f32 = jnp.bfloat16, jnp.float32
    vmem = pl.BlockSpec(memory_space=pltpu.VMEM)
    hbm = pl.BlockSpec(memory_space=pltpu.HBM)
    dma = pltpu.SemaphoreType.DMA
    flops = 2 * tokens * (2 * features * channels + 3 * features * gate_weight.shape[1])
    return pl.pallas_call(
        functools.partial(pair_kernel, sizes),
        out_shape=jax.ShapeDtypeStruct(stream.shape, bf),
        in_specs=[hbm] * 10,
        out_specs=vmem,
        scratch_shapes=[
            pltpu.VMEM((in_weight.shape[0] * fs, 2 * channels), bf),
            pltpu.VMEM((2 * out_weight.shape[0], out_weight.shape[1] * fs), bf),
            pltpu.VMEM((up_weight.shape[0] * fs, units), bf),
            pltpu.VMEM((gate_weight.shape[0] * fs, units), bf),
            pltpu.VMEM((units, down_weight.shape[1] * fs), bf),
            pltpu.VMEM((rows, features), bf),
            pltpu.VMEM((rows, features), bf),
            pltpu.VMEM((rows, 2 * channels), bf),
            pltpu.VMEM((2 * rows, units), bf),
            pltpu.VMEM((2 * rows, units), f32),
            pltpu.VMEM((2 * rows, units), f32),
            pltpu.VMEM((2 * rows, features), bf),
            pltpu.VMEM((2 * rows, features), bf),
            pltpu.VMEM(pool_weight.shape, bf),
            pltpu.VMEM((channels,), bf),
            pltpu.VMEM(mix_gain.shape, bf),
            pltpu.VMEM(ffn_gain.shape, bf),
            pltpu.VMEM(pool_weight.shape, bf),
            pltpu.VMEM((channels,), bf),
            pltpu.VMEM((rows, 2 * width), f32),
            pltpu.VMEM((rows, 2 * width), bf),
            pltpu.VMEM((rows, 2 * width), bf),
            pltpu.VMEM((4, 2 * rows, sub), f32),
            pltpu.VMEM((4, 2 * rows, sub), bf),
            pltpu.VMEM((4, 2 * rows, sub), bf),
            pltpu.VMEM((2, 2, rows, sub), bf),
            pltpu.VMEM((2, 2, rows, sub), bf),
            pltpu.VMEM((2 * rows, sub), f32),
            pltpu.VMEM((2, rows, sub), bf),
            pltpu.VMEM((2, rows, sub), bf),
            pltpu.VMEM((2, rows, sub), f32),
            pltpu.VMEM((2, rows, sub), bf),
            pltpu.VMEM((2, rows, sub), bf),
            pltpu.VMEM((2, rows, sub), bf),
            pltpu.VMEM((2, rows, sub), bf),
            dma((24,)), dma((24,)), dma((2, 2)), dma((1,)), dma((24,)),
            dma((27,)), dma((27,)), dma((10,)),
            dma((3,)), dma((3,)), dma((2,)), dma((2,)), dma((2,)), dma((3,)), dma((3,)),
            dma((4, 2)), dma((4, 2)), dma((2, 2)), dma((2, 2)), dma((2,)), dma((2,)),
            dma((3,)), dma((3,)), dma((2, 3)),
        ],
        compiler_params=pltpu.CompilerParams(
            collective_id=0, has_side_effects=True, vmem_limit_bytes=52 * 1024 * 1024),
        cost_estimate=pl.CostEstimate(flops=flops, bytes_accessed=flops // 512, transcendentals=0),
    )(*[pltpu.with_memory_space_constraint(v, pltpu.HBM) for v in (
        stream, in_weight, out_weight, up_weight, gate_weight, down_weight, pool_weight,
        pool_scale, mix_gain, ffn_gain)])


def solution(mesh):
    sizes = tuple(mesh.shape[name] for name in ("rep", "fs", "tp"))
    return jax.shard_map(
        functools.partial(pair_on_device, sizes),
        mesh=mesh,
        in_specs=(
            P(("rep", "fs"), "tp"),
            P("fs", "tp"),
            P("tp", None, None),
            P("tp"),
            P("tp", "fs"),
            P(),
            P(),
            P("fs", "tp"),
            P("fs", "tp"),
            P("tp", "fs"),
        ),
        out_specs=P(("rep", "fs"), "tp"),
        check_vma=False,
    )
```
